32 devices in a mesh: ep: 8 (over z, x), tp: 4 (over y, core).
Axes of the slice: x: 2, y: 2, z: 4, core: 2. Of those that a mesh axis runs over, the one named last changes fastest.
Arguments:
- tokens: bfloat16 [512, 4096], P('ep'), may hold values from -6 to 6
- state_in: float32 [512, 4096], P('ep', 'tp'), may hold values from -6 to 6
- conv_in: bfloat16 [512, 3, 4096], P('ep', None, 'tp'), may hold values from -6 to 6
- mix_gain: bfloat16 [4096], replicated, may hold values from 0.099609375 to 1.8984375
- rnn_weight: bfloat16 [4096, 4096], P('ep', 'tp'), may hold values from -0.09375 to 0.09375
- gate_weight: bfloat16 [4096, 4096], P('ep', 'tp'), may hold values from -0.09375 to 0.09375
- conv_weight: bfloat16 [4, 4096], P(None, 'tp'), may hold values from -3 to 3
- rate_weight: bfloat16 [16, 256, 256], P('tp'), may hold values from -0.375 to 0.375
- input_weight: bfloat16 [16, 256, 256], P('tp'), may hold values from -0.375 to 0.375
- rate_param: float32 [4096], P('tp'), may hold values from 1 to 6
- out_weight: bfloat16 [4096, 4096], P('tp'), may hold values from -0.09375 to 0.09375
- moe_gain: bfloat16 [4096], replicated, may hold values from 0.099609375 to 1.8984375
- expert_gate: bfloat16 [8, 4096, 2048], P('ep', None, 'tp'), may hold values from -0.09375 to 0.09375
- expert_up: bfloat16 [8, 4096, 2048], P('ep', None, 'tp'), may hold values from -0.09375 to 0.09375
- expert_down: bfloat16 [8, 2048, 4096], P('ep', 'tp'), may hold values from -0.125 to 0.125
- routes: int32 [512, 2], P('ep'), may hold values from 0 to 7, all different within a row; in each aligned block of 64 rows (0 to 63, 64 to 127, ...) at most 32 rows name the same one
- route_prob: float32 [512, 2], P('ep'), may hold values from 0.1 to 1
Outputs:
- layer_out: bfloat16 [512, 4096], P('ep', 'tp')
- state_out: float32 [512, 4096], P('ep', 'tp')
- conv_out: bfloat16 [512, 3, 4096], P('ep', None, 'tp')
The draws below stay inside these ranges and needn't reach their ends.
Inputs may be any that keep to these rules, and one draw needn't show every extreme that they name: `routes`: the 2 experts of a sequence differ. Among the rows of one index of ep no expert is named more than 32 times, and in every draw some expert is named exactly 32 times there.
All inputs are finite; a program needn't handle non-finite values.
Results may differ from the reference program's by a relative error of at most 0.014.
Values may be sent and summed in bfloat16 or wider, within the bound.
A program may use at most 64 MiB of HBM per device.

```python
import math
import jax
import jax.numpy as jnp
import numpy as np
from jax import lax

D = 4096
D_RNN = 4096
RG_BLOCKS = 16
RG_BW = 256
FF_E = 2048
TOPK = 2
SEQ_GRP = 64
BATCH = 512
EXPERTS = 8
CAP = 32
N_EP = 8
N_TP = 4


def shard_levels(rng, extent, split, low, high):
    def one(dim, shards_of):
        steps = jax.random.uniform(jax.random.fold_in(jax.random.fold_in(rng, 6), dim), (shards_of,), jnp.float32, low / len(split), high / len(split))
        return jnp.repeat(jnp.exp(steps), extent[dim] // shards_of).reshape((-1,) + (1,) * (len(extent) - dim - 1))

    loudness = one(*split[0])
    for cut in split[1:]:
        loudness = loudness * one(*cut)
    return loudness


def assign_block(key, own, number, rows, amount, top, reach, lean):
    ranking = jax.random.permutation(key, amount)
    crowded, ordinary = portions_of(amount, rows * top, reach, lean, True), portions_of(amount, rows * top, reach, lean, False)
    places = jnp.arange(amount)

    def named(tallies, offset_by):
        used = int((tallies > 0).sum())
        fixed = max(1, used // 4)
        passed = fixed + (places - fixed + offset_by * (used - fixed)) % max(1, amount - fixed)
        return jnp.zeros((amount,), jnp.int32).at[ranking[jnp.where(places < fixed, places, passed)]].set(jnp.asarray(tallies, jnp.int32))

    tallies = jnp.where(number % 4 == 0, named(crowded, number // 4), named(ordinary, number - number // 4 - 1))
    mixed = jax.random.permutation(jax.random.fold_in(own, 3), amount)
    source_of, taker = mixed[0:amount // 2 * 2:2], mixed[1:amount // 2 * 2:2]
    room = jnp.minimum(tallies[source_of] - 1, reach - tallies[taker]) // 2
    room = jnp.where((source_of == ranking[0]) | (taker == ranking[0]) | (tallies[taker] == 0), 0, jnp.maximum(room, 0))
    passed = jax.random.randint(jax.random.fold_in(own, 4), (amount // 2,), 0, 1 << 20) % (room + 1)
    tallies = tallies.at[source_of].add(-passed).at[taker].add(passed)
    items = jnp.searchsorted(jnp.cumsum(tallies), jnp.arange(rows * top), side="right").astype(jnp.int32)
    table = items.reshape(top, rows).T
    table = table[jax.random.permutation(jax.random.fold_in(own, 1), rows)]
    offset_by = jax.random.randint(jax.random.fold_in(own, 2), (rows, 1), 0, top)
    return jnp.take_along_axis(table, (jnp.arange(top)[None, :] + offset_by) % top, axis=1)


def portions_of(number_of, total, limit, slope, full):
    portions = [(1 << 20) // math.isqrt(standing ** slope) + 1 for standing in range(1, number_of + 1)]
    largest = limit if full else min(limit, max(-(-total // number_of), total * portions[0] // sum(portions)))
    least = 1 if total - largest >= number_of - 1 else 0
    given, spare = [largest] + [least] * (number_of - 1), total - largest - least * (number_of - 1)
    while spare > 0:
        movable = [i for i in range(1, number_of) if given[i] < largest] or [i for i in range(1, number_of) if given[i] < limit]
        whole, budget = sum([portions[i] for i in movable]), spare
        for i in movable:
            addition = min(limit - given[i], max(1, budget * portions[i] // whole), spare)
            given[i] = given[i] + addition
            spare = spare - addition
    return np.array(given)


def scatter_about(own_key, dims, scale, limit, shards=(), held_as=jnp.bfloat16):
    level = shard_levels(own_key, dims, shards, -0.22, 0.18) if shards else 1.0
    drawn = jax.random.normal(own_key, dims, jnp.float32) * scale * level
    return jnp.minimum(jnp.maximum(drawn, -limit), limit).astype(held_as)


def setup_inputs(seed: int = 0) -> dict:
    streams_of = jax.random.split(jax.random.key(seed), 18)
    tokens = scatter_about(streams_of[0], (BATCH, D), 1.0, 6.0, ((0, 8),))
    state_in = scatter_about(streams_of[1], (BATCH, D_RNN), 1.0, 6.0, ((0, 8), (1, 4)), jnp.float32)
    conv_in = scatter_about(streams_of[2], (BATCH, 3, D_RNN), 1.0, 6.0, ((0, 8), (2, 4)))
    mix_gain = jnp.clip(1.0 + 0.18 * jax.random.normal(streams_of[3], (D,), jnp.float32), 0.099609375, 1.8984375).astype(jnp.bfloat16)
    rnn_weight = scatter_about(streams_of[4], (D, D_RNN), D ** -0.5, 0.09375, ((0, 8), (1, 4)))
    gate_weight = scatter_about(streams_of[5], (D, D_RNN), D ** -0.5, 0.09375, ((0, 8), (1, 4)))
    conv_weight = scatter_about(streams_of[6], (4, D_RNN), 0.5, 3.0, ((1, 4),))
    rate_weight = scatter_about(streams_of[7], (RG_BLOCKS, RG_BW, RG_BW), RG_BW ** -0.5, 0.375, ((0, 4),))
    input_weight = scatter_about(streams_of[8], (RG_BLOCKS, RG_BW, RG_BW), RG_BW ** -0.5, 0.375, ((0, 4),))
    rate_param = jnp.clip(1.0 + 5.0 * jax.random.uniform(streams_of[9], (D_RNN,), jnp.float32) ** shard_levels(streams_of[9], (D_RNN,), ((0, 4),), -0.2, 0.2), 1.0, 6.0)
    out_weight = scatter_about(streams_of[10], (D_RNN, D), D_RNN ** -0.5, 0.09375, ((0, 4),))
    moe_gain = jnp.clip(1.0 + 0.18 * jax.random.normal(streams_of[11], (D,), jnp.float32), 0.099609375, 1.8984375).astype(jnp.bfloat16)
    expert_gate = scatter_about(streams_of[12], (EXPERTS, D, FF_E), D ** -0.5, 0.09375, ((0, 8), (2, 4)))
    expert_up = scatter_about(streams_of[13], (EXPERTS, D, FF_E), D ** -0.5, 0.09375, ((0, 8), (2, 4)))
    expert_down = scatter_about(streams_of[14], (EXPERTS, FF_E, D), FF_E ** -0.5, 0.125, ((0, 8), (1, 4)))
    routes_keys = jax.random.split(jax.random.fold_in(streams_of[15], 1), BATCH // SEQ_GRP)
    routes_turns = jax.random.permutation(jax.random.fold_in(streams_of[15], 3), BATCH // SEQ_GRP)
    routes = jax.vmap(lambda own, number: assign_block(jax.random.fold_in(streams_of[15], 2), own, number, SEQ_GRP, EXPERTS, TOPK, CAP, 2))(routes_keys, routes_turns).reshape((BATCH, TOPK))
    route_prob = jnp.clip(0.1 + 0.9 * jax.random.uniform(streams_of[16], (BATCH, TOPK), jnp.float32) ** shard_levels(streams_of[16], (BATCH, TOPK), ((0, 8),), -0.2, 0.2), 0.1, 1.0)
    return dict(tokens=tokens, state_in=state_in, conv_in=conv_in, mix_gain=mix_gain, rnn_weight=rnn_weight, gate_weight=gate_weight, conv_weight=conv_weight, rate_weight=rate_weight, input_weight=input_weight, rate_param=rate_param, out_weight=out_weight, moe_gain=moe_gain, expert_gate=expert_gate, expert_up=expert_up, expert_down=expert_down, routes=routes, route_prob=route_prob)


def rms_scale(values, gain):
    scale = lax.rsqrt(lax.optimization_barrier(jnp.mean(values * values, axis=-1, keepdims=True)) + 1e-06)
    return values * scale * gain.astype(jnp.float32)

def slot_targets(route_ids, experts, capacity):
    flat_ids = route_ids.reshape(-1)
    onehot = (flat_ids[:, None] == jnp.arange(experts, dtype=jnp.int32)[None, :]).astype(jnp.int32)
    before = jnp.cumsum(onehot, axis=0) - onehot
    slot_ids = lax.optimization_barrier(jnp.sum(before * onehot, axis=1))
    return (flat_ids * capacity + slot_ids).astype(jnp.int32)

def block_map(conv, weight):
    rows = conv.shape[0]
    parts = conv.reshape(rows, RG_BLOCKS, RG_BW).astype(jnp.float32)
    mapped = jnp.einsum('snc,ncd->snd', parts, weight.astype(jnp.float32))
    return mapped.reshape(rows, D_RNN)

def run_expert(args):
    rows, w_gate, w_up, w_down = args
    rows32 = rows.astype(jnp.float32)
    gate_part = jnp.dot(rows32, w_gate.astype(jnp.float32))
    up_part = jnp.dot(rows32, w_up.astype(jnp.float32))
    hidden = (jax.nn.silu(gate_part) * up_part).astype(jnp.bfloat16)
    split_hidden = hidden.reshape(rows.shape[0], N_TP, FF_E // N_TP).astype(jnp.float32)
    split_down = w_down.reshape(N_TP, FF_E // N_TP, D).astype(jnp.float32)
    pieces = jnp.einsum('rtf,tfd->trd', split_hidden, split_down)
    rounded = lax.optimization_barrier(pieces.astype(jnp.bfloat16)).astype(jnp.float32)
    return lax.optimization_barrier(jnp.sum(rounded, axis=0)).astype(jnp.bfloat16)

def reference(tokens, state_in, conv_in, mix_gain, rnn_weight, gate_weight, conv_weight, rate_weight, input_weight, rate_param, out_weight, moe_gain, expert_gate, expert_up, expert_down, routes, route_prob):
    base = tokens.astype(jnp.float32)
    normed = rms_scale(base, mix_gain).astype(jnp.bfloat16)
    proj_x = jnp.dot(normed, rnn_weight, preferred_element_type=jnp.float32)
    proj_y = jnp.dot(normed, gate_weight, preferred_element_type=jnp.float32)
    moved = proj_x.astype(jnp.bfloat16)
    conv_out = jnp.concatenate([conv_in[:, 1:], moved[:, None, :]], axis=1)
    taps = conv_weight.astype(jnp.float32)
    history = conv_in.astype(jnp.float32)
    summed = history[:, 0] * taps[0] + history[:, 1] * taps[1] + history[:, 2] * taps[2] + moved.astype(jnp.float32) * taps[3]
    conv = summed.astype(jnp.bfloat16)
    rate = jax.nn.sigmoid(block_map(conv, rate_weight))
    in_gate = jax.nn.sigmoid(block_map(conv, input_weight))
    log_decay = -8.0 * rate * jax.nn.softplus(-rate_param)
    state_out = jnp.exp(log_decay) * state_in + jnp.sqrt(-jnp.expm1(2.0 * log_decay)) * in_gate * conv.astype(jnp.float32)
    gated = (state_out * jax.nn.gelu(proj_y, approximate=True)).astype(jnp.bfloat16)
    split_gated = gated.reshape(BATCH, N_TP, D_RNN // N_TP).astype(jnp.float32)
    split_out = out_weight.reshape(N_TP, D_RNN // N_TP, D).astype(jnp.float32)
    pieces = jnp.einsum('btc,tcd->tbd', split_gated, split_out)
    rounded = lax.optimization_barrier(pieces.astype(jnp.bfloat16)).astype(jnp.float32)
    mixed = base + lax.optimization_barrier(jnp.sum(rounded, axis=0))
    normed2 = rms_scale(mixed, moe_gain).astype(jnp.bfloat16)
    group_routes = routes.reshape(N_EP, SEQ_GRP * TOPK)
    targets = jax.vmap(lambda group_ids: slot_targets(group_ids, EXPERTS, CAP))(group_routes)
    dispatch = (jnp.arange(EXPERTS * CAP, dtype=jnp.int32)[None, :, None] == targets[:, None, :]).astype(jnp.float32)
    repeated = jnp.repeat(normed2, TOPK, axis=0).reshape(N_EP, SEQ_GRP * TOPK, D).astype(jnp.float32)
    send = jnp.einsum('grj,gjd->grd', dispatch, repeated).astype(jnp.bfloat16)
    by_expert = send.reshape(N_EP, EXPERTS, CAP, D).transpose(1, 0, 2, 3).reshape(EXPERTS, N_EP * CAP, D)
    outputs = lax.map(run_expert, (by_expert, expert_gate, expert_up, expert_down))
    back = outputs.reshape(EXPERTS, N_EP, CAP, D).transpose(1, 0, 2, 3).reshape(N_EP, EXPERTS * CAP, D).astype(jnp.float32)
    picked = jnp.einsum('grj,grd->gjd', dispatch, back).reshape(BATCH, TOPK, D)
    weights = route_prob / lax.optimization_barrier(jnp.sum(route_prob, axis=1, keepdims=True))
    experts_sum = lax.optimization_barrier(jnp.sum(picked * weights[:, :, None], axis=1))
    layer_out = (mixed + experts_sum).astype(jnp.bfloat16)
    return (layer_out, state_out, conv_out)
```

```python
import functools

import jax
import jax.numpy as jnp
from jax import lax
from jax.experimental import pallas as pl
from jax.experimental.pallas import tpu as pltpu
from jax.sharding import PartitionSpec as P

MESH = pl.DeviceIdType.MESH
F32 = jnp.float32
BF16 = jnp.bfloat16


def dot(a, b):
    return jnp.dot(a, b, preferred_element_type=F32)


def remote(src, dst, send, recv, where):
    return pltpu.make_async_remote_copy(
        src_ref=src, dst_ref=dst, send_sem=send, recv_sem=recv, device_id=where, device_id_type=MESH
    )


def kernel(
    n, p, nx, cap,
    tokens, state_in, conv_in, mix_gain_in, moe_gain_in, conv_w, rate_param, routes, prob,
    rnn_h, gate_h, rate_h, input_h, out_h, eg_h, eu_h, ed_h,
    layer_out, state_out, moved_out,
    wr, wg, wrate, winput, wout, weg, weu, wed,
    mix_gain, moe_gain, normed, cols, part, bx, zsend, rz, gated, oacc,
    op_p, op_o, op_r, hs, hr, mixed,
    sd, rows, xn, hid, e_p, e_o, e_r, es, er, outb, ret,
    wsem, sa, ra, sa2, ra2, sb, rb, sz, rzs, sd1, rd1, sd2, rd2, sc1, rc1, sc2, rc2, sc3, rc3,
    se1, re1, se2, re2, se3, re3,
):
    e = lax.axis_index("ep")
    t = lax.axis_index("tp")
    core = lax.rem(t, 2)
    y = t // 2
    q = t + 1 - 2 * core
    ys = p // 2
    nz = n // nx
    z = e // nx
    x = lax.rem(e, nx)
    far_first = sorted(range(nz), key=lambda dz: -min(dz, nz - dz))

    def up(d):
        return lax.rem(z + d // nx, nz) * nx + lax.rem(x + d % nx, nx)

    def down_of(d):
        return lax.rem(z - d // nx + nz, nz) * nx + lax.rem(x - d % nx + nx, nx)

    rows_g, width = tokens.shape
    depth = width // n
    chans = rnn_h.shape[1]
    share = width // p
    slots = n * cap

    loads = [
        pltpu.make_async_copy(a, b, wsem.at[i])
        for i, (a, b) in enumerate(
            [(rnn_h, wr), (gate_h, wg), (rate_h, wrate), (input_h, winput), (out_h, wout),
             (eg_h.at[0], weg), (eu_h.at[0], weu), (ed_h.at[0], wed)]
        )
    ]
    for load in loads[:4]:
        load.start()

    barrier = pltpu.get_barrier_semaphore()

    @pl.loop(1, n)
    def _(d):
        pl.semaphore_signal(barrier, inc=1, device_id={"ep": lax.rem(e + d, n)}, device_id_type=MESH)

    @pl.loop(1, p)
    def _(d):
        pl.semaphore_signal(barrier, inc=1, device_id={"tp": lax.rem(t + d, p)}, device_id_type=MESH)

    for j in range(width // 128):
        cs = slice(j * 128, (j + 1) * 128)
        mix_gain[:, cs] = mix_gain_in[j:j + 1, :].astype(F32)
        moe_gain[:, cs] = moe_gain_in[j:j + 1, :].astype(F32)

    ssq = jnp.zeros((rows_g, 1), F32)
    for j in range(n):
        v = tokens[:, j * depth:(j + 1) * depth].astype(F32)
        ssq = ssq + jnp.sum(v * v, axis=1, keepdims=True)
    scale = lax.rsqrt(ssq / width + 1e-06)
    for j in range(n):
        cs = slice(j * depth, (j + 1) * depth)
        normed[j] = (tokens[:, cs].astype(F32) * scale * mix_gain[:, cs]).astype(BF16)

    @pl.when(z == 0)
    def _():
        rz[0] = jnp.zeros(rz.shape[1:], BF16)

    @pl.when(z == nz - 1)
    def _():
        rz[1] = jnp.zeros(rz.shape[1:], BF16)

    pl.semaphore_wait(barrier, n + p - 2)


    half = pl.ds(pl.multiple_of(core * (rows_g // 2), rows_g // 2), rows_g // 2)
    nc, bw = rate_h.shape[0], rate_h.shape[1]
    high = (2 * z) // nz
    folded = z + high * (nz - 1 - 2 * z)

    def far(j):
        plane = nz - 1 - j
        plane = plane - (folded >= plane).astype(jnp.int32)
        return plane + high * (nz - 1 - 2 * plane)

    def beside(dx):
        return lax.rem(x + dx, nx)

    def copy_a(peer):
        return remote(normed.at[peer, half], cols.at[e, half], sa.at[peer], ra.at[e], {"ep": peer})

    def landed_a(src):
        return remote(normed.at[src, half], cols.at[src, half], sa.at[src], ra.at[src], {"ep": src})

    def copy_a2(src):
        return remote(cols.at[src, half], cols.at[src, half], sa2.at[src], ra2.at[src], {"tp": q})

    for dx in range(1, nx):
        copy_a(z * nx + beside(dx)).start()

    @pl.loop(0, nz - 1)
    def _(j):
        for dx in range(nx):
            copy_a(far(j) * nx + beside(dx)).start()

    cols[e] = normed[e]

    ids = routes[...]
    sub_e = lax.broadcasted_iota(jnp.int32, (n, rows_g), 0)
    named = [(ids[k:k + 1, :] == sub_e).astype(F32) for k in range(ids.shape[0])]
    member = functools.reduce(lambda a, b: a + b, named)
    earlier = (
        lax.broadcasted_iota(jnp.int32, (rows_g, rows_g), 0)
        < lax.broadcasted_iota(jnp.int32, (rows_g, rows_g), 1)
    ).astype(F32)
    before = dot(member.astype(BF16), earlier.astype(BF16))
    sub_s = lax.broadcasted_iota(jnp.int32, (slots, rows_g), 0).astype(F32)
    total_prob = jnp.sum(prob[...], axis=0, keepdims=True)
    dispatch = jnp.zeros((slots, rows_g), F32)
    comb = jnp.zeros((slots, rows_g), F32)
    for k in range(ids.shape[0]):
        slot = jnp.sum(before * named[k], axis=0, keepdims=True)
        target = ids[k:k + 1, :].astype(F32) * cap + slot
        hit = (sub_s == target).astype(F32)
        dispatch = dispatch + hit
        comb = comb + hit * (prob[k:k + 1, :] / total_prob)
    dispatch = dispatch.astype(BF16)
    comb_hi = comb.astype(BF16)
    comb_lo = (comb - comb_hi.astype(F32)).astype(BF16)

    loads[0].wait()
    loads[1].wait()
    for load in loads[4:]:
        load.start()

    def copy_x(plane, dx, c):
        return remote(
            part.at[plane, dx, c], bx.at[plane, dx, c], sb.at[plane, dx, c], rb.at[plane, dx, c],
            {"ep": z * nx + beside(dx)},
        )

    def project(plane, first, last, own):
        skip = 1 if own else 0
        for dx in range(skip, nx):
            src = plane * nx + beside(dx)
            landed_a(src).wait_recv()
            copy_a2(src).start()
        for dx in list(range(1, nx)) + [0]:
            src = plane * nx + beside(dx)
            if dx >= skip:
                copy_a2(src).wait_recv()
            for c in range(nc):
                cs = slice(c * bw, (c + 1) * bw)
                part[plane, dx, c, :, :bw] = dot(cols[src], wr[:, cs]).astype(BF16)
                part[plane, dx, c, :, bw:] = dot(cols[src], wg[:, cs]).astype(BF16)
                if dx and first <= c < last:
                    copy_x(plane, dx, c).start()

    project(z, 0, nc // 2, True)

    @pl.loop(0, nz - 1)
    def _(j):
        project(far(j), 0, nc, False)

    for c in range(nc // 2, nc):
        for dx in range(1, nx):
            copy_x(z, dx, c).start()

    def copy_z(side, plane, c):
        to = z + 1 - 2 * side
        return remote(
            zsend.at[plane, c], rz.at[side, plane, c], sz.at[plane, c], rzs.at[side, plane, c],
            {"ep": to * nx + x},
        )

    def summed(side, plane, c):
        for dx in range(1, nx):
            copy_x(plane, dx, c).wait_recv()
        total = part[plane, 0, c].astype(F32)
        for dx in range(1, nx):
            total = total + bx[plane, dx, c].astype(F32)
        for s in side:
            origin = z - 1 + 2 * s

            @pl.when((origin >= 0) & (origin < nz))
            def _():
                copy_z(s, plane, c).wait_recv()

            total = total + rz[s, plane, c].astype(F32)
        return total

    @pl.loop(0, nz - 1)
    def _(j):
        plane = far(j)
        side = (plane < z).astype(jnp.int32)
        for c in range(nc):
            zsend[plane, c] = summed([side], plane, c).astype(BF16)
            copy_z(side, plane, c).start()

    def block(i):
        return pl.ds(pl.multiple_of(i * share, share), share)

    loads[2].wait()
    loads[3].wait()
    loads[4].wait()
    for c in range(nc):
        cs = slice(c * bw, (c + 1) * bw)
        proj = summed([0, 1], z, c)
        moved = proj[:, :bw].astype(BF16)
        moved_out[:, cs] = moved
        taps = conv_w[:, cs].astype(F32)
        hist = conv_in[0, :, cs].astype(F32) * taps[0:1]
        for i in range(1, 3):
            hist = hist + conv_in[i, :, cs].astype(F32) * taps[i:i + 1]
        conv = (hist + moved.astype(F32) * taps[3:4]).astype(BF16)
        rate = jax.nn.sigmoid(dot(conv, wrate[c]))
        in_gate = jax.nn.sigmoid(dot(conv, winput[c]))
        log_decay = -8.0 * rate * jnp.log1p(jnp.exp(-rate_param[:, cs]))
        th = jnp.tanh(log_decay)
        rest = -2.0 * th / (1.0 - th)
        state = jnp.exp(log_decay) * state_in[:, cs] + jnp.sqrt(rest) * in_gate * conv.astype(F32)
        state_out[:, cs] = state
        gated[:, cs] = (state * jax.nn.gelu(proj[:, bw:], approximate=True)).astype(BF16)
        if c < nc - 1:
            for i in range(p):
                os = slice(i * share, (i + 1) * share)
                piece = dot(gated[:, cs], wout[cs, os])
                oacc[i] = piece if c == 0 else oacc[i] + piece

    last = slice((nc - 1) * bw, nc * bw)

    def out_part(i):
        piece = dot(gated[:, last], wout[last, block(i)])
        return oacc[i] + piece if nc > 1 else piece

    def copy_d1(yy):
        return remote(op_p.at[yy], op_r.at[yy], sd1.at[yy], rd1.at[yy], {"tp": q})

    def copy_d2(dy):
        ty = lax.rem(y + dy, ys)
        return remote(hs.at[ty], hr.at[y], sd2.at[dy], rd2.at[dy], {"tp": ty * 2 + core})

    for dy in range(ys):
        yy = lax.rem(y + dy + 1, ys)
        op_p[yy] = out_part(yy * 2 + 1 - core).astype(BF16)
        copy_d1(yy).start()
    for dy in range(ys):
        yy = lax.rem(y + dy + 1, ys)
        op_o[yy] = out_part(yy * 2 + core)
    for dy in range(1, ys):
        ty = lax.rem(y + dy, ys)
        copy_d1(ty).wait_recv()
        hs[ty] = (op_o[ty] + op_r[ty].astype(F32)).astype(BF16)
        copy_d2(dy).start()
    copy_d1(y).wait_recv()
    total = tokens[:, block(t)].astype(F32) + op_o[y] + op_r[y].astype(F32)
    for dy in range(1, ys):
        copy_d2(dy).wait_recv()
        total = total + hr[lax.rem(y - dy + ys, ys)].astype(F32)
    mixed[...] = total

    sent = dot(dispatch, mixed[...].astype(BF16))
    sd[...] = sent.reshape(n, cap, share).astype(BF16)

    def copy_c1(d):
        peer = up(d)
        return remote(sd.at[peer], rows.at[t, e], sc1.at[d], rc1.at[d], {"ep": peer})

    def copy_c2(dy, d):
        src = down_of(d)
        to = lax.rem(y + dy, ys) * 2 + core
        return remote(rows.at[t, src], rows.at[t, src], sc2.at[dy, d], rc2.at[dy, d], {"tp": to})

    def copy_c3(dy, d):
        src = down_of(d)
        held = lax.rem(y - dy + ys, ys) * 2 + core
        return remote(rows.at[held, src], rows.at[held, src], sc3.at[dy, d], rc3.at[dy, d], {"tp": q})

    order = [dz * nx + dx for dz in far_first for dx in range(nx) if dz + dx]
    for d in order:
        copy_c1(d).start()

    rows[t, e] = sd[e]

    def spread(d):
        for dy in range(1, ys):
            copy_c2(dy, d).start()
        copy_c3(0, d).start()

    def relay(d):
        for dy in range(1, ys):
            copy_c2(dy, d).wait_recv()
            copy_c3(dy, d).start()

    near = order[::-1]
    spread(0)
    for i, d in enumerate(near):
        copy_c1(d).wait_recv()
        spread(d)
        if i >= 1:
            relay(([0] + near)[i - 1])
    for d in ([0] + near)[len(near) - 1:]:
        relay(d)
    for d in range(n):
        for dy in range(ys):
            copy_c3(dy, d).wait_recv()

    gs = min(n, max(1, 64 // cap))
    span = gs * cap

    @pl.loop(0, n // gs)
    def _(g):
        def piece(i):
            return rows[i, pl.ds(g * gs, gs)].astype(F32).reshape(span, share)

        acc = jnp.zeros((span, 1), F32)
        for i in range(p):
            v = piece(i)
            acc = acc + jnp.sum(v * v, axis=1, keepdims=True)
        sc = lax.rsqrt(acc / width + 1e-06)
        for i in range(p):
            cs = slice(i * share, (i + 1) * share)
            xn[pl.ds(pl.multiple_of(g * span, span), span), cs] = (
                piece(i) * sc * moe_gain[:, cs]
            ).astype(BF16)

    loads[5].wait()
    loads[6].wait()
    hidden = hid.shape[1]
    fc = min(256, hidden)

    @pl.loop(0, hidden // fc)
    def _(c):
        cs = pl.ds(pl.multiple_of(c * fc, fc), fc)
        gate_part = dot(xn[...], weg[:, cs])
        up_part = dot(xn[...], weu[:, cs])
        hid[:, cs] = (jax.nn.silu(gate_part) * up_part).astype(BF16)

    loads[7].wait()

    def copy_e1(yy):
        return remote(e_p.at[yy], e_r.at[yy], se1.at[yy], re1.at[yy], {"tp": q})

    def copy_e2(dy, dz):
        ty = lax.rem(y + dy, ys)
        zc = lax.rem(z + dz, nz)
        return remote(
            es.at[ty, zc], er.at[y, zc], se2.at[dy, dz], re2.at[dy, dz], {"tp": ty * 2 + core}
        )

    def copy_e3(d):
        peer = up(d)
        return remote(outb.at[peer], ret.at[e], se3.at[d], re3.at[d], {"ep": peer})

    tile = min(256, share)
    chunk = nx * cap

    def down(yy, parity, dst):
        @pl.loop(0, share // tile)
        def _(c):
            at = pl.ds(pl.multiple_of((yy * 2 + parity) * share + c * tile, tile), tile)
            value = dot(hid[...], wed[:, at]).reshape(nz, chunk, tile)
            dst[yy, :, :, pl.ds(pl.multiple_of(c * tile, tile), tile)] = value.astype(dst.dtype)

    for dy in list(range(1, ys)) + [0]:
        ty = lax.rem(y + dy, ys)
        down(ty, 1 - core, e_p)
        copy_e1(ty).start()
        down(ty, core, e_o)
        copy_e1(ty).wait_recv()
        if dy:
            for dz in far_first:
                zc = lax.rem(z + dz, nz)
                es[ty, zc] = (e_o[ty, zc] + e_r[ty, zc].astype(F32)).astype(BF16)
                copy_e2(dy, dz).start()
    for dz in far_first:
        zc = lax.rem(z + dz, nz)
        result = e_o[y, zc] + e_r[y, zc].astype(F32)
        for dy in range(1, ys):
            copy_e2(dy, dz).wait_recv()
            result = result + er[lax.rem(y - dy + ys, ys), zc].astype(F32)
        outb[pl.ds(zc * nx, nx)] = result.reshape(nx, cap, share).astype(BF16)
        for dx in range(nx):
            if dz + dx:
                copy_e3(dz * nx + dx).start()

    ret[e] = outb[e]
    for d in order:
        copy_e3(d).wait_recv()

    back = ret[...].astype(F32).reshape(slots, share).astype(BF16)

    def combine(weights):
        return lax.dot_general(weights, back, (((0,), (0,)), ((), ())), preferred_element_type=F32)

    layer_out[...] = (mixed[...] + combine(comb_hi) + combine(comb_lo)).astype(BF16)

    @pl.loop(1, n)
    def _(d):
        copy_a(up(d)).wait_send()
        copy_a2(up(d)).wait_send()
        copy_c1(d).wait_send()
        copy_e3(d).wait_send()

    @pl.loop(0, n)
    def _(d):
        for dy in range(1, ys):
            copy_c2(dy, d).wait_send()
        for dy in range(ys):
            copy_c3(dy, d).wait_send()

    for dy in range(ys):
        copy_d1(dy).wait_send()
        copy_e1(dy).wait_send()
    for dy in range(1, ys):
        copy_d2(dy).wait_send()
        for dz in range(nz):
            copy_e2(dy, dz).wait_send()
    @pl.loop(0, nz)
    def _(plane):
        for c in range(nc):
            for dx in range(1, nx):
                copy_x(plane, dx, c).wait_send()

    @pl.loop(0, nz - 1)
    def _(j):
        plane = far(j)
        for c in range(nc):
            copy_z((plane < z).astype(jnp.int32), plane, c).wait_send()


def finish(layer_in, state_in, moved, conv_in, layer_out, state_out, conv_out):
    layer_out[...] = layer_in[...]
    state_out[...] = state_in[...]
    kept = conv_in.shape[0] - 1
    for i in range(kept):
        conv_out[i] = conv_in[i + 1]
    conv_out[kept] = moved[...]


def shards(
    n, p,
    tokens, state_in, conv_in, mix_gain, rnn_weight, gate_weight, conv_weight, rate_weight,
    input_weight, rate_param, out_weight, moe_gain, expert_gate, expert_up, expert_down, routes, route_prob,
):
    g, width = tokens.shape
    depth, chans = rnn_weight.shape
    share = width // p
    cap = max(2, 2 * g * routes.shape[1] // n)
    slots = n * cap
    hidden = expert_gate.shape[2]
    ys = p // 2
    nx = 1 << ((n.bit_length() - 1) // 2)
    nx = nx if n % nx == 0 else 1
    nz = n // nx
    nc, cw = rate_weight.shape[0], 2 * rate_weight.shape[1]
    conv_t = jnp.transpose(conv_in, (1, 0, 2))
    vm = pl.BlockSpec(memory_space=pltpu.VMEM)
    hb = pl.BlockSpec(memory_space=pl.ANY)
    dma = pltpu.SemaphoreType.DMA
    V = pltpu.VMEM
    scratch = [
        V((depth, chans), BF16), V((depth, chans), BF16),
        V(rate_weight.shape, BF16), V(input_weight.shape, BF16), V(out_weight.shape, BF16),
        V(expert_gate.shape[1:], BF16), V(expert_up.shape[1:], BF16), V(expert_down.shape[1:], BF16),
        V((1, width), F32), V((1, width), F32),
        V((n, g, depth), BF16), V((n, g, depth), BF16),
        V((nz, nx, nc, g, cw), BF16), V((nz, nx, nc, g, cw), BF16),
        V((nz, nc, g, cw), BF16), V((2, nz, nc, g, cw), BF16),
        V((g, chans), BF16), V((p, g, share), F32),
        V((ys, g, share), BF16), V((ys, g, share), F32), V((ys, g, share), BF16),
        V((ys, g, share), BF16), V((ys, g, share), BF16), V((g, share), F32),
        V((n, cap, share), BF16), V((p, n, cap, share), BF16), V((slots, width), BF16), V((slots, hidden), BF16),
        V((ys, nz, nx * cap, share), BF16), V((ys, nz, nx * cap, share), F32), V((ys, nz, nx * cap, share), BF16),
        V((ys, nz, nx * cap, share), BF16), V((ys, nz, nx * cap, share), BF16),
        V((n, cap, share), BF16), V((n, cap, share), BF16),
        dma((8,)),
        dma((n,)), dma((n,)), dma((n,)), dma((n,)), dma((nz, nx, nc)), dma((nz, nx, nc)), dma((nz, nc)), dma((2, nz, nc)),
        dma((ys,)), dma((ys,)), dma((ys,)), dma((ys,)),
        dma((n,)), dma((n,)), dma((ys, n)), dma((ys, n)), dma((ys, n)), dma((ys, n)),
        dma((ys,)), dma((ys,)), dma((ys, nz)), dma((ys, nz)), dma((n,)), dma((n,)),
    ]
    layer, state, moved = pl.pallas_call(
        functools.partial(kernel, n, p, nx, cap),
        out_shape=(
            jax.ShapeDtypeStruct((g, share), BF16),
            jax.ShapeDtypeStruct((g, chans), F32),
            jax.ShapeDtypeStruct((g, chans), BF16),
        ),
        in_specs=[vm] * 9 + [hb] * 8,
        out_specs=(vm, vm, vm),
        scratch_shapes=scratch,
        compiler_params=pltpu.CompilerParams(
            collective_id=0, has_side_effects=True, vmem_limit_bytes=60 * 1024 * 1024
        ),
    )(
        tokens, state_in, conv_t, mix_gain.reshape(-1, 128), moe_gain.reshape(-1, 128),
        conv_weight, rate_param[None], routes.T, route_prob.T,
        rnn_weight, gate_weight, rate_weight, input_weight, out_weight, expert_gate, expert_up, expert_down,
    )
    layer_out, state_out, conv_out = pl.pallas_call(
        finish,
        out_shape=(
            jax.ShapeDtypeStruct(layer.shape, layer.dtype),
            jax.ShapeDtypeStruct(state.shape, state.dtype),
            jax.ShapeDtypeStruct(conv_t.shape, conv_t.dtype),
        ),
        in_specs=[vm] * 4,
        out_specs=(vm, vm, vm),
    )(layer, state, moved, conv_t)
    return (layer_out, state_out, jnp.transpose(conv_out, (1, 0, 2)))


def solution(mesh):
    in_specs = (
        P("ep", None),
        P("ep", "tp"),
        P("ep", None, "tp"),
        P(),
        P("ep", "tp"),
        P("ep", "tp"),
        P(None, "tp"),
        P("tp", None, None),
        P("tp", None, None),
        P("tp"),
        P("tp", None),
        P(),
        P("ep", None, "tp"),
        P("ep", None, "tp"),
        P("ep", "tp", None),
        P("ep", None),
        P("ep", None),
    )
    out_specs = (P("ep", "tp"), P("ep", "tp"), P("ep", None, "tp"))
    body = functools.partial(shards, mesh.shape["ep"], mesh.shape["tp"])
    return jax.shard_map(body, mesh=mesh, in_specs=in_specs, out_specs=out_specs, check_vma=False)
```

```python
import functools

import jax
import jax.numpy as jnp
from jax import lax
from jax.experimental import pallas as pl
from jax.experimental.pallas import tpu as pltpu
from jax.sharding import PartitionSpec as P

MESH = pl.DeviceIdType.MESH
F32 = jnp.float32
BF16 = jnp.bfloat16
HALVES = 2
LAG = 3


def dot(a, b):
    return jnp.dot(a, b, preferred_element_type=F32)


def remote(src, dst, send, recv, where):
    return pltpu.make_async_remote_copy(
        src_ref=src, dst_ref=dst, send_sem=send, recv_sem=recv, device_id=where, device_id_type=MESH
    )


def kernel(
    n, p, nx, cap,
    tokens_h, state_h, conv_h, mix_h, moe_h, taps_h, param_h, routes_h, prob_h,
    rnn_h, gate_h, rate_h, input_h, out_h, eg_h, eu_h, ed_h,
    layer_out, state_out, conv_out,
    tokens, state_in, conv_in, mix_gain_in, moe_gain_in, conv_w, rate_param, routes, prob,
    layer_v, state_v, conv_v,
    wr, wg, wrate, winput, wout, weg, weu, wed,
    mix_gain, moe_gain, normed, cols, part, bx, zsend, rz, gated, oacc,
    op_p, op_o, op_r, hs, hr, mixed,
    sd, rows, xn, ssq, gacc, hid, e_p, e_o, e_r, es, er, outb, ret,
    wsem, lsem, osem, sa, ra, sa2, ra2, sb, rb, sz, rzs, sd1, rd1, sd2, rd2,
    sc1, rc1, sc2, rc2, sc3, rc3, se1, re1, se2, re2, se3, re3,
):
    e = lax.axis_index("ep")
    t = lax.axis_index("tp")
    core = lax.rem(t, 2)
    y = t // 2
    q = t + 1 - 2 * core
    ys = p // 2
    nz = n // nx
    z = e // nx
    x = lax.rem(e, nx)

    rows_g, width = tokens.shape
    depth = width // n
    share = width // p
    sw = share // HALVES
    slots = n * cap

    small = [
        pltpu.make_async_copy(a, b, lsem.at[i])
        for i, (a, b) in enumerate(
            [(tokens_h, tokens), (mix_h, mix_gain_in), (moe_h, moe_gain_in), (routes_h, routes), (prob_h, prob),
             (taps_h, conv_w), (param_h, rate_param), (conv_h, conv_in), (state_h, state_in)]
        )
    ]
    loads = [
        pltpu.make_async_copy(a, b, wsem.at[i])
        for i, (a, b) in enumerate(
            [(rnn_h, wr), (gate_h, wg), (rate_h, wrate), (input_h, winput), (out_h, wout),
             (eg_h.at[0], weg), (eu_h.at[0], weu), (ed_h.at[0], wed)]
        )
    ]
    small[0].start()
    small[1].start()

    barrier = pltpu.get_barrier_semaphore()

    @pl.loop(1, n)
    def _(d):
        pl.semaphore_signal(barrier, inc=1, device_id={"ep": lax.rem(e + d, n)}, device_id_type=MESH)

    @pl.loop(1, p)
    def _(d):
        pl.semaphore_signal(barrier, inc=1, device_id={"tp": lax.rem(t + d, p)}, device_id_type=MESH)

    for load in small[2:] + loads[:4]:
        load.start()

    @pl.when(z == 0)
    def _():
        rz[0] = jnp.zeros(rz.shape[1:], BF16)

    @pl.when(z == nz - 1)
    def _():
        rz[1] = jnp.zeros(rz.shape[1:], BF16)

    small[0].wait()
    small[1].wait()
    for j in range(width // 128):
        cs = slice(j * 128, (j + 1) * 128)
        mix_gain[:, cs] = mix_gain_in[j:j + 1, :].astype(F32)

    total_sq = jnp.zeros((rows_g, 1), F32)
    for j in range(n):
        v = tokens[:, j * depth:(j + 1) * depth].astype(F32)
        total_sq = total_sq + jnp.sum(v * v, axis=1, keepdims=True)
    scale = lax.rsqrt(total_sq / width + 1e-06)
    for j in range(n):
        cs = slice(j * depth, (j + 1) * depth)
        normed[j] = (tokens[:, cs].astype(F32) * scale * mix_gain[:, cs]).astype(BF16)

    pl.semaphore_wait(barrier, n + p - 2)

    half = pl.ds(pl.multiple_of(core * (rows_g // 2), rows_g // 2), rows_g // 2)
    nc, bw = rate_h.shape[0], rate_h.shape[1]
    high = (2 * z) // nz
    folded = z + high * (nz - 1 - 2 * z)

    def far(j):
        plane = nz - 1 - j
        plane = plane - (folded >= plane).astype(jnp.int32)
        return plane + high * (nz - 1 - 2 * plane)

    def beside(dx):
        return lax.rem(x + dx, nx)

    def peer_of(plane, dx):
        return plane * nx + beside(dx)

    def copy_a(peer):
        return remote(normed.at[peer, half], cols.at[e, half], sa.at[peer], ra.at[e], {"ep": peer})

    def landed_a(src):
        return remote(normed.at[src, half], cols.at[src, half], sa.at[src], ra.at[src], {"ep": src})

    def copy_a2(src):
        return remote(cols.at[src, half], cols.at[src, half], sa2.at[src], ra2.at[src], {"tp": q})

    for dx in range(1, nx):
        copy_a(peer_of(z, dx)).start()

    @pl.loop(0, nz - 1)
    def _(j):
        for dx in range(nx):
            copy_a(peer_of(far(j), dx)).start()

    cols[e] = normed[e]

    for j in range(2, 5):
        small[j].wait()
    for j in range(width // 128):
        cs = slice(j * 128, (j + 1) * 128)
        moe_gain[:, cs] = moe_gain_in[j:j + 1, :].astype(F32)
    ids = routes[...]
    sub_e = lax.broadcasted_iota(jnp.int32, (n, rows_g), 0)
    named = [(ids[k:k + 1, :] == sub_e).astype(F32) for k in range(ids.shape[0])]
    member = functools.reduce(lambda a, b: a + b, named)
    earlier = (
        lax.broadcasted_iota(jnp.int32, (rows_g, rows_g), 0)
        < lax.broadcasted_iota(jnp.int32, (rows_g, rows_g), 1)
    ).astype(F32)
    before = dot(member.astype(BF16), earlier.astype(BF16))
    sub_s = lax.broadcasted_iota(jnp.int32, (slots, rows_g), 0).astype(F32)
    total_prob = jnp.sum(prob[...], axis=0, keepdims=True)
    dispatch = jnp.zeros((slots, rows_g), F32)
    comb = jnp.zeros((slots, rows_g), F32)
    for k in range(ids.shape[0]):
        slot = jnp.sum(before * named[k], axis=0, keepdims=True)
        target = ids[k:k + 1, :].astype(F32) * cap + slot
        hit = (sub_s == target).astype(F32)
        dispatch = dispatch + hit
        comb = comb + hit * (prob[k:k + 1, :] / total_prob)
    dispatch = dispatch.astype(BF16)
    comb_hi = comb.astype(BF16)
    comb_lo = (comb - comb_hi.astype(F32)).astype(BF16)

    loads[0].wait()
    loads[1].wait()
    for load in loads[4:]:
        load.start()

    def copy_x(plane, dx, c):
        return remote(
            part.at[plane, beside(dx), c], bx.at[plane, dx, c], sb.at[plane, dx, c], rb.at[plane, dx, c],
            {"ep": peer_of(z, dx)},
        )

    def project(plane, last, own):
        first = 1 if own else 0
        for dx in range(first, nx):
            src = peer_of(plane, dx)
            landed_a(src).wait_recv()
            copy_a2(src).start()
        for dx in range(first, nx):
            copy_a2(peer_of(plane, dx)).wait_recv()
        feats = cols[pl.ds(plane * nx, nx)].reshape(nx * rows_g, depth)
        for c in range(nc):
            cs = slice(c * bw, (c + 1) * bw)
            for lo, weight in ((0, wr), (bw, wg)):
                value = dot(feats, weight[:, cs]).astype(BF16)
                for i in range(nx):
                    part[plane, i, c, :, lo:lo + bw] = value[i * rows_g:(i + 1) * rows_g]
            if c < last:
                for dx in range(1, nx):
                    copy_x(plane, dx, c).start()

    project(z, nc // 2, True)

    @pl.loop(0, nz - 1)
    def _(j):
        project(far(j), nc, False)

    for c in range(nc // 2, nc):
        for dx in range(1, nx):
            copy_x(z, dx, c).start()

    def copy_z(side, plane, c):
        to = z + 1 - 2 * side
        return remote(
            zsend.at[plane, c], rz.at[side, plane, c], sz.at[plane, c], rzs.at[side, plane, c],
            {"ep": to * nx + x},
        )

    def summed(sides, plane, c):
        for dx in range(1, nx):
            copy_x(plane, dx, c).wait_recv()
        total = part[plane, x, c].astype(F32)
        for dx in range(1, nx):
            total = total + bx[plane, dx, c].astype(F32)
        for s in sides:
            origin = z - 1 + 2 * s

            @pl.when((origin >= 0) & (origin < nz))
            def _():
                copy_z(s, plane, c).wait_recv()

            total = total + rz[s, plane, c].astype(F32)
        return total

    @pl.loop(0, nz - 1)
    def _(j):
        plane = far(j)
        side = (plane < z).astype(jnp.int32)
        for c in range(nc):
            zsend[plane, c] = summed([side], plane, c).astype(BF16)
            copy_z(side, plane, c).start()

    def block(i, h):
        return pl.ds(pl.multiple_of(i * share + h * sw, sw), sw)

    for load in small[5:]:
        load.wait()
    loads[2].wait()
    loads[3].wait()
    loads[4].wait()
    for i in range(1, conv_in.shape[0]):
        conv_v[i - 1] = conv_in[i]
    for c in range(nc):
        cs = slice(c * bw, (c + 1) * bw)
        proj = summed([0, 1], z, c)
        moved = proj[:, :bw].astype(BF16)
        conv_v[conv_in.shape[0] - 1, :, cs] = moved
        taps = conv_w[:, cs].astype(F32)
        hist = conv_in[0, :, cs].astype(F32) * taps[0:1]
        for i in range(1, 3):
            hist = hist + conv_in[i, :, cs].astype(F32) * taps[i:i + 1]
        conv = (hist + moved.astype(F32) * taps[3:4]).astype(BF16)
        rate = jax.nn.sigmoid(dot(conv, wrate[c]))
        in_gate = jax.nn.sigmoid(dot(conv, winput[c]))
        log_decay = -8.0 * rate * jnp.log1p(jnp.exp(-rate_param[:, cs]))
        th = jnp.tanh(log_decay)
        rest = -2.0 * th / (1.0 - th)
        state = jnp.exp(log_decay) * state_in[:, cs] + jnp.sqrt(rest) * in_gate * conv.astype(F32)
        state_v[:, cs] = state
        gated[:, cs] = (state * jax.nn.gelu(proj[:, bw:], approximate=True)).astype(BF16)
        if c < nc - 1:
            for i in range(p):
                for h in range(HALVES):
                    lo = i * share + h * sw
                    piece = dot(gated[:, cs], wout[cs, lo:lo + sw])
                    oacc[i, h] = piece if c == 0 else oacc[i, h] + piece

    last = slice((nc - 1) * bw, nc * bw)

    def out_part(i, h):
        piece = dot(gated[:, last], wout[last, block(i, h)])
        return oacc[i, h] + piece if nc > 1 else piece

    def copy_d1(yy, h):
        return remote(op_p.at[yy, h], op_r.at[yy, h], sd1.at[yy, h], rd1.at[yy, h], {"tp": q})

    def copy_d2(dy, h):
        ty = lax.rem(y + dy, ys)
        return remote(hs.at[ty, h], hr.at[y, h], sd2.at[dy, h], rd2.at[dy, h], {"tp": ty * 2 + core})

    for dy in range(ys):
        yy = lax.rem(y + dy + 1, ys)
        for h in range(HALVES):
            op_p[yy, h] = out_part(yy * 2 + 1 - core, h).astype(BF16)
            copy_d1(yy, h).start()
    for dy in range(ys):
        yy = lax.rem(y + dy + 1, ys)
        for h in range(HALVES):
            op_o[yy, h] = out_part(yy * 2 + core, h)
    for h in range(HALVES):
        for dy in range(1, ys):
            ty = lax.rem(y + dy, ys)
            copy_d1(ty, h).wait_recv()
            hs[ty, h] = (op_o[ty, h] + op_r[ty, h].astype(F32)).astype(BF16)
            copy_d2(dy, h).start()

    puts = [
        pltpu.make_async_copy(a, b, osem.at[i])
        for i, (a, b) in enumerate([(state_v, state_out), (conv_v, conv_out), (layer_v, layer_out)])
    ]
    puts[0].start()
    puts[1].start()

    def copy_c1(peer, h):
        return remote(sd.at[peer, h], rows.at[t, e, h], sc1.at[peer, h], rc1.at[e, h], {"ep": peer})

    def landed_c1(src, h):
        return remote(sd.at[src, h], rows.at[t, src, h], sc1.at[src, h], rc1.at[src, h], {"ep": src})

    def copy_c2(dy, src, h):
        to = lax.rem(y + dy, ys) * 2 + core
        return remote(rows.at[t, src, h], rows.at[t, src, h], sc2.at[dy, src, h], rc2.at[dy, src, h], {"tp": to})

    def landed_c2(dy, src, h):
        held = lax.rem(y - dy + ys, ys) * 2 + core
        return remote(
            rows.at[held, src, h], rows.at[held, src, h], sc2.at[dy, src, h], rc2.at[dy, src, h], {"tp": held}
        )

    def copy_c3(dy, src, h):
        held = lax.rem(y - dy + ys, ys) * 2 + core
        return remote(
            rows.at[held, src, h], rows.at[held, src, h], sc3.at[dy, src, h], rc3.at[dy, src, h], {"tp": q}
        )

    def landed_c3(dy, src, h):
        held = lax.rem(y - dy + ys, ys) * 2 + 1 - core
        return remote(
            rows.at[held, src, h], rows.at[held, src, h], sc3.at[dy, src, h], rc3.at[dy, src, h], {"tp": q}
        )

    for h in range(HALVES):
        copy_d1(y, h).wait_recv()
        total = tokens[:, block(t, h)].astype(F32) + op_o[y, h] + op_r[y, h].astype(F32)
        for dy in range(1, ys):
            copy_d2(dy, h).wait_recv()
            total = total + hr[lax.rem(y - dy + ys, ys), h].astype(F32)
        mixed[h] = total
        sent = dot(dispatch, total.astype(BF16)).reshape(n, cap, sw).astype(BF16)
        for i in range(n):
            sd[i, h] = sent[i]
        for dx in range(1, nx):
            copy_c1(peer_of(z, dx), h).start()

        @pl.loop(0, nz - 1)
        def _(j):
            for dx in range(nx):
                copy_c1(peer_of(far(j), dx), h).start()

        rows[t, e, h] = sd[e, h]
        for dy in range(1, ys):
            copy_c2(dy, e, h).start()
        copy_c3(0, e, h).start()

    gs = min(n, max(1, 64 // cap))
    span = gs * cap
    hidden = hid.shape[1]
    fc = min(256, hidden)

    def scaled_rows(h):
        @pl.loop(0, n)
        def _(src):
            for dy in range(ys):
                landed_c3(dy, src, h).wait_recv()

        @pl.loop(0, n // gs)
        def _(g):
            at = pl.ds(pl.multiple_of(g * span, span), span)
            acc = jnp.zeros((span, 1), F32)
            for i in range(p):
                lo = i * share + h * sw
                v = rows[i, pl.ds(g * gs, gs), h].astype(F32).reshape(span, sw)
                acc = acc + jnp.sum(v * v, axis=1, keepdims=True)
                xn[h, at, i * sw:(i + 1) * sw] = (v * moe_gain[:, lo:lo + sw]).astype(BF16)
            ssq[at, :] = acc if h == 0 else ssq[at, :] + acc

    def partial_dot(weight, h, cs):
        acc = None
        for i in range(p):
            lo = i * share + h * sw
            piece = dot(xn[h, :, i * sw:(i + 1) * sw], weight[lo:lo + sw, cs])
            acc = piece if acc is None else acc + piece
        return acc

    def early(k, weight, f):
        cs = slice(f * fc, (f + 1) * fc)
        gacc[k, :, cs] = partial_dot(weight, 0, cs)

    def first_half():
        loads[5].wait()
        loads[6].wait()
        scaled_rows(0)

    tasks = [first_half]
    for f in range(hidden // fc):
        tasks.append(functools.partial(early, 0, weg, f))
        tasks.append(functools.partial(early, 1, weu, f))

    near = [(z, dx) for dx in range(1, nx)]
    near = near + [(far(j), dx) for j in reversed(range(nz - 1)) for dx in range(nx)]
    steps = [(peer_of(plane, dx), h) for h in range(HALVES) for plane, dx in near]
    queue = [(e, h) for h in range(HALVES)]
    begin = len(near) + len(near) // 2
    for i, (src, h) in enumerate(steps):
        landed_c1(src, h).wait_recv()
        for dy in range(1, ys):
            copy_c2(dy, src, h).start()
        copy_c3(0, src, h).start()
        queue.append((src, h))
        if len(queue) > LAG:
            was, wh = queue.pop(0)
            for dy in range(1, ys):
                landed_c2(dy, was, wh).wait_recv()
                copy_c3(dy, was, wh).start()
        if i >= begin and tasks:
            tasks.pop(0)()
    for was, wh in queue:
        for dy in range(1, ys):
            landed_c2(dy, was, wh).wait_recv()
            copy_c3(dy, was, wh).start()
    for task in tasks:
        task()

    scaled_rows(HALVES - 1)
    row_scale = lax.rsqrt(ssq[...] / width + 1e-06)
    for f in range(hidden // fc):
        cs = slice(f * fc, (f + 1) * fc)
        gate_part = (gacc[0, :, cs] + partial_dot(weg, 1, cs)) * row_scale
        up_part = (gacc[1, :, cs] + partial_dot(weu, 1, cs)) * row_scale
        hid[:, cs] = (jax.nn.silu(gate_part) * up_part).astype(BF16)

    loads[7].wait()
    chunk = nx * cap

    def copy_e1(plane, yy):
        return remote(e_p.at[plane, yy], e_r.at[plane, yy], se1.at[plane, yy], re1.at[plane, yy], {"tp": q})

    def copy_e2(plane, dy, h):
        ty = lax.rem(y + dy, ys)
        return remote(
            es.at[plane, ty, h], er.at[plane, y, h], se2.at[plane, dy, h], re2.at[plane, dy, h],
            {"tp": ty * 2 + core},
        )

    def copy_e3(peer, h):
        return remote(outb.at[peer, h], ret.at[e, h], se3.at[peer, h], re3.at[e, h], {"ep": peer})

    def landed_e3(src, h):
        return remote(outb.at[src, h], ret.at[src, h], se3.at[src, h], re3.at[src, h], {"ep": src})

    def issue(plane):
        mine = hid[pl.ds(pl.multiple_of(plane * chunk, chunk), chunk), :]
        for dy in list(range(1, ys)) + [0]:
            ty = lax.rem(y + dy, ys)
            for h in range(HALVES):
                e_p[plane, ty, h] = dot(mine, wed[:, block(ty * 2 + 1 - core, h)]).astype(BF16)
            copy_e1(plane, ty).start()
            for h in range(HALVES):
                e_o[plane, ty, h] = dot(mine, wed[:, block(ty * 2 + core, h)])

    def push(plane):
        for dy in range(1, ys):
            ty = lax.rem(y + dy, ys)
            copy_e1(plane, ty).wait_recv()
            for h in range(HALVES):
                es[plane, ty, h] = (e_o[plane, ty, h] + e_r[plane, ty, h].astype(F32)).astype(BF16)
                copy_e2(plane, dy, h).start()

    def deliver(plane, first):
        copy_e1(plane, y).wait_recv()
        for h in range(HALVES):
            result = e_o[plane, y, h] + e_r[plane, y, h].astype(F32)
            for dy in range(1, ys):
                copy_e2(plane, dy, h).wait_recv()
                result = result + er[plane, lax.rem(y - dy + ys, ys), h].astype(F32)
            result = result.reshape(nx, cap, sw).astype(BF16)
            for i in range(nx):
                outb[plane * nx + i, h] = result[i]
            for dx in range(first, nx):
                copy_e3(peer_of(plane, dx), h).start()

    @pl.loop(0, nz - 1)
    def _(j):
        issue(far(j))

        @pl.when(j > 0)
        def _():
            push(far(j - 1))

    issue(z)
    if nz > 1:
        push(far(nz - 2))
    push(z)

    @pl.loop(0, nz - 1)
    def _(j):
        deliver(far(j), 0)

    deliver(z, 1)
    for h in range(HALVES):
        ret[e, h] = outb[e, h]

    def combine(weights, back):
        return lax.dot_general(weights, back, (((0,), (0,)), ((), ())), preferred_element_type=F32)

    for h in range(HALVES):
        @pl.loop(1, n)
        def _(d):
            landed_e3(lax.rem(e + d, n), h).wait_recv()

        back = jnp.concatenate([ret[i, h] for i in range(n)], axis=0)
        layer_v[:, h * sw:(h + 1) * sw] = (
            mixed[h] + combine(comb_hi, back) + combine(comb_lo, back)
        ).astype(BF16)

    puts[2].start()

    @pl.loop(1, n)
    def _(d):
        peer = lax.rem(e + d, n)
        copy_a(peer).wait_send()
        copy_a2(peer).wait_send()
        for h in range(HALVES):
            copy_c1(peer, h).wait_send()
            copy_e3(peer, h).wait_send()

    @pl.loop(0, n)
    def _(src):
        for h in range(HALVES):
            for dy in range(1, ys):
                copy_c2(dy, src, h).wait_send()
            for dy in range(ys):
                copy_c3(dy, src, h).wait_send()

    for dy in range(ys):
        for h in range(HALVES):
            copy_d1(dy, h).wait_send()
            if dy:
                copy_d2(dy, h).wait_send()

    @pl.loop(0, nz)
    def _(plane):
        for yy in range(ys):
            copy_e1(plane, yy).wait_send()
        for dy in range(1, ys):
            for h in range(HALVES):
                copy_e2(plane, dy, h).wait_send()
        for c in range(nc):
            for dx in range(1, nx):
                copy_x(plane, dx, c).wait_send()

    @pl.loop(0, nz - 1)
    def _(j):
        plane = far(j)
        for c in range(nc):
            copy_z((plane < z).astype(jnp.int32), plane, c).wait_send()

    for put in puts:
        put.wait()


def finish(layer_in, state_in, conv_in, layer_out, state_out, conv_out):
    layer_out[...] = layer_in[...]
    state_out[...] = state_in[...]
    conv_out[...] = conv_in[...]


def shards(
    n, p,
    tokens, state_in, conv_in, mix_gain, rnn_weight, gate_weight, conv_weight, rate_weight,
    input_weight, rate_param, out_weight, moe_gain, expert_gate, expert_up, expert_down, routes, route_prob,
):
    g, width = tokens.shape
    depth, chans = rnn_weight.shape
    share = width // p
    cap = max(2, 2 * g * routes.shape[1] // n)
    slots = n * cap
    hidden = expert_gate.shape[2]
    ys = p // 2
    nx = 1 << ((n.bit_length() - 1) // 2)
    nx = nx if n % nx == 0 else 1
    nz = n // nx
    nc, cw = rate_weight.shape[0], 2 * rate_weight.shape[1]
    nh, sw = HALVES, share // HALVES
    chunk = nx * cap
    vm = pl.BlockSpec(memory_space=pltpu.VMEM)
    hb = pl.BlockSpec(memory_space=pl.ANY)
    dma = pltpu.SemaphoreType.DMA
    V = pltpu.VMEM
    small = (
        tokens, state_in, jnp.transpose(conv_in, (1, 0, 2)), mix_gain.reshape(-1, 128), moe_gain.reshape(-1, 128),
        conv_weight, rate_param[None], routes.T, route_prob.T,
    )
    scratch = [V(a.shape, a.dtype) for a in small] + [
        V((g, share), BF16), V((g, chans), F32), V((conv_in.shape[1], g, chans), BF16),
        V((depth, chans), BF16), V((depth, chans), BF16),
        V(rate_weight.shape, BF16), V(input_weight.shape, BF16), V(out_weight.shape, BF16),
        V(expert_gate.shape[1:], BF16), V(expert_up.shape[1:], BF16), V(expert_down.shape[1:], BF16),
        V((1, width), F32), V((1, width), F32),
        V((n, g, depth), BF16), V((n, g, depth), BF16),
        V((nz, nx, nc, g, cw), BF16), V((nz, nx, nc, g, cw), BF16),
        V((nz, nc, g, cw), BF16), V((2, nz, nc, g, cw), BF16),
        V((g, chans), BF16), V((p, nh, g, sw), F32),
        V((ys, nh, g, sw), BF16), V((ys, nh, g, sw), F32), V((ys, nh, g, sw), BF16),
        V((ys, nh, g, sw), BF16), V((ys, nh, g, sw), BF16), V((nh, g, sw), F32),
        V((n, nh, cap, sw), BF16), V((p, n, nh, cap, sw), BF16), V((nh, slots, p * sw), BF16), V((slots, 1), F32),
        V((2, slots, hidden), F32), V((slots, hidden), BF16),
        V((nz, ys, nh, chunk, sw), BF16), V((nz, ys, nh, chunk, sw), F32), V((nz, ys, nh, chunk, sw), BF16),
        V((nz, ys, nh, chunk, sw), BF16), V((nz, ys, nh, chunk, sw), BF16),
        V((n, nh, cap, sw), BF16), V((n, nh, cap, sw), BF16),
        dma((8,)), dma((len(small),)), dma((3,)),
        dma((n,)), dma((n,)), dma((n,)), dma((n,)),
        dma((nz, nx, nc)), dma((nz, nx, nc)), dma((nz, nc)), dma((2, nz, nc)),
        dma((ys, nh)), dma((ys, nh)), dma((ys, nh)), dma((ys, nh)),
        dma((n, nh)), dma((n, nh)), dma((ys, n, nh)), dma((ys, n, nh)), dma((ys, n, nh)), dma((ys, n, nh)),
        dma((nz, ys)), dma((nz, ys)), dma((nz, ys, nh)), dma((nz, ys, nh)), dma((n, nh)), dma((n, nh)),
    ]
    outs = (
        jax.ShapeDtypeStruct((g, share), BF16),
        jax.ShapeDtypeStruct((g, chans), F32),
        jax.ShapeDtypeStruct((conv_in.shape[1], g, chans), BF16),
    )
    held = pl.pallas_call(
        functools.partial(kernel, n, p, nx, cap),
        out_shape=outs,
        in_specs=[hb] * 17,
        out_specs=(hb, hb, hb),
        scratch_shapes=scratch,
        compiler_params=pltpu.CompilerParams(
            collective_id=0, has_side_effects=True, vmem_limit_bytes=60 * 1024 * 1024
        ),
    )(
        *small,
        rnn_weight, gate_weight, rate_weight, input_weight, out_weight, expert_gate, expert_up, expert_down,
    )
    layer_out, state_out, conv_out = pl.pallas_call(
        finish,
        out_shape=outs,
        in_specs=[vm] * 3,
        out_specs=(vm, vm, vm),
    )(*held)
    return (layer_out, state_out, jnp.transpose(conv_out, (1, 0, 2)))


def solution(mesh):
    in_specs = (
        P("ep", None),
        P("ep", "tp"),
        P("ep", None, "tp"),
        P(),
        P("ep", "tp"),
        P("ep", "tp"),
        P(None, "tp"),
        P("tp", None, None),
        P("tp", None, None),
        P("tp"),
        P("tp", None),
        P(),
        P("ep", None, "tp"),
        P("ep", None, "tp"),
        P("ep", "tp", None),
        P("ep", None),
        P("ep", None),
    )
    out_specs = (P("ep", "tp"), P("ep", "tp"), P("ep", None, "tp"))
    body = functools.partial(shards, mesh.shape["ep"], mesh.shape["tp"])
    return jax.shard_map(body, mesh=mesh, in_specs=in_specs, out_specs=out_specs, check_vma=False)
```

```python
import functools

import jax
import jax.numpy as jnp
from jax import lax
from jax.experimental import pallas as pl
from jax.experimental.pallas import tpu as pltpu
from jax.sharding import PartitionSpec as P

MESH = pl.DeviceIdType.MESH
F32 = jnp.float32
BF16 = jnp.bfloat16
HALVES = 2
LAG = 3


def dot(a, b):
    return jnp.dot(a, b, preferred_element_type=F32)


def remote(src, dst, send, recv, where):
    return pltpu.make_async_remote_copy(
        src_ref=src, dst_ref=dst, send_sem=send, recv_sem=recv, device_id=where, device_id_type=MESH
    )


def kernel(
    n, p, nx, cap,
    tokens_h, state_h, conv_h, mix_h, moe_h, taps_h, param_h, routes_h, prob_h,
    rnn_h, gate_h, rate_h, input_h, out_h, eg_h, eu_h, ed_h,
    layer_out, state_out, conv_out,
    tokens, state_in, conv_in, mix_gain_in, moe_gain_in, conv_w, rate_param, routes, prob,
    layer_v, state_v, conv_v,
    wr, wg, wrate, winput, wout, weg, weu, wed,
    mix_gain, moe_gain, normed, cols, part, bx, zsend, rz, gated, oacc,
    op_p, op_o, op_r, hs, hr, mixed,
    sd, rows, xn, ssq, gacc, hid, e_p, e_o, e_r, es, er, outb, ret,
    wsem, lsem, osem, sa, ra, sa2, ra2, sb, rb, sz, rzs, sd1, rd1, sd2, rd2,
    sc1, rc1, sc2, rc2, sc3, rc3, se1, re1, se2, re2, se3, re3,
):
    e = lax.axis_index("ep")
    t = lax.axis_index("tp")
    core = lax.rem(t, 2)
    y = t // 2
    q = t + 1 - 2 * core
    ys = p // 2
    nz = n // nx
    z = e // nx
    x = lax.rem(e, nx)

    rows_g, width = tokens.shape
    depth = width // n
    share = width // p
    sw = share // HALVES
    slots = n * cap

    small = [
        pltpu.make_async_copy(a, b, lsem.at[i])
        for i, (a, b) in enumerate(
            [(tokens_h, tokens), (mix_h, mix_gain_in), (moe_h, moe_gain_in), (routes_h, routes), (prob_h, prob),
             (taps_h, conv_w), (param_h, rate_param), (conv_h, conv_in), (state_h, state_in)]
        )
    ]
    loads = [
        pltpu.make_async_copy(a, b, wsem.at[i])
        for i, (a, b) in enumerate(
            [(rnn_h, wr), (gate_h, wg), (rate_h, wrate), (input_h, winput), (out_h, wout),
             (eg_h.at[0], weg), (eu_h.at[0], weu), (ed_h.at[0], wed)]
        )
    ]
    small[0].start()
    small[1].start()

    barrier = pltpu.get_barrier_semaphore()

    @pl.loop(1, n)
    def _(d):
        pl.semaphore_signal(barrier, inc=1, device_id={"ep": lax.rem(e + d, n)}, device_id_type=MESH)

    @pl.loop(1, p)
    def _(d):
        pl.semaphore_signal(barrier, inc=1, device_id={"tp": lax.rem(t + d, p)}, device_id_type=MESH)

    for load in small[2:] + loads[:4]:
        load.start()

    @pl.when(z == 0)
    def _():
        rz[0] = jnp.zeros(rz.shape[1:], BF16)

    @pl.when(z == nz - 1)
    def _():
        rz[1] = jnp.zeros(rz.shape[1:], BF16)

    small[0].wait()
    small[1].wait()
    for j in range(width // 128):
        cs = slice(j * 128, (j + 1) * 128)
        mix_gain[:, cs] = mix_gain_in[j:j + 1, :].astype(F32)

    total_sq = jnp.zeros((rows_g, 1), F32)
    for j in range(n):
        v = tokens[:, j * depth:(j + 1) * depth].astype(F32)
        total_sq = total_sq + jnp.sum(v * v, axis=1, keepdims=True)
    scale = lax.rsqrt(total_sq / width + 1e-06)
    for j in range(n):
        cs = slice(j * depth, (j + 1) * depth)
        normed[j] = (tokens[:, cs].astype(F32) * scale * mix_gain[:, cs]).astype(BF16)

    pl.semaphore_wait(barrier, n + p - 2)

    half = pl.ds(pl.multiple_of(core * (rows_g // 2), rows_g // 2), rows_g // 2)
    nc, bw = rate_h.shape[0], rate_h.shape[1]
    high = (2 * z) // nz
    folded = z + high * (nz - 1 - 2 * z)

    def far(j):
        plane = nz - 1 - j
        plane = plane - (folded >= plane).astype(jnp.int32)
        return plane + high * (nz - 1 - 2 * plane)

    def beside(dx):
        return lax.rem(x + dx, nx)

    def peer_of(plane, dx):
        return plane * nx + beside(dx)

    def copy_a(peer):
        return remote(normed.at[peer, half], cols.at[e, half], sa, ra.at[e], {"ep": peer})

    def landed_a(src):
        return remote(normed.at[src, half], cols.at[src, half], sa, ra.at[src], {"ep": src})

    def copy_a2(src):
        return remote(cols.at[src, half], cols.at[src, half], sa2, ra2.at[src], {"tp": q})

    for dx in range(1, nx):
        copy_a(peer_of(z, dx)).start()

    @pl.loop(0, nz - 1)
    def _(j):
        for dx in range(nx):
            copy_a(peer_of(far(j), dx)).start()

    cols[e] = normed[e]

    for j in range(2, 5):
        small[j].wait()
    for j in range(width // 128):
        cs = slice(j * 128, (j + 1) * 128)
        moe_gain[:, cs] = moe_gain_in[j:j + 1, :].astype(F32)
    ids = routes[...]
    sub_e = lax.broadcasted_iota(jnp.int32, (n, rows_g), 0)
    named = [(ids[k:k + 1, :] == sub_e).astype(F32) for k in range(ids.shape[0])]
    member = functools.reduce(lambda a, b: a + b, named)
    earlier = (
        lax.broadcasted_iota(jnp.int32, (rows_g, rows_g), 0)
        < lax.broadcasted_iota(jnp.int32, (rows_g, rows_g), 1)
    ).astype(F32)
    before = dot(member.astype(BF16), earlier.astype(BF16))
    sub_s = lax.broadcasted_iota(jnp.int32, (slots, rows_g), 0).astype(F32)
    total_prob = jnp.sum(prob[...], axis=0, keepdims=True)
    dispatch = jnp.zeros((slots, rows_g), F32)
    comb = jnp.zeros((slots, rows_g), F32)
    for k in range(ids.shape[0]):
        slot = jnp.sum(before * named[k], axis=0, keepdims=True)
        target = ids[k:k + 1, :].astype(F32) * cap + slot
        hit = (sub_s == target).astype(F32)
        dispatch = dispatch + hit
        comb = comb + hit * (prob[k:k + 1, :] / total_prob)
    dispatch = dispatch.astype(BF16)
    comb_hi = comb.astype(BF16)
    comb_lo = (comb - comb_hi.astype(F32)).astype(BF16)

    loads[0].wait()
    loads[1].wait()
    for load in loads[4:]:
        load.start()

    def copy_x(plane, dx, c):
        return remote(
            part.at[plane, beside(dx), c], bx.at[plane, dx, c], sb, rb.at[plane, dx - 1, c],
            {"ep": peer_of(z, dx)},
        )

    def project(plane, last, own):
        first = 1 if own else 0
        for dx in range(first, nx):
            src = peer_of(plane, dx)
            landed_a(src).wait_recv()
            copy_a2(src).start()
        for dx in range(first, nx):
            copy_a2(peer_of(plane, dx)).wait_recv()
        feats = cols[pl.ds(plane * nx, nx)].reshape(nx * rows_g, depth)
        for c in range(nc):
            cs = slice(c * bw, (c + 1) * bw)
            for lo, weight in ((0, wr), (bw, wg)):
                value = dot(feats, weight[:, cs]).astype(BF16)
                for i in range(nx):
                    part[plane, i, c, :, lo:lo + bw] = value[i * rows_g:(i + 1) * rows_g]
            if c < last:
                for dx in range(1, nx):
                    copy_x(plane, dx, c).start()

    project(z, nc // 2, True)

    @pl.loop(0, nz - 1)
    def _(j):
        project(far(j), nc, False)

    for c in range(nc // 2, nc):
        for dx in range(1, nx):
            copy_x(z, dx, c).start()

    def copy_z(side, plane, c):
        to = z + 1 - 2 * side
        return remote(
            zsend.at[plane, c], rz.at[side, plane, c], sz, rzs.at[side, plane, c],
            {"ep": to * nx + x},
        )

    def summed(sides, plane, c):
        for dx in range(1, nx):
            copy_x(plane, dx, c).wait_recv()
        total = part[plane, x, c].astype(F32)
        for dx in range(1, nx):
            total = total + bx[plane, dx, c].astype(F32)
        for s in sides:
            origin = z - 1 + 2 * s

            @pl.when((origin >= 0) & (origin < nz))
            def _():
                copy_z(s, plane, c).wait_recv()

            total = total + rz[s, plane, c].astype(F32)
        return total

    @pl.loop(0, nz - 1)
    def _(j):
        plane = far(j)
        side = (plane < z).astype(jnp.int32)
        for c in range(nc):
            zsend[plane, c] = summed([side], plane, c).astype(BF16)
            copy_z(side, plane, c).start()

    def block(i, h):
        return pl.ds(pl.multiple_of(i * share + h * sw, sw), sw)

    for load in small[5:]:
        load.wait()
    loads[2].wait()
    loads[3].wait()
    loads[4].wait()
    for i in range(1, conv_in.shape[0]):
        conv_v[i - 1] = conv_in[i]
    for c in range(nc):
        cs = slice(c * bw, (c + 1) * bw)
        proj = summed([0, 1], z, c)
        moved = proj[:, :bw].astype(BF16)
        conv_v[conv_in.shape[0] - 1, :, cs] = moved
        taps = conv_w[:, cs].astype(F32)
        hist = conv_in[0, :, cs].astype(F32) * taps[0:1]
        for i in range(1, 3):
            hist = hist + conv_in[i, :, cs].astype(F32) * taps[i:i + 1]
        conv = (hist + moved.astype(F32) * taps[3:4]).astype(BF16)
        rate = jax.nn.sigmoid(dot(conv, wrate[c]))
        in_gate = jax.nn.sigmoid(dot(conv, winput[c]))
        log_decay = -8.0 * rate * jnp.log1p(jnp.exp(-rate_param[:, cs]))
        th = jnp.tanh(log_decay)
        rest = -2.0 * th / (1.0 - th)
        state = jnp.exp(log_decay) * state_in[:, cs] + jnp.sqrt(rest) * in_gate * conv.astype(F32)
        state_v[:, cs] = state
        gated[:, cs] = (state * jax.nn.gelu(proj[:, bw:], approximate=True)).astype(BF16)
        if c < nc - 1:
            for i in range(p):
                for h in range(HALVES):
                    lo = i * share + h * sw
                    piece = dot(gated[:, cs], wout[cs, lo:lo + sw])
                    oacc[i, h] = piece if c == 0 else oacc[i, h] + piece

    last = slice((nc - 1) * bw, nc * bw)

    def out_part(i, h):
        piece = dot(gated[:, last], wout[last, block(i, h)])
        return oacc[i, h] + piece if nc > 1 else piece

    def copy_d1(yy, h):
        return remote(op_p.at[yy, h], op_r.at[yy, h], sd1, rd1.at[yy, h], {"tp": q})

    def copy_d2(dy, h):
        ty = lax.rem(y + dy, ys)
        return remote(hs.at[ty, h], hr.at[y, h], sd2, rd2.at[dy - 1, h], {"tp": ty * 2 + core})

    for dy in range(ys):
        yy = lax.rem(y + dy + 1, ys)
        for h in range(HALVES):
            op_p[yy, h] = out_part(yy * 2 + 1 - core, h).astype(BF16)
            copy_d1(yy, h).start()
    for dy in range(ys):
        yy = lax.rem(y + dy + 1, ys)
        for h in range(HALVES):
            op_o[yy, h] = out_part(yy * 2 + core, h)
    for h in range(HALVES):
        for dy in range(1, ys):
            ty = lax.rem(y + dy, ys)
            copy_d1(ty, h).wait_recv()
            hs[ty, h] = (op_o[ty, h] + op_r[ty, h].astype(F32)).astype(BF16)
            copy_d2(dy, h).start()

    puts = [
        pltpu.make_async_copy(a, b, osem.at[i])
        for i, (a, b) in enumerate([(state_v, state_out), (conv_v, conv_out), (layer_v, layer_out)])
    ]
    puts[0].start()
    puts[1].start()

    def copy_c1(peer, h):
        return remote(sd.at[h, peer], rows.at[h, t, e], sc1, rc1.at[e, h], {"ep": peer})

    def landed_c1(src, h):
        return remote(sd.at[h, src], rows.at[h, t, src], sc1, rc1.at[src, h], {"ep": src})

    def copy_c2(dy, src, h):
        to = lax.rem(y + dy, ys) * 2 + core
        return remote(rows.at[h, t, src], rows.at[h, t, src], sc2, rc2.at[dy - 1, src, h], {"tp": to})

    def landed_c2(dy, src, h):
        held = lax.rem(y - dy + ys, ys) * 2 + core
        return remote(
            rows.at[h, held, src], rows.at[h, held, src], sc2, rc2.at[dy - 1, src, h], {"tp": held}
        )

    def copy_c3(dy, src, h):
        held = lax.rem(y - dy + ys, ys) * 2 + core
        return remote(
            rows.at[h, held, src], rows.at[h, held, src], sc3, rc3.at[h], {"tp": q}
        )

    for h in range(HALVES):
        copy_d1(y, h).wait_recv()
        total = tokens[:, block(t, h)].astype(F32) + op_o[y, h] + op_r[y, h].astype(F32)
        for dy in range(1, ys):
            copy_d2(dy, h).wait_recv()
            total = total + hr[lax.rem(y - dy + ys, ys), h].astype(F32)
        mixed[h] = total
        sent = dot(dispatch, total.astype(BF16)).reshape(n, cap, sw).astype(BF16)
        sd[h] = sent
        for dx in range(1, nx):
            copy_c1(peer_of(z, dx), h).start()

        @pl.loop(0, nz - 1)
        def _(j):
            for dx in range(nx):
                copy_c1(peer_of(far(nz - 2 - j), dx), h).start()

        rows[h, t, e] = sd[h, e]
        for dy in range(1, ys):
            copy_c2(dy, e, h).start()
        copy_c3(0, e, h).start()

    gs = min(n, max(1, 64 // cap))
    span = gs * cap
    hidden = hid.shape[1]
    fc = min(256, hidden)

    def scaled_rows(h):
        mate = rows.at[h, pl.ds(0, ys)]
        remote(mate, mate, sc3, rc3.at[h], {"tp": q}).wait_recv()

        @pl.loop(0, n // gs)
        def _(g):
            at = pl.ds(pl.multiple_of(g * span, span), span)
            acc = jnp.zeros((span, 1), F32)
            for i in range(p):
                lo = i * share + h * sw
                v = rows[h, i, pl.ds(g * gs, gs)].astype(F32).reshape(span, sw)
                acc = acc + jnp.sum(v * v, axis=1, keepdims=True)
                xn[h, at, i * sw:(i + 1) * sw] = (v * moe_gain[:, lo:lo + sw]).astype(BF16)
            ssq[at, :] = acc if h == 0 else ssq[at, :] + acc

    def partial_dot(weight, h, cs):
        acc = None
        for i in range(p):
            lo = i * share + h * sw
            piece = dot(xn[h, :, i * sw:(i + 1) * sw], weight[lo:lo + sw, cs])
            acc = piece if acc is None else acc + piece
        return acc

    def early(k, weight, f):
        cs = slice(f * fc, (f + 1) * fc)
        gacc[k, :, cs] = partial_dot(weight, 0, cs)

    def first_half():
        loads[5].wait()
        loads[6].wait()
        scaled_rows(0)

    tasks = [first_half]
    for f in range(hidden // fc):
        tasks.append(functools.partial(early, 0, weg, f))
        tasks.append(functools.partial(early, 1, weu, f))

    near = [(z, dx) for dx in range(1, nx)]
    near = near + [(far(j), dx) for j in reversed(range(nz - 1)) for dx in range(nx)]
    steps = [(peer_of(plane, dx), h) for h in range(HALVES) for plane, dx in near]
    queue = [(e, h) for h in range(HALVES)]
    begin = len(near) + len(near) // 2
    for i, (src, h) in enumerate(steps):
        landed_c1(src, h).wait_recv()
        for dy in range(1, ys):
            copy_c2(dy, src, h).start()
        copy_c3(0, src, h).start()
        queue.append((src, h))
        if len(queue) > LAG:
            was, wh = queue.pop(0)
            for dy in range(1, ys):
                landed_c2(dy, was, wh).wait_recv()
                copy_c3(dy, was, wh).start()
        if i >= begin and tasks:
            tasks.pop(0)()
    for was, wh in queue:
        for dy in range(1, ys):
            landed_c2(dy, was, wh).wait_recv()
            copy_c3(dy, was, wh).start()
    for task in tasks:
        task()

    scaled_rows(HALVES - 1)
    row_scale = lax.rsqrt(ssq[...] / width + 1e-06)
    for f in range(hidden // fc):
        cs = slice(f * fc, (f + 1) * fc)
        gate_part = (gacc[0, :, cs] + partial_dot(weg, 1, cs)) * row_scale
        up_part = (gacc[1, :, cs] + partial_dot(weu, 1, cs)) * row_scale
        hid[:, cs] = (jax.nn.silu(gate_part) * up_part).astype(BF16)

    loads[7].wait()
    chunk = nx * cap

    def copy_e1(plane, yy):
        return remote(e_p.at[plane, yy], e_r.at[plane, yy], se1, re1.at[plane, yy], {"tp": q})

    def copy_e2(plane, dy, h):
        ty = lax.rem(y + dy, ys)
        return remote(
            es.at[plane, ty, h], er.at[plane, y, h], se2, re2.at[plane, dy - 1, h],
            {"tp": ty * 2 + core},
        )

    def copy_e3(peer, h):
        return remote(outb.at[h, peer], ret.at[h, e], se3, re3.at[h], {"ep": peer})

    def issue(planes, dys):
        mine = jnp.concatenate([hid[pl.ds(pl.multiple_of(k * chunk, chunk), chunk), :] for k in planes], axis=0)
        for dy in dys:
            ty = lax.rem(y + dy, ys)
            for h in range(HALVES):
                value = dot(mine, wed[:, block(ty * 2 + 1 - core, h)]).astype(BF16)
                for i, k in enumerate(planes):
                    e_p[k, ty, h] = value[i * chunk:(i + 1) * chunk]
            for k in planes:
                copy_e1(k, ty).start()
            for h in range(HALVES):
                value = dot(mine, wed[:, block(ty * 2 + core, h)])
                for i, k in enumerate(planes):
                    e_o[k, ty, h] = value[i * chunk:(i + 1) * chunk]

    def push(plane):
        for dy in range(1, ys):
            ty = lax.rem(y + dy, ys)
            copy_e1(plane, ty).wait_recv()
            for h in range(HALVES):
                es[plane, ty, h] = (e_o[plane, ty, h] + e_r[plane, ty, h].astype(F32)).astype(BF16)
                copy_e2(plane, dy, h).start()

    def deliver(plane, first):
        copy_e1(plane, y).wait_recv()
        for h in range(HALVES):
            result = e_o[plane, y, h] + e_r[plane, y, h].astype(F32)
            for dy in range(1, ys):
                copy_e2(plane, dy, h).wait_recv()
                result = result + er[plane, lax.rem(y - dy + ys, ys), h].astype(F32)
            result = result.reshape(nx, cap, sw).astype(BF16)
            outb[h, pl.ds(plane * nx, nx)] = result
            for dx in range(first, nx):
                copy_e3(peer_of(plane, dx), h).start()

    order = [far(j) for j in range(nz - 1)] + [z]
    pairs = [order[i:i + 2] for i in range(0, nz, 2)]
    for planes in pairs:
        issue(planes, range(1, ys))
        issue(planes, [0])
        for plane in planes:
            push(plane)

    @pl.loop(0, nz - 1)
    def _(j):
        deliver(far(j), 0)

    deliver(z, 1)
    for h in range(HALVES):
        ret[h, e] = outb[h, e]

    def combine(weights, back):
        return lax.dot_general(weights, back, (((0,), (0,)), ((), ())), preferred_element_type=F32)

    for h in range(HALVES):
        others = ret.at[h, pl.ds(0, n - 1)]
        remote(others, others, se3, re3.at[h], {"ep": peer_of(z, 1)}).wait_recv()
        back = ret[h].astype(F32).reshape(slots, sw).astype(BF16)
        layer_v[:, h * sw:(h + 1) * sw] = (
            mixed[h] + combine(comb_hi, back) + combine(comb_lo, back)
        ).astype(BF16)

    puts[2].start()

    def drain(ref, sem):
        remote(ref, ref, sem, ra.at[0], {"tp": q}).wait_send()

    drain(normed.at[pl.ds(0, n - 1), half], sa)
    drain(cols.at[pl.ds(0, n - 1), half], sa2)
    drain(part.at[:, pl.ds(0, nx - 1)], sb)
    drain(zsend.at[pl.ds(0, nz - 1)], sz)
    drain(op_p, sd1)
    drain(hs.at[pl.ds(0, ys - 1)], sd2)
    drain(sd.at[:, pl.ds(0, n - 1)], sc1)
    drain(rows.at[:, pl.ds(0, ys - 1)], sc2)
    drain(rows.at[:, pl.ds(0, ys)], sc3)
    drain(e_p, se1)
    drain(es.at[:, pl.ds(0, ys - 1)], se2)
    drain(outb.at[:, pl.ds(0, n - 1)], se3)

    for put in puts:
        put.wait()


def finish(layer_in, state_in, conv_in, layer_out, state_out, conv_out):
    layer_out[...] = layer_in[...]
    state_out[...] = state_in[...]
    conv_out[...] = conv_in[...]


def shards(
    n, p,
    tokens, state_in, conv_in, mix_gain, rnn_weight, gate_weight, conv_weight, rate_weight,
    input_weight, rate_param, out_weight, moe_gain, expert_gate, expert_up, expert_down, routes, route_prob,
):
    g, width = tokens.shape
    depth, chans = rnn_weight.shape
    share = width // p
    cap = max(2, 2 * g * routes.shape[1] // n)
    slots = n * cap
    hidden = expert_gate.shape[2]
    ys = p // 2
    nx = 1 << ((n.bit_length() - 1) // 2)
    nx = nx if n % nx == 0 else 1
    nz = n // nx
    nc, cw = rate_weight.shape[0], 2 * rate_weight.shape[1]
    nh, sw = HALVES, share // HALVES
    chunk = nx * cap
    vm = pl.BlockSpec(memory_space=pltpu.VMEM)
    hb = pl.BlockSpec(memory_space=pl.ANY)
    dma = pltpu.SemaphoreType.DMA
    V = pltpu.VMEM
    small = (
        tokens, state_in, jnp.transpose(conv_in, (1, 0, 2)), mix_gain.reshape(-1, 128), moe_gain.reshape(-1, 128),
        conv_weight, rate_param[None], routes.T, route_prob.T,
    )
    scratch = [V(a.shape, a.dtype) for a in small] + [
        V((g, share), BF16), V((g, chans), F32), V((conv_in.shape[1], g, chans), BF16),
        V((depth, chans), BF16), V((depth, chans), BF16),
        V(rate_weight.shape, BF16), V(input_weight.shape, BF16), V(out_weight.shape, BF16),
        V(expert_gate.shape[1:], BF16), V(expert_up.shape[1:], BF16), V(expert_down.shape[1:], BF16),
        V((1, width), F32), V((1, width), F32),
        V((n, g, depth), BF16), V((n, g, depth), BF16),
        V((nz, nx, nc, g, cw), BF16), V((nz, nx, nc, g, cw), BF16),
        V((nz, nc, g, cw), BF16), V((2, nz, nc, g, cw), BF16),
        V((g, chans), BF16), V((p, nh, g, sw), F32),
        V((ys, nh, g, sw), BF16), V((ys, nh, g, sw), F32), V((ys, nh, g, sw), BF16),
        V((ys, nh, g, sw), BF16), V((ys, nh, g, sw), BF16), V((nh, g, sw), F32),
        V((nh, n, cap, sw), BF16), V((nh, p, n, cap, sw), BF16), V((nh, slots, p * sw), BF16), V((slots, 1), F32),
        V((2, slots, hidden), F32), V((slots, hidden), BF16),
        V((nz, ys, nh, chunk, sw), BF16), V((nz, ys, nh, chunk, sw), F32), V((nz, ys, nh, chunk, sw), BF16),
        V((nz, ys, nh, chunk, sw), BF16), V((nz, ys, nh, chunk, sw), BF16),
        V((nh, n, cap, sw), BF16), V((nh, n, cap, sw), BF16),
        dma((8,)), dma((len(small),)), dma((3,)),
        dma, dma((n,)), dma, dma((n,)),
        dma, dma((nz, nx - 1, nc)), dma, dma((2, nz, nc)),
        dma, dma((ys, nh)), dma, dma((ys - 1, nh)),
        dma, dma((n, nh)), dma, dma((ys - 1, n, nh)), dma, dma((nh,)),
        dma, dma((nz, ys)), dma, dma((nz, ys - 1, nh)), dma, dma((nh,)),
    ]
    outs = (
        jax.ShapeDtypeStruct((g, share), BF16),
        jax.ShapeDtypeStruct((g, chans), F32),
        jax.ShapeDtypeStruct((conv_in.shape[1], g, chans), BF16),
    )
    held = pl.pallas_call(
        functools.partial(kernel, n, p, nx, cap),
        out_shape=outs,
        in_specs=[hb] * 17,
        out_specs=(hb, hb, hb),
        scratch_shapes=scratch,
        compiler_params=pltpu.CompilerParams(
            collective_id=0, has_side_effects=True, vmem_limit_bytes=60 * 1024 * 1024
        ),
    )(
        *small,
        rnn_weight, gate_weight, rate_weight, input_weight, out_weight, expert_gate, expert_up, expert_down,
    )
    layer_out, state_out, conv_out = pl.pallas_call(
        finish,
        out_shape=outs,
        in_specs=[vm] * 3,
        out_specs=(vm, vm, vm),
    )(*held)
    return (layer_out, state_out, jnp.transpose(conv_out, (1, 0, 2)))


def solution(mesh):
    in_specs = (
        P("ep", None),
        P("ep", "tp"),
        P("ep", None, "tp"),
        P(),
        P("ep", "tp"),
        P("ep", "tp"),
        P(None, "tp"),
        P("tp", None, None),
        P("tp", None, None),
        P("tp"),
        P("tp", None),
        P(),
        P("ep", None, "tp"),
        P("ep", None, "tp"),
        P("ep", "tp", None),
        P("ep", None),
        P("ep", None),
    )
    out_specs = (P("ep", "tp"), P("ep", "tp"), P("ep", None, "tp"))
    body = functools.partial(shards, mesh.shape["ep"], mesh.shape["tp"])
    return jax.shard_map(body, mesh=mesh, in_specs=in_specs, out_specs=out_specs, check_vma=False)
```

```python
import functools

import jax
import jax.numpy as jnp
from jax import lax
from jax.experimental import pallas as pl
from jax.experimental.pallas import tpu as pltpu
from jax.sharding import PartitionSpec as P

MESH = pl.DeviceIdType.MESH
F32 = jnp.float32
BF16 = jnp.bfloat16
HALVES = 2
LAG = 5


def dot(a, b):
    return jnp.dot(a, b, preferred_element_type=F32)


def remote(src, dst, send, recv, where):
    return pltpu.make_async_remote_copy(
        src_ref=src, dst_ref=dst, send_sem=send, recv_sem=recv, device_id=where, device_id_type=MESH
    )


def kernel(
    n, p, nx, cap,
    tokens_h, state_h, conv_h, mix_h, moe_h, taps_h, param_h, routes_h, prob_h,
    rnn_h, gate_h, rate_h, input_h, out_h, eg_h, eu_h, ed_h,
    layer_out, state_out, conv_out,
    tokens, state_in, conv_in, mix_gain_in, moe_gain_in, conv_w, rate_param, routes, prob,
    layer_v, state_v, conv_v,
    wr, wg, wrate, winput, wout, weg, weu, wed,
    mix_gain, moe_gain, normed, cols, part, bx, zsend, rz, zf, gated, oacc,
    op_p, op_o, op_r, hs, hr, mixed,
    sd, rows, xn, ssq, gacc, hid, e_p, e_o, e_r, es, er, outb, ret,
    wsem, lsem, osem, sa, ra, sa2, ra2, sb, rb, sz, rzs, szf, rzf, sd1, rd1, sd2, rd2,
    sc1, rc1, sc2, rc2, sc3, rc3, se1, re1, se2, re2, se3, re3,
):
    e = lax.axis_index("ep")
    t = lax.axis_index("tp")
    core = lax.rem(t, 2)
    y = t // 2
    q = t + 1 - 2 * core
    ys = p // 2
    nz = n // nx
    z = e // nx
    x = lax.rem(e, nx)

    rows_g, width = tokens.shape
    depth = width // n
    share = width // p
    sw = share // HALVES
    slots = n * cap

    small = [
        pltpu.make_async_copy(a, b, lsem.at[i])
        for i, (a, b) in enumerate(
            [(tokens_h, tokens), (mix_h, mix_gain_in), (moe_h, moe_gain_in), (routes_h, routes), (prob_h, prob),
             (taps_h, conv_w), (param_h, rate_param), (conv_h, conv_in), (state_h, state_in)]
        )
    ]
    loads = [
        pltpu.make_async_copy(a, b, wsem.at[i])
        for i, (a, b) in enumerate(
            [(rnn_h, wr), (gate_h, wg), (rate_h, wrate), (input_h, winput), (out_h, wout),
             (eg_h.at[0], weg), (eu_h.at[0], weu), (ed_h.at[0], wed)]
        )
    ]
    small[0].start()
    small[1].start()

    barrier = pltpu.get_barrier_semaphore()

    @pl.loop(1, n)
    def _(d):
        pl.semaphore_signal(barrier, inc=1, device_id={"ep": lax.rem(e + d, n)}, device_id_type=MESH)

    @pl.loop(1, p)
    def _(d):
        pl.semaphore_signal(barrier, inc=1, device_id={"tp": lax.rem(t + d, p)}, device_id_type=MESH)

    for load in small[2:] + loads[:4]:
        load.start()

    @pl.when(z == 0)
    def _():
        rz[0] = jnp.zeros(rz.shape[1:], BF16)

    @pl.when(z == nz - 1)
    def _():
        rz[1] = jnp.zeros(rz.shape[1:], BF16)

    small[0].wait()
    small[1].wait()
    nc, bw = rate_h.shape[0], rate_h.shape[1]
    late = nc // 2
    paired = nz % 2 == 0 and nz > 2
    middle = (z == nz // 2) | (z == nz // 2 - 1)
    opposite = nz - 1 - z
    if paired:
        @pl.when(middle)
        def _():
            for dx in range(1, nx):
                bx[opposite, dx, late:] = jnp.zeros((nc - late,) + bx.shape[3:], BF16)

    for j in range(width // 128):
        cs = slice(j * 128, (j + 1) * 128)
        mix_gain[:, cs] = mix_gain_in[j:j + 1, :].astype(F32)

    total_sq = jnp.zeros((rows_g, 1), F32)
    for j in range(n):
        v = tokens[:, j * depth:(j + 1) * depth].astype(F32)
        total_sq = total_sq + jnp.sum(v * v, axis=1, keepdims=True)
    scale = lax.rsqrt(total_sq / width + 1e-06)
    for j in range(n):
        cs = slice(j * depth, (j + 1) * depth)
        normed[j] = (tokens[:, cs].astype(F32) * scale * mix_gain[:, cs]).astype(BF16)

    pl.semaphore_wait(barrier, n + p - 2)

    half = pl.ds(pl.multiple_of(core * (rows_g // 2), rows_g // 2), rows_g // 2)
    high = (2 * z) // nz
    folded = z + high * (nz - 1 - 2 * z)

    lead = nz - 1 - 2 * folded

    def across(j):
        plane = nz - 1 - j
        plane = plane - (folded >= plane).astype(jnp.int32)
        return plane + high * (nz - 1 - 2 * plane)

    def far(j):
        ahead = (j < lead).astype(jnp.int32)
        k = (1 - ahead) * (j - lead)
        turn = folded + (folded - k // 2) * (2 * lax.rem(k, 2) - 1)
        plane = ahead * (nz - 1 - j) + (1 - ahead) * turn
        return plane + high * (nz - 1 - 2 * plane)

    def beside(dx):
        return lax.rem(x + dx, nx)

    def peer_of(plane, dx):
        return plane * nx + beside(dx)

    def copy_a(peer):
        return remote(normed.at[peer, half], cols.at[e, half], sa, ra.at[e], {"ep": peer})

    def landed_a(src):
        return remote(normed.at[src, half], cols.at[src, half], sa, ra.at[src], {"ep": src})

    def copy_a2(src):
        return remote(cols.at[src, half], cols.at[src, half], sa2, ra2.at[src], {"tp": q})

    for dx in range(1, nx):
        copy_a(peer_of(z, dx)).start()

    @pl.loop(0, nz - 1)
    def _(j):
        for dx in range(nx):
            copy_a(peer_of(across(j), dx)).start()

    cols[e] = normed[e]

    for j in range(2, 5):
        small[j].wait()
    for j in range(width // 128):
        cs = slice(j * 128, (j + 1) * 128)
        moe_gain[:, cs] = moe_gain_in[j:j + 1, :].astype(F32)
    ids = routes[...]
    sub_e = lax.broadcasted_iota(jnp.int32, (n, rows_g), 0)
    named = [(ids[k:k + 1, :] == sub_e).astype(F32) for k in range(ids.shape[0])]
    member = functools.reduce(lambda a, b: a + b, named)
    earlier = (
        lax.broadcasted_iota(jnp.int32, (rows_g, rows_g), 0)
        < lax.broadcasted_iota(jnp.int32, (rows_g, rows_g), 1)
    ).astype(F32)
    before = dot(member.astype(BF16), earlier.astype(BF16))
    sub_s = lax.broadcasted_iota(jnp.int32, (slots, rows_g), 0).astype(F32)
    total_prob = jnp.sum(prob[...], axis=0, keepdims=True)
    dispatch = jnp.zeros((slots, rows_g), F32)
    comb = jnp.zeros((slots, rows_g), F32)
    for k in range(ids.shape[0]):
        slot = jnp.sum(before * named[k], axis=0, keepdims=True)
        target = ids[k:k + 1, :].astype(F32) * cap + slot
        hit = (sub_s == target).astype(F32)
        dispatch = dispatch + hit
        comb = comb + hit * (prob[k:k + 1, :] / total_prob)
    dispatch = dispatch.astype(BF16)
    comb_hi = comb.astype(BF16)
    comb_lo = (comb - comb_hi.astype(F32)).astype(BF16)

    loads[0].wait()
    loads[1].wait()
    for load in loads[4:]:
        load.start()

    def copy_x(plane, dx, c):
        return remote(
            part.at[plane, beside(dx), c], bx.at[plane, dx, c], sb, rb.at[plane, dx - 1, c],
            {"ep": peer_of(z, dx)},
        )

    def copy_f(dx, c):
        return remote(
            part.at[opposite, beside(dx), c], zf.at[dx - 1, c - late], szf, rzf.at[dx - 1, c - late],
            {"ep": opposite * nx + x},
        )

    def by_line(plane, c):
        return middle & (plane == opposite) if paired and c >= late else None

    def unless(flag, action):
        if flag is None:
            action()
        else:
            pl.when(jnp.logical_not(flag))(action)

    def project(plane, last, own):
        first = 1 if own else 0
        for dx in range(first, nx):
            src = peer_of(plane, dx)
            landed_a(src).wait_recv()
            copy_a2(src).start()
        for dx in range(first, nx):
            copy_a2(peer_of(plane, dx)).wait_recv()
        feats = cols[pl.ds(plane * nx, nx)].reshape(nx * rows_g, depth)
        for c in range(nc):
            cs = slice(c * bw, (c + 1) * bw)
            for lo, weight in ((0, wr), (bw, wg)):
                value = dot(feats, weight[:, cs]).astype(BF16)
                for i in range(nx):
                    part[plane, i, c, :, lo:lo + bw] = value[i * rows_g:(i + 1) * rows_g]
            if c < last:
                flag = None if own else by_line(plane, c)
                for dx in range(1, nx):
                    unless(flag, copy_x(plane, dx, c).start)
                    if flag is not None:
                        pl.when(flag)(copy_f(dx, c).start)

    project(z, late, True)

    @pl.loop(0, nz - 1)
    def _(j):
        project(far(j), nc, False)

    def rest_of_own():
        for c in range(late, nc):
            for dx in range(1, nx):
                if paired:
                    @pl.when(middle)
                    def _():
                        copy_f(dx, c).wait_recv()
                        mine = part[z, beside(dx), c].astype(F32)
                        part[z, beside(dx), c] = (mine + zf[dx - 1, c - late].astype(F32)).astype(BF16)

                copy_x(z, dx, c).start()

    def copy_z(side, plane, c):
        to = z + 1 - 2 * side
        return remote(
            zsend.at[plane, c], rz.at[side, plane, c], sz, rzs.at[side, plane, c],
            {"ep": to * nx + x},
        )

    def summed(sides, plane, c):
        for dx in range(1, nx):
            unless(by_line(plane, c) if len(sides) == 1 else None, copy_x(plane, dx, c).wait_recv)
        total = part[plane, x, c].astype(F32)
        for dx in range(1, nx):
            total = total + bx[plane, dx, c].astype(F32)
        for s in sides:
            origin = z - 1 + 2 * s

            @pl.when((origin >= 0) & (origin < nz))
            def _():
                copy_z(s, plane, c).wait_recv()

            total = total + rz[s, plane, c].astype(F32)
        return total

    def line_step(j):
        plane = far(j)
        side = (plane < z).astype(jnp.int32)
        for c in range(nc):
            zsend[plane, c] = summed([side], plane, c).astype(BF16)
            copy_z(side, plane, c).start()

    if nz > 1:
        line_step(jnp.int32(0))
    rest_of_own()
    if nz > 1:
        pl.loop(1, nz - 1)(line_step)

    def block(i, h):
        return pl.ds(pl.multiple_of(i * share + h * sw, sw), sw)

    for load in small[5:]:
        load.wait()
    loads[2].wait()
    loads[3].wait()
    loads[4].wait()
    for i in range(1, conv_in.shape[0]):
        conv_v[i - 1] = conv_in[i]
    for c in range(nc):
        cs = slice(c * bw, (c + 1) * bw)
        proj = summed([0, 1], z, c)
        moved = proj[:, :bw].astype(BF16)
        conv_v[conv_in.shape[0] - 1, :, cs] = moved
        taps = conv_w[:, cs].astype(F32)
        hist = conv_in[0, :, cs].astype(F32) * taps[0:1]
        for i in range(1, 3):
            hist = hist + conv_in[i, :, cs].astype(F32) * taps[i:i + 1]
        conv = (hist + moved.astype(F32) * taps[3:4]).astype(BF16)
        rate = jax.nn.sigmoid(dot(conv, wrate[c]))
        in_gate = jax.nn.sigmoid(dot(conv, winput[c]))
        log_decay = -8.0 * rate * jnp.log1p(jnp.exp(-rate_param[:, cs]))
        th = jnp.tanh(log_decay)
        rest = -2.0 * th / (1.0 - th)
        state = jnp.exp(log_decay) * state_in[:, cs] + jnp.sqrt(rest) * in_gate * conv.astype(F32)
        state_v[:, cs] = state
        gated[:, cs] = (state * jax.nn.gelu(proj[:, bw:], approximate=True)).astype(BF16)
        if c < nc - 1:
            for i in range(p):
                for h in range(HALVES):
                    lo = i * share + h * sw
                    piece = dot(gated[:, cs], wout[cs, lo:lo + sw])
                    oacc[i, h] = piece if c == 0 else oacc[i, h] + piece

    last = slice((nc - 1) * bw, nc * bw)

    def out_part(i, h):
        piece = dot(gated[:, last], wout[last, block(i, h)])
        return oacc[i, h] + piece if nc > 1 else piece

    def copy_d1(yy, h):
        return remote(op_p.at[yy, h], op_r.at[yy, h], sd1, rd1.at[yy, h], {"tp": q})

    def copy_d2(dy, h):
        ty = lax.rem(y + dy, ys)
        return remote(hs.at[ty, h], hr.at[y, h], sd2, rd2.at[dy - 1, h], {"tp": ty * 2 + core})

    def out_parts(dys):
        for yy in [lax.rem(y + dy, ys) for dy in dys]:
            for h in range(HALVES):
                op_p[yy, h] = out_part(yy * 2 + 1 - core, h).astype(BF16)
                copy_d1(yy, h).start()
        for yy in [lax.rem(y + dy, ys) for dy in dys]:
            for h in range(HALVES):
                op_o[yy, h] = out_part(yy * 2 + core, h)

    out_parts(range(1, ys))
    out_parts([0])
    for h in range(HALVES):
        for dy in range(1, ys):
            ty = lax.rem(y + dy, ys)
            copy_d1(ty, h).wait_recv()
            hs[ty, h] = (op_o[ty, h] + op_r[ty, h].astype(F32)).astype(BF16)
            copy_d2(dy, h).start()

    puts = [
        pltpu.make_async_copy(a, b, osem.at[i])
        for i, (a, b) in enumerate([(state_v, state_out), (conv_v, conv_out), (layer_v, layer_out)])
    ]
    puts[0].start()
    puts[1].start()

    def copy_c1(peer, h):
        return remote(sd.at[h, peer], rows.at[h, t, e], sc1, rc1.at[e, h], {"ep": peer})

    def landed_c1(src, h):
        return remote(sd.at[h, src], rows.at[h, t, src], sc1, rc1.at[src, h], {"ep": src})

    def copy_c2(dy, src, h):
        to = lax.rem(y + dy, ys) * 2 + core
        return remote(rows.at[h, t, src], rows.at[h, t, src], sc2, rc2.at[dy - 1, src, h], {"tp": to})

    def landed_c2(dy, src, h):
        held = lax.rem(y - dy + ys, ys) * 2 + core
        return remote(
            rows.at[h, held, src], rows.at[h, held, src], sc2, rc2.at[dy - 1, src, h], {"tp": held}
        )

    def copy_c3(dy, src, h):
        held = lax.rem(y - dy + ys, ys) * 2 + core
        return remote(
            rows.at[h, held, src], rows.at[h, held, src], sc3, rc3.at[h], {"tp": q}
        )

    for h in range(HALVES):
        copy_d1(y, h).wait_recv()
        total = tokens[:, block(t, h)].astype(F32) + op_o[y, h] + op_r[y, h].astype(F32)
        for dy in range(1, ys):
            copy_d2(dy, h).wait_recv()
            total = total + hr[lax.rem(y - dy + ys, ys), h].astype(F32)
        mixed[h] = total
        sent = dot(dispatch, total.astype(BF16)).reshape(n, cap, sw).astype(BF16)
        sd[h] = sent
        for dx in range(1, nx):
            copy_c1(peer_of(z, dx), h).start()

        @pl.loop(0, nz - 1)
        def _(j):
            for dx in range(nx):
                copy_c1(peer_of(across(j), dx), h).start()

        rows[h, t, e] = sd[h, e]
        for dy in range(1, ys):
            copy_c2(dy, e, h).start()
        copy_c3(0, e, h).start()

    gs = min(n, max(1, 64 // cap))
    span = gs * cap
    hidden = hid.shape[1]
    fc = min(256, hidden)

    def scaled_rows(h):
        mate = rows.at[h, pl.ds(0, ys)]
        remote(mate, mate, sc3, rc3.at[h], {"tp": q}).wait_recv()

        @pl.loop(0, n // gs)
        def _(g):
            at = pl.ds(pl.multiple_of(g * span, span), span)
            acc = jnp.zeros((span, 1), F32)
            for i in range(p):
                lo = i * share + h * sw
                v = rows[h, i, pl.ds(g * gs, gs)].astype(F32).reshape(span, sw)
                acc = acc + jnp.sum(v * v, axis=1, keepdims=True)
                xn[h, at, i * sw:(i + 1) * sw] = (v * moe_gain[:, lo:lo + sw]).astype(BF16)
            ssq[at, :] = acc if h == 0 else ssq[at, :] + acc

    def partial_dot(weight, h, cs):
        acc = None
        for i in range(p):
            lo = i * share + h * sw
            piece = dot(xn[h, :, i * sw:(i + 1) * sw], weight[lo:lo + sw, cs])
            acc = piece if acc is None else acc + piece
        return acc

    def early(k, weight, f):
        cs = slice(f * fc, (f + 1) * fc)
        gacc[k, :, cs] = partial_dot(weight, 0, cs)

    def first_half():
        loads[5].wait()
        loads[6].wait()
        scaled_rows(0)

    tasks = [first_half]
    for f in range(hidden // fc):
        tasks.append(functools.partial(early, 0, weg, f))
        tasks.append(functools.partial(early, 1, weu, f))

    groups = [[peer_of(z, dx) for dx in range(1, nx)]]
    groups = groups + [[peer_of(across(j), dx) for dx in range(nx)] for j in reversed(range(nz - 1))]
    steps = []
    for k in range(nz + 1):
        steps = steps + [(src, 0) for src in (groups[k] if k < nz else [])]
        steps = steps + [(src, 1) for src in (groups[k - 1] if k else [])]
    queue = [(e, h) for h in range(HALVES)]

    def pass_on():
        src, h = queue.pop(0)
        for dy in range(1, ys):
            landed_c2(dy, src, h).wait_recv()
            copy_c3(dy, src, h).start()

    for src, h in steps:
        landed_c1(src, h).wait_recv()
        for dy in range(1, ys):
            copy_c2(dy, src, h).start()
        copy_c3(0, src, h).start()
        queue.append((src, h))
        if len(queue) > LAG:
            pass_on()
    while queue:
        pass_on()
        if tasks:
            tasks.pop(0)()
    for task in tasks:
        task()

    scaled_rows(HALVES - 1)
    row_scale = lax.rsqrt(ssq[...] / width + 1e-06)
    for f in range(hidden // fc):
        cs = slice(f * fc, (f + 1) * fc)
        gate_part = (gacc[0, :, cs] + partial_dot(weg, 1, cs)) * row_scale
        up_part = (gacc[1, :, cs] + partial_dot(weu, 1, cs)) * row_scale
        hid[:, cs] = (jax.nn.silu(gate_part) * up_part).astype(BF16)

    loads[7].wait()
    chunk = nx * cap

    def copy_e1(plane, yy, h):
        return remote(e_p.at[plane, yy, h], e_r.at[plane, yy, h], se1, re1.at[plane, yy, h], {"tp": q})

    def copy_e2(plane, dy, h):
        ty = lax.rem(y + dy, ys)
        return remote(
            es.at[plane, ty, h], er.at[plane, y, h], se2, re2.at[plane, dy - 1, h],
            {"tp": ty * 2 + core},
        )

    def copy_e3(peer, h):
        return remote(outb.at[h, peer], ret.at[h, e], se3, re3.at[h], {"ep": peer})

    def issue(planes, dys):
        mine = jnp.concatenate([hid[pl.ds(pl.multiple_of(k * chunk, chunk), chunk), :] for k in planes], axis=0)
        for dy in dys:
            ty = lax.rem(y + dy, ys)
            for h in range(HALVES):
                value = dot(mine, wed[:, block(ty * 2 + 1 - core, h)]).astype(BF16)
                for i, k in enumerate(planes):
                    e_p[k, ty, h] = value[i * chunk:(i + 1) * chunk]
                    copy_e1(k, ty, h).start()
            for h in range(HALVES):
                value = dot(mine, wed[:, block(ty * 2 + core, h)])
                for i, k in enumerate(planes):
                    e_o[k, ty, h] = value[i * chunk:(i + 1) * chunk]

    def push(plane):
        for dy in range(1, ys):
            ty = lax.rem(y + dy, ys)
            for h in range(HALVES):
                copy_e1(plane, ty, h).wait_recv()
                es[plane, ty, h] = (e_o[plane, ty, h] + e_r[plane, ty, h].astype(F32)).astype(BF16)
                copy_e2(plane, dy, h).start()

    def deliver(plane, first):
        for h in range(HALVES):
            copy_e1(plane, y, h).wait_recv()
            result = e_o[plane, y, h] + e_r[plane, y, h].astype(F32)
            for dy in range(1, ys):
                copy_e2(plane, dy, h).wait_recv()
                result = result + er[plane, lax.rem(y - dy + ys, ys), h].astype(F32)
            result = result.reshape(nx, cap, sw).astype(BF16)
            outb[h, pl.ds(plane * nx, nx)] = result
            for dx in range(first, nx):
                copy_e3(peer_of(plane, dx), h).start()

    order = [across(j) for j in range(nz - 1)] + [z]
    pairs = [order[i:i + 2] for i in range(0, nz, 2)]
    for planes in pairs:
        issue(planes, range(1, ys))
        issue(planes, [0])
        for plane in planes:
            push(plane)

    @pl.loop(0, nz - 1)
    def _(j):
        deliver(across(j), 0)

    deliver(z, 1)
    for h in range(HALVES):
        ret[h, e] = outb[h, e]

    def combine(weights, back):
        return lax.dot_general(weights, back, (((0,), (0,)), ((), ())), preferred_element_type=F32)

    for h in range(HALVES):
        others = ret.at[h, pl.ds(0, n - 1)]
        remote(others, others, se3, re3.at[h], {"ep": peer_of(z, 1)}).wait_recv()
        back = ret[h].astype(F32).reshape(slots, sw).astype(BF16)
        layer_v[:, h * sw:(h + 1) * sw] = (
            mixed[h] + combine(comb_hi, back) + combine(comb_lo, back)
        ).astype(BF16)

    puts[2].start()

    def drain(ref, sem):
        remote(ref, ref, sem, ra.at[0], {"tp": q}).wait_send()

    drain(normed.at[pl.ds(0, n - 1), half], sa)
    drain(cols.at[pl.ds(0, n - 1), half], sa2)
    if paired:
        @pl.when(middle)
        def _():
            drain(part.at[pl.ds(0, nz - 1), pl.ds(0, nx - 1)], sb)
            drain(part.at[0, pl.ds(0, nx - 1), pl.ds(0, late)], sb)
            drain(zf, szf)

        @pl.when(jnp.logical_not(middle))
        def _():
            drain(part.at[:, pl.ds(0, nx - 1)], sb)
    else:
        drain(part.at[:, pl.ds(0, nx - 1)], sb)
    drain(zsend.at[pl.ds(0, nz - 1)], sz)
    drain(op_p, sd1)
    drain(hs.at[pl.ds(0, ys - 1)], sd2)
    drain(sd.at[:, pl.ds(0, n - 1)], sc1)
    drain(rows.at[:, pl.ds(0, ys - 1)], sc2)
    drain(rows.at[:, pl.ds(0, ys)], sc3)
    drain(e_p, se1)
    drain(es.at[:, pl.ds(0, ys - 1)], se2)
    drain(outb.at[:, pl.ds(0, n - 1)], se3)

    for put in puts:
        put.wait()


def finish(layer_in, state_in, conv_in, layer_out, state_out, conv_out):
    layer_out[...] = layer_in[...]
    state_out[...] = state_in[...]
    conv_out[...] = conv_in[...]


def shards(
    n, p,
    tokens, state_in, conv_in, mix_gain, rnn_weight, gate_weight, conv_weight, rate_weight,
    input_weight, rate_param, out_weight, moe_gain, expert_gate, expert_up, expert_down, routes, route_prob,
):
    g, width = tokens.shape
    depth, chans = rnn_weight.shape
    share = width // p
    cap = max(2, 2 * g * routes.shape[1] // n)
    slots = n * cap
    hidden = expert_gate.shape[2]
    ys = p // 2
    nx = 1 << ((n.bit_length() - 1) // 2)
    nx = nx if n % nx == 0 else 1
    nz = n // nx
    nc, cw = rate_weight.shape[0], 2 * rate_weight.shape[1]
    nh, sw = HALVES, share // HALVES
    chunk = nx * cap
    vm = pl.BlockSpec(memory_space=pltpu.VMEM)
    hb = pl.BlockSpec(memory_space=pl.ANY)
    dma = pltpu.SemaphoreType.DMA
    V = pltpu.VMEM
    small = (
        tokens, state_in, jnp.transpose(conv_in, (1, 0, 2)), mix_gain.reshape(-1, 128), moe_gain.reshape(-1, 128),
        conv_weight, rate_param[None], routes.T, route_prob.T,
    )
    scratch = [V(a.shape, a.dtype) for a in small] + [
        V((g, share), BF16), V((g, chans), F32), V((conv_in.shape[1], g, chans), BF16),
        V((depth, chans), BF16), V((depth, chans), BF16),
        V(rate_weight.shape, BF16), V(input_weight.shape, BF16), V(out_weight.shape, BF16),
        V(expert_gate.shape[1:], BF16), V(expert_up.shape[1:], BF16), V(expert_down.shape[1:], BF16),
        V((1, width), F32), V((1, width), F32),
        V((n, g, depth), BF16), V((n, g, depth), BF16),
        V((nz, nx, nc, g, cw), BF16), V((nz, nx, nc, g, cw), BF16),
        V((nz, nc, g, cw), BF16), V((2, nz, nc, g, cw), BF16), V((nx - 1, nc - nc // 2, g, cw), BF16),
        V((g, chans), BF16), V((p, nh, g, sw), F32),
        V((ys, nh, g, sw), BF16), V((ys, nh, g, sw), F32), V((ys, nh, g, sw), BF16),
        V((ys, nh, g, sw), BF16), V((ys, nh, g, sw), BF16), V((nh, g, sw), F32),
        V((nh, n, cap, sw), BF16), V((nh, p, n, cap, sw), BF16), V((nh, slots, p * sw), BF16), V((slots, 1), F32),
        V((2, slots, hidden), F32), V((slots, hidden), BF16),
        V((nz, ys, nh, chunk, sw), BF16), V((nz, ys, nh, chunk, sw), F32), V((nz, ys, nh, chunk, sw), BF16),
        V((nz, ys, nh, chunk, sw), BF16), V((nz, ys, nh, chunk, sw), BF16),
        V((nh, n, cap, sw), BF16), V((nh, n, cap, sw), BF16),
        dma((8,)), dma((len(small),)), dma((3,)),
        dma, dma((n,)), dma, dma((n,)),
        dma, dma((nz, nx - 1, nc)), dma, dma((2, nz, nc)), dma, dma((nx - 1, nc - nc // 2)),
        dma, dma((ys, nh)), dma, dma((ys - 1, nh)),
        dma, dma((n, nh)), dma, dma((ys - 1, n, nh)), dma, dma((nh,)),
        dma, dma((nz, ys, nh)), dma, dma((nz, ys - 1, nh)), dma, dma((nh,)),
    ]
    outs = (
        jax.ShapeDtypeStruct((g, share), BF16),
        jax.ShapeDtypeStruct((g, chans), F32),
        jax.ShapeDtypeStruct((conv_in.shape[1], g, chans), BF16),
    )
    held = pl.pallas_call(
        functools.partial(kernel, n, p, nx, cap),
        out_shape=outs,
        in_specs=[hb] * 17,
        out_specs=(hb, hb, hb),
        scratch_shapes=scratch,
        compiler_params=pltpu.CompilerParams(
            collective_id=0, has_side_effects=True, vmem_limit_bytes=60 * 1024 * 1024
        ),
    )(
        *small,
        rnn_weight, gate_weight, rate_weight, input_weight, out_weight, expert_gate, expert_up, expert_down,
    )
    layer_out, state_out, conv_out = pl.pallas_call(
        finish,
        out_shape=outs,
        in_specs=[vm] * 3,
        out_specs=(vm, vm, vm),
    )(*held)
    return (layer_out, state_out, jnp.transpose(conv_out, (1, 0, 2)))


def solution(mesh):
    in_specs = (
        P("ep", None),
        P("ep", "tp"),
        P("ep", None, "tp"),
        P(),
        P("ep", "tp"),
        P("ep", "tp"),
        P(None, "tp"),
        P("tp", None, None),
        P("tp", None, None),
        P("tp"),
        P("tp", None),
        P(),
        P("ep", None, "tp"),
        P("ep", None, "tp"),
        P("ep", "tp", None),
        P("ep", None),
        P("ep", None),
    )
    out_specs = (P("ep", "tp"), P("ep", "tp"), P("ep", None, "tp"))
    body = functools.partial(shards, mesh.shape["ep"], mesh.shape["tp"])
    return jax.shard_map(body, mesh=mesh, in_specs=in_specs, out_specs=out_specs, check_vma=False)
```

```python
import functools

import jax
import jax.numpy as jnp
from jax import lax
from jax.experimental import pallas as pl
from jax.experimental.pallas import tpu as pltpu
from jax.sharding import PartitionSpec as P

MESH = pl.DeviceIdType.MESH
F32 = jnp.float32
BF16 = jnp.bfloat16
HALVES = 2


def dot(a, b):
    return jnp.dot(a, b, preferred_element_type=F32)


def remote(src, dst, send, recv, where):
    return pltpu.make_async_remote_copy(
        src_ref=src, dst_ref=dst, send_sem=send, recv_sem=recv, device_id=where, device_id_type=MESH
    )


def kernel(
    n, p, nx, cap,
    tokens_h, state_h, conv_h, mix_h, moe_h, taps_h, param_h, routes_h, prob_h,
    rnn_h, gate_h, rate_h, input_h, out_h, eg_h, eu_h, ed_h,
    layer_out, state_out, conv_out,
    tokens, state_in, conv_in, mix_gain_in, moe_gain_in, conv_w, rate_param, routes, prob,
    layer_v, state_v, conv_v,
    wr, wg, wrate, winput, wout, weg, weu, wed,
    mix_gain, moe_gain, normed, cols, part, bx, zsend, rz, zf, gated, oacc,
    op_p, op_o, op_r, hs, hr, mixed,
    mb, ag, sdo, sd, rows, xn, ssq, gacc, hid, e_p, e_o, e_r, es, er, outb, ret,
    wsem, lsem, osem, sa, ra, sa2, ra2, sb, rb, sz, rzs, szf, rzf, sd1, rd1, sd2, rd2,
    sag, rag, sco, sc1, rc1, sc2, rc2, sc3, rc3, se1, re1, se2, re2, ro2, se3, re3,
):
    e = lax.axis_index("ep")
    t = lax.axis_index("tp")
    core = lax.rem(t, 2)
    y = t // 2
    q = t + 1 - 2 * core
    ys = p // 2
    nz = n // nx
    z = e // nx
    x = lax.rem(e, nx)

    rows_g, width = tokens.shape
    depth = width // n
    share = width // p
    sw = share // HALVES
    slots = n * cap

    small = [
        pltpu.make_async_copy(a, b, lsem.at[i])
        for i, (a, b) in enumerate(
            [(tokens_h, tokens), (mix_h, mix_gain_in), (moe_h, moe_gain_in), (routes_h, routes), (prob_h, prob),
             (taps_h, conv_w), (param_h, rate_param), (conv_h, conv_in), (state_h, state_in)]
        )
    ]
    loads = [
        pltpu.make_async_copy(a, b, wsem.at[i])
        for i, (a, b) in enumerate(
            [(rnn_h, wr), (gate_h, wg), (rate_h, wrate), (input_h, winput), (out_h, wout),
             (eg_h.at[0], weg), (eu_h.at[0], weu), (ed_h.at[0], wed)]
        )
    ]
    small[0].start()
    small[1].start()

    barrier = pltpu.get_barrier_semaphore()

    @pl.loop(1, n)
    def _(d):
        pl.semaphore_signal(barrier, inc=1, device_id={"ep": lax.rem(e + d, n)}, device_id_type=MESH)

    @pl.loop(1, p)
    def _(d):
        pl.semaphore_signal(barrier, inc=1, device_id={"tp": lax.rem(t + d, p)}, device_id_type=MESH)

    for load in small[2:] + loads[:4]:
        load.start()

    @pl.when(z == 0)
    def _():
        rz[0] = jnp.zeros(rz.shape[1:], BF16)

    @pl.when(z == nz - 1)
    def _():
        rz[1] = jnp.zeros(rz.shape[1:], BF16)

    small[0].wait()
    small[1].wait()
    nc, bw = rate_h.shape[0], rate_h.shape[1]
    late = nc // 2
    paired = nz % 2 == 0 and nz > 2
    middle = (z == nz // 2) | (z == nz // 2 - 1)
    opposite = nz - 1 - z
    if paired:
        @pl.when(middle)
        def _():
            for dx in range(1, nx):
                bx[opposite, dx, late:] = jnp.zeros((nc - late,) + bx.shape[3:], BF16)

    for j in range(width // 128):
        cs = slice(j * 128, (j + 1) * 128)
        mix_gain[:, cs] = mix_gain_in[j:j + 1, :].astype(F32)

    total_sq = jnp.zeros((rows_g, 1), F32)
    for j in range(n):
        v = tokens[:, j * depth:(j + 1) * depth].astype(F32)
        total_sq = total_sq + jnp.sum(v * v, axis=1, keepdims=True)
    scale = lax.rsqrt(total_sq / width + 1e-06)
    for j in range(n):
        cs = slice(j * depth, (j + 1) * depth)
        normed[j] = (tokens[:, cs].astype(F32) * scale * mix_gain[:, cs]).astype(BF16)

    pl.semaphore_wait(barrier, n + p - 2)

    half = pl.ds(pl.multiple_of(core * (rows_g // 2), rows_g // 2), rows_g // 2)
    high = (2 * z) // nz
    folded = z + high * (nz - 1 - 2 * z)

    lead = nz - 1 - 2 * folded

    def across(j):
        plane = nz - 1 - j
        plane = plane - (folded >= plane).astype(jnp.int32)
        return plane + high * (nz - 1 - 2 * plane)

    def far(j):
        ahead = (j < lead).astype(jnp.int32)
        k = (1 - ahead) * (j - lead)
        turn = folded + (folded - k // 2) * (2 * lax.rem(k, 2) - 1)
        plane = ahead * (nz - 1 - j) + (1 - ahead) * turn
        return plane + high * (nz - 1 - 2 * plane)

    def beside(dx):
        return lax.rem(x + dx, nx)

    def peer_of(plane, dx):
        return plane * nx + beside(dx)

    def copy_a(peer):
        return remote(normed.at[peer, half], cols.at[e, half], sa, ra.at[z], {"ep": peer})

    def copy_a2(src, plane):
        return remote(cols.at[src, half], cols.at[src, half], sa2, ra2.at[plane], {"tp": q})

    def landed(plane, count, sem):
        block = cols.at[pl.ds(0, count), half]
        remote(block, block, sa, sem.at[plane], {"tp": q}).wait_recv()

    for dx in range(1, nx):
        copy_a(peer_of(z, dx)).start()

    @pl.loop(0, nz - 1)
    def _(j):
        for dx in range(nx):
            copy_a(peer_of(across(j), dx)).start()

    cols[e] = normed[e]

    for j in range(2, 5):
        small[j].wait()
    for j in range(width // 128):
        cs = slice(j * 128, (j + 1) * 128)
        moe_gain[:, cs] = moe_gain_in[j:j + 1, :].astype(F32)
    ids = routes[...]
    sub_e = lax.broadcasted_iota(jnp.int32, (n, rows_g), 0)
    named = [(ids[k:k + 1, :] == sub_e).astype(F32) for k in range(ids.shape[0])]
    member = functools.reduce(lambda a, b: a + b, named)
    earlier = (
        lax.broadcasted_iota(jnp.int32, (rows_g, rows_g), 0)
        < lax.broadcasted_iota(jnp.int32, (rows_g, rows_g), 1)
    ).astype(F32)
    before = dot(member.astype(BF16), earlier.astype(BF16))
    sub_s = lax.broadcasted_iota(jnp.int32, (slots, rows_g), 0).astype(F32)
    total_prob = jnp.sum(prob[...], axis=0, keepdims=True)
    dispatch = jnp.zeros((slots, rows_g), F32)
    comb = jnp.zeros((slots, rows_g), F32)
    for k in range(ids.shape[0]):
        slot = jnp.sum(before * named[k], axis=0, keepdims=True)
        target = ids[k:k + 1, :].astype(F32) * cap + slot
        hit = (sub_s == target).astype(F32)
        dispatch = dispatch + hit
        comb = comb + hit * (prob[k:k + 1, :] / total_prob)
    dispatch = dispatch.astype(BF16)
    comb_hi = comb.astype(BF16)
    comb_lo = (comb - comb_hi.astype(F32)).astype(BF16)

    loads[0].wait()
    loads[1].wait()
    for load in loads[4:]:
        load.start()

    def copy_x(plane, dx, c):
        return remote(
            part.at[plane, beside(dx), c], bx.at[plane, dx, c], sb, rb.at[plane, dx - 1, c],
            {"ep": peer_of(z, dx)},
        )

    def copy_f(dx, c):
        return remote(
            part.at[opposite, beside(dx), c], zf.at[dx - 1, c - late], szf, rzf.at[dx - 1, c - late],
            {"ep": opposite * nx + x},
        )

    def by_line(plane, c):
        return middle & (plane == opposite) if paired and c >= late else None

    def unless(flag, action):
        if flag is None:
            action()
        else:
            pl.when(jnp.logical_not(flag))(action)

    def project(plane, last, own):
        first = 1 if own else 0
        if nx > first:
            landed(plane, nx - first, ra)
            for dx in range(first, nx):
                copy_a2(peer_of(plane, dx), plane).start()
            landed(plane, nx - first, ra2)
        feats = cols[pl.ds(plane * nx, nx)].reshape(nx * rows_g, depth)
        for c in range(nc):
            cs = slice(c * bw, (c + 1) * bw)
            for lo, weight in ((0, wr), (bw, wg)):
                value = dot(feats, weight[:, cs]).astype(BF16)
                for i in range(nx):
                    part[plane, i, c, :, lo:lo + bw] = value[i * rows_g:(i + 1) * rows_g]
            if c < last:
                flag = None if own else by_line(plane, c)
                for dx in range(1, nx):
                    unless(flag, copy_x(plane, dx, c).start)
                    if flag is not None:
                        pl.when(flag)(copy_f(dx, c).start)

    project(z, late, True)

    @pl.loop(0, nz - 1)
    def _(j):
        project(far(j), nc, False)

    def rest_of_own():
        for c in range(late, nc):
            for dx in range(1, nx):
                if paired:
                    @pl.when(middle)
                    def _():
                        copy_f(dx, c).wait_recv()
                        mine = part[z, beside(dx), c].astype(F32)
                        part[z, beside(dx), c] = (mine + zf[dx - 1, c - late].astype(F32)).astype(BF16)

                copy_x(z, dx, c).start()

    def copy_z(side, plane, c, at=None):
        to = z + 1 - 2 * side
        slot = plane + side * ((to if at is None else at) == plane).astype(jnp.int32) * (nz - plane)
        return remote(
            zsend.at[plane, c], rz.at[side, plane, c], sz, rzs.at[slot, c],
            {"ep": to * nx + x},
        )

    def summed(sides, plane, c):
        for dx in range(1, nx):
            unless(by_line(plane, c) if len(sides) == 1 else None, copy_x(plane, dx, c).wait_recv)
        total = part[plane, x, c].astype(F32)
        for dx in range(1, nx):
            total = total + bx[plane, dx, c].astype(F32)
        for s in sides:
            origin = z - 1 + 2 * s

            @pl.when((origin >= 0) & (origin < nz))
            def _():
                copy_z(s, plane, c, z).wait_recv()

            total = total + rz[s, plane, c].astype(F32)
        return total

    def line_step(j):
        plane = far(j)
        side = (plane < z).astype(jnp.int32)
        for c in range(nc):
            zsend[plane, c] = summed([side], plane, c).astype(BF16)
            copy_z(side, plane, c).start()

    if nz > 1:
        line_step(jnp.int32(0))
    rest_of_own()
    if nz > 1:
        pl.loop(1, nz - 1)(line_step)

    def block(i, h):
        return pl.ds(pl.multiple_of(i * share + h * sw, sw), sw)

    for load in small[5:]:
        load.wait()
    loads[2].wait()
    loads[3].wait()
    loads[4].wait()
    for i in range(1, conv_in.shape[0]):
        conv_v[i - 1] = conv_in[i]
    for c in range(nc):
        cs = slice(c * bw, (c + 1) * bw)
        proj = summed([0, 1], z, c)
        moved = proj[:, :bw].astype(BF16)
        conv_v[conv_in.shape[0] - 1, :, cs] = moved
        taps = conv_w[:, cs].astype(F32)
        hist = conv_in[0, :, cs].astype(F32) * taps[0:1]
        for i in range(1, 3):
            hist = hist + conv_in[i, :, cs].astype(F32) * taps[i:i + 1]
        conv = (hist + moved.astype(F32) * taps[3:4]).astype(BF16)
        rate = jax.nn.sigmoid(dot(conv, wrate[c]))
        in_gate = jax.nn.sigmoid(dot(conv, winput[c]))
        log_decay = -8.0 * rate * jnp.log1p(jnp.exp(-rate_param[:, cs]))
        th = jnp.tanh(log_decay)
        rest = -2.0 * th / (1.0 - th)
        state = jnp.exp(log_decay) * state_in[:, cs] + jnp.sqrt(rest) * in_gate * conv.astype(F32)
        state_v[:, cs] = state
        gated[:, cs] = (state * jax.nn.gelu(proj[:, bw:], approximate=True)).astype(BF16)
        if c < nc - 1:
            for i in range(p):
                for h in range(HALVES):
                    lo = i * share + h * sw
                    piece = dot(gated[:, cs], wout[cs, lo:lo + sw])
                    oacc[i, h] = piece if c == 0 else oacc[i, h] + piece

    last = slice((nc - 1) * bw, nc * bw)

    def out_part(i, h):
        piece = dot(gated[:, last], wout[last, block(i, h)])
        return oacc[i, h] + piece if nc > 1 else piece

    def copy_d1(yy, h):
        return remote(op_p.at[yy, h], op_r.at[yy, h], sd1, rd1.at[yy, h], {"tp": q})

    def copy_d2(dy, h):
        ty = lax.rem(y + dy, ys)
        return remote(hs.at[ty, h], hr.at[y, h], sd2, rd2.at[dy - 1, h], {"tp": ty * 2 + core})

    def out_parts(dys):
        for yy in [lax.rem(y + dy, ys) for dy in dys]:
            for h in range(HALVES):
                op_p[yy, h] = out_part(yy * 2 + 1 - core, h).astype(BF16)
                copy_d1(yy, h).start()
        for yy in [lax.rem(y + dy, ys) for dy in dys]:
            for h in range(HALVES):
                op_o[yy, h] = out_part(yy * 2 + core, h)

    out_parts(range(1, ys))
    out_parts([0])
    for h in range(HALVES):
        for dy in range(1, ys):
            ty = lax.rem(y + dy, ys)
            copy_d1(ty, h).wait_recv()
            hs[ty, h] = (op_o[ty, h] + op_r[ty, h].astype(F32)).astype(BF16)
            copy_d2(dy, h).start()

    puts = [
        pltpu.make_async_copy(a, b, osem.at[i])
        for i, (a, b) in enumerate([(state_v, state_out), (conv_v, conv_out), (layer_v, layer_out)])
    ]
    puts[0].start()
    puts[1].start()

    def copy_c1(peer, h):
        return remote(sd.at[h, peer], rows.at[h, t, e], sc1, rc1.at[e, h], {"ep": peer})

    def landed_c1(src, h):
        return remote(sd.at[h, src], rows.at[h, t, src], sc1, rc1.at[src, h], {"ep": src})

    def copy_c2(dy, src, h):
        to = lax.rem(y + dy, ys) * 2 + core
        return remote(rows.at[h, t, src], rows.at[h, t, src], sc2, rc2.at[dy - 1, src, h], {"tp": to})

    def landed_c2(dy, src, h):
        held = lax.rem(y - dy + ys, ys) * 2 + core
        return remote(
            rows.at[h, held, src], rows.at[h, held, src], sc2, rc2.at[dy - 1, src, h], {"tp": held}
        )

    def copy_c3(dy, src, h):
        held = lax.rem(y - dy + ys, ys) * 2 + core
        return remote(
            rows.at[h, held, src], rows.at[h, held, src], sc3, rc3.at[h], {"tp": q}
        )

    def copy_g(dy, h):
        ty = lax.rem(y + dy, ys)
        return remote(mb.at[h], ag.at[y, h], sag, rag.at[dy - 1, h], {"tp": ty * 2 + core})

    def copy_o(dy, peer, h):
        held = lax.rem(y - dy + ys, ys) * 2 + core
        return remote(sdo.at[dy - 1, h, peer], rows.at[h, held, e], sco, rc2.at[dy - 1, e, h], {"ep": peer})

    def landed_o(dy, src, h):
        held = lax.rem(y - dy + ys, ys) * 2 + core
        return remote(sdo.at[dy - 1, h, src], rows.at[h, held, src], sco, rc2.at[dy - 1, src, h], {"ep": src})

    ncross = nz // 2 if nz % 2 == 0 else nz - 1
    beyond = [[peer_of(across(j), dx) for dx in range(nx)] for j in reversed(range(ncross))]
    near = [peer_of(z, dx) for dx in range(1, nx)]
    near = near + [peer_of(across(j), dx) for j in range(ncross, nz - 1) for dx in range(nx)]

    for h in range(HALVES):
        copy_d1(y, h).wait_recv()
        total = tokens[:, block(t, h)].astype(F32) + op_o[y, h] + op_r[y, h].astype(F32)
        for dy in range(1, ys):
            copy_d2(dy, h).wait_recv()
            total = total + hr[lax.rem(y - dy + ys, ys), h].astype(F32)
        mixed[h] = total
        mb[h] = total.astype(BF16)
        for dy in range(1, ys):
            copy_g(dy, h).start()
        sd[h] = dot(dispatch, mb[h]).reshape(n, cap, sw).astype(BF16)

        @pl.loop(0, ncross)
        def _(j):
            for dx in range(nx):
                copy_c1(peer_of(across(j), dx), h).start()

        for peer in near:
            copy_c1(peer, h).start()
        rows[h, t, e] = sd[h, e]
        copy_c3(0, e, h).start()

    gs = min(n, max(1, 64 // cap))
    span = gs * cap
    hidden = hid.shape[1]
    fc = min(256, hidden)

    def scaled_rows(h):
        mate = rows.at[h, pl.ds(0, ys)]
        remote(mate, mate, sc3, rc3.at[h], {"tp": q}).wait_recv()

        @pl.loop(0, n // gs)
        def _(g):
            at = pl.ds(pl.multiple_of(g * span, span), span)
            acc = jnp.zeros((span, 1), F32)
            for i in range(p):
                lo = i * share + h * sw
                v = rows[h, i, pl.ds(g * gs, gs)].astype(F32).reshape(span, sw)
                acc = acc + jnp.sum(v * v, axis=1, keepdims=True)
                xn[h, at, i * sw:(i + 1) * sw] = (v * moe_gain[:, lo:lo + sw]).astype(BF16)
            ssq[at, :] = acc if h == 0 else ssq[at, :] + acc

    def partial_dot(weight, h, cs):
        acc = None
        for i in range(p):
            lo = i * share + h * sw
            piece = dot(xn[h, :, i * sw:(i + 1) * sw], weight[lo:lo + sw, cs])
            acc = piece if acc is None else acc + piece
        return acc

    def early(k, weight, f):
        cs = slice(f * fc, (f + 1) * fc)
        gacc[k, :, cs] = partial_dot(weight, 0, cs)

    def first_half():
        loads[5].wait()
        loads[6].wait()
        scaled_rows(0)

    tasks = [first_half]
    for f in range(hidden // fc):
        tasks.append(functools.partial(early, 0, weg, f))
        tasks.append(functools.partial(early, 1, weu, f))

    def gathered(h):
        for dy in range(1, ys):
            origin = lax.rem(y - dy + ys, ys)
            copy_g(dy, h).wait_recv()
            sdo[dy - 1, h] = dot(dispatch, ag[origin, h]).reshape(n, cap, sw).astype(BF16)
            for peer in near:
                copy_o(dy, peer, h).start()
            rows[h, origin * 2 + core, e] = sdo[dy - 1, h, e]
            copy_c3(dy, e, h).start()

    def near_own(src, h):
        landed_c1(src, h).wait_recv()
        copy_c3(0, src, h).start()

    def near_other(src, h):
        for dy in range(1, ys):
            landed_o(dy, src, h).wait_recv()
            copy_c3(dy, src, h).start()

    def pass_on(src, h):
        for dy in range(1, ys):
            landed_c2(dy, src, h).wait_recv()
            copy_c3(dy, src, h).start()

    def cross(src, h):
        landed_c1(src, h).wait_recv()
        for dy in range(1, ys):
            copy_c2(dy, src, h).start()
        copy_c3(0, src, h).start()

    gathered(0)
    for h in range(HALVES):
        for i, group in enumerate(beyond):
            for src in group:
                cross(src, h)
            if h == 0 and i == 0:
                gathered(1)
            if h and i == 0:
                for src in near:
                    near_own(src, 0)
                    near_other(src, 0)
        if h == 0:
            for group in beyond[:-1]:
                for src in group:
                    pass_on(src, 0)
    for src in beyond[-1] if beyond else []:
        pass_on(src, 0)
    if not beyond:
        gathered(1)
        for src in near:
            near_own(src, 0)
            near_other(src, 0)
    rest = [functools.partial(near_own, src, 1) for src in near]
    rest = rest + [functools.partial(near_other, src, 1) for src in near]
    for step in rest:
        step()
    rest = [functools.partial(pass_on, src, 1) for group in beyond for src in group]
    while rest:
        tasks.pop(0)() if tasks else None
        rest.pop(0)()
    for task in tasks:
        task()

    scaled_rows(HALVES - 1)
    row_scale = lax.rsqrt(ssq[...] / width + 1e-06)
    for f in range(hidden // fc):
        cs = slice(f * fc, (f + 1) * fc)
        gate_part = (gacc[0, :, cs] + partial_dot(weg, 1, cs)) * row_scale
        up_part = (gacc[1, :, cs] + partial_dot(weu, 1, cs)) * row_scale
        hid[:, cs] = (jax.nn.silu(gate_part) * up_part).astype(BF16)

    loads[7].wait()
    chunk = nx * cap

    def copy_e1(plane, yy, h):
        return remote(e_p.at[plane, yy, h], e_r.at[plane, yy, h], se1, re1.at[plane, yy, h], {"tp": q})

    def copy_e2(plane, dy, h):
        ty = lax.rem(y + dy, ys)
        return remote(
            es.at[plane, ty, h], er.at[plane, y, h], se2, re2.at[plane, dy - 1, h],
            {"tp": ty * 2 + core},
        )

    def mine_of(dx):
        return pl.ds(pl.multiple_of(beside(dx) * cap, cap), cap)

    def copy_own(dy, dx, h):
        ty = lax.rem(y + dy, ys)
        return remote(
            es.at[z, ty, h, mine_of(dx)], er.at[z, y, h, mine_of(dx)], se2, ro2.at[dy - 1, dx, h],
            {"tp": ty * 2 + core},
        )

    own_order = [(dx, h) for dx in list(range(1, nx)) + [0] for h in range(HALVES)]

    def copy_e3(peer, h):
        return remote(outb.at[h, peer], ret.at[h, e], se3, re3.at[h], {"ep": peer})

    def issue(planes, dys):
        mine = jnp.concatenate([hid[pl.ds(pl.multiple_of(k * chunk, chunk), chunk), :] for k in planes], axis=0)
        for dy in dys:
            ty = lax.rem(y + dy, ys)
            for h in range(HALVES):
                value = dot(mine, wed[:, block(ty * 2 + 1 - core, h)]).astype(BF16)
                for i, k in enumerate(planes):
                    e_p[k, ty, h] = value[i * chunk:(i + 1) * chunk]
                    copy_e1(k, ty, h).start()
            for h in range(HALVES):
                value = dot(mine, wed[:, block(ty * 2 + core, h)])
                for i, k in enumerate(planes):
                    e_o[k, ty, h] = value[i * chunk:(i + 1) * chunk]

    def push(plane):
        for dy in range(1, ys):
            ty = lax.rem(y + dy, ys)
            for h in range(HALVES):
                copy_e1(plane, ty, h).wait_recv()
                es[plane, ty, h] = (e_o[plane, ty, h] + e_r[plane, ty, h].astype(F32)).astype(BF16)
                copy_e2(plane, dy, h).start()

    def push_own():
        for dy in range(1, ys):
            ty = lax.rem(y + dy, ys)
            for h in range(HALVES):
                copy_e1(z, ty, h).wait_recv()
            for dx, h in own_order:
                at = mine_of(dx)
                es[z, ty, h, at] = (e_o[z, ty, h, at] + e_r[z, ty, h, at].astype(F32)).astype(BF16)
                copy_own(dy, dx, h).start()

    def deliver_own():
        for h in range(HALVES):
            copy_e1(z, y, h).wait_recv()
        for dx, h in own_order:
            at = mine_of(dx)
            result = e_o[z, y, h, at] + e_r[z, y, h, at].astype(F32)
            for dy in range(1, ys):
                copy_own(dy, dx, h).wait_recv()
                result = result + er[z, lax.rem(y - dy + ys, ys), h, at].astype(F32)
            if dx:
                outb[h, peer_of(z, dx)] = result.astype(BF16)
                copy_e3(peer_of(z, dx), h).start()
            else:
                ret[h, e] = result.astype(BF16)

    def deliver(plane):
        for h in range(HALVES):
            copy_e1(plane, y, h).wait_recv()
            result = e_o[plane, y, h] + e_r[plane, y, h].astype(F32)
            for dy in range(1, ys):
                copy_e2(plane, dy, h).wait_recv()
                result = result + er[plane, lax.rem(y - dy + ys, ys), h].astype(F32)
            result = result.reshape(nx, cap, sw).astype(BF16)
            outb[h, pl.ds(plane * nx, nx)] = result
            for dx in range(nx):
                copy_e3(peer_of(plane, dx), h).start()

    order = [across(j) for j in range(nz - 1)] + [z]
    pairs = [order[i:i + 2] for i in range(0, nz, 2)]
    for planes in pairs:
        issue(planes, range(1, ys))
        issue(planes, [0])
        for plane in planes:
            push_own() if plane is z else push(plane)

    @pl.loop(0, nz - 1)
    def _(j):
        deliver(across(j))

    deliver_own()

    def combine(weights, back):
        return lax.dot_general(weights, back, (((0,), (0,)), ((), ())), preferred_element_type=F32)

    for h in range(HALVES):
        others = ret.at[h, pl.ds(0, n - 1)]
        remote(others, others, se3, re3.at[h], {"ep": peer_of(z, 1)}).wait_recv()
        back = ret[h].astype(F32).reshape(slots, sw).astype(BF16)
        layer_v[:, h * sw:(h + 1) * sw] = (
            mixed[h] + combine(comb_hi, back) + combine(comb_lo, back)
        ).astype(BF16)

    puts[2].start()

    def drain(ref, sem):
        remote(ref, ref, sem, ra.at[0], {"tp": q}).wait_send()

    drain(normed.at[pl.ds(0, n - 1), half], sa)
    drain(cols.at[pl.ds(0, n - 1), half], sa2)
    if paired:
        @pl.when(middle)
        def _():
            drain(part.at[pl.ds(0, nz - 1), pl.ds(0, nx - 1)], sb)
            drain(part.at[0, pl.ds(0, nx - 1), pl.ds(0, late)], sb)
            drain(zf, szf)

        @pl.when(jnp.logical_not(middle))
        def _():
            drain(part.at[:, pl.ds(0, nx - 1)], sb)
    else:
        drain(part.at[:, pl.ds(0, nx - 1)], sb)
    drain(zsend.at[pl.ds(0, nz - 1)], sz)
    drain(op_p, sd1)
    drain(hs.at[pl.ds(0, ys - 1)], sd2)
    drain(sd.at[:, pl.ds(0, n - 1)], sc1)
    drain(rows.at[:, pl.ds(0, ys - 1), pl.ds(0, n - 1 - len(near))], sc2)
    drain(ag.at[pl.ds(0, ys - 1)], sag)
    drain(sdo.at[:, :, pl.ds(0, len(near))], sco)
    drain(rows.at[:, pl.ds(0, ys)], sc3)
    drain(e_p, se1)
    drain(es.at[:, pl.ds(0, ys - 1)], se2)
    drain(outb.at[:, pl.ds(0, n - 1)], se3)

    for put in puts:
        put.wait()


def finish(layer_in, state_in, conv_in, layer_out, state_out, conv_out):
    layer_out[...] = layer_in[...]
    state_out[...] = state_in[...]
    conv_out[...] = conv_in[...]


def shards(
    n, p,
    tokens, state_in, conv_in, mix_gain, rnn_weight, gate_weight, conv_weight, rate_weight,
    input_weight, rate_param, out_weight, moe_gain, expert_gate, expert_up, expert_down, routes, route_prob,
):
    g, width = tokens.shape
    depth, chans = rnn_weight.shape
    share = width // p
    cap = max(2, 2 * g * routes.shape[1] // n)
    slots = n * cap
    hidden = expert_gate.shape[2]
    ys = p // 2
    nx = 1 << ((n.bit_length() - 1) // 2)
    nx = nx if n % nx == 0 else 1
    nz = n // nx
    nc, cw = rate_weight.shape[0], 2 * rate_weight.shape[1]
    nh, sw = HALVES, share // HALVES
    chunk = nx * cap
    vm = pl.BlockSpec(memory_space=pltpu.VMEM)
    hb = pl.BlockSpec(memory_space=pl.ANY)
    dma = pltpu.SemaphoreType.DMA
    V = pltpu.VMEM
    small = (
        tokens, state_in, jnp.transpose(conv_in, (1, 0, 2)), mix_gain.reshape(-1, 128), moe_gain.reshape(-1, 128),
        conv_weight, rate_param[None], routes.T, route_prob.T,
    )
    scratch = [V(a.shape, a.dtype) for a in small] + [
        V((g, share), BF16), V((g, chans), F32), V((conv_in.shape[1], g, chans), BF16),
        V((depth, chans), BF16), V((depth, chans), BF16),
        V(rate_weight.shape, BF16), V(input_weight.shape, BF16), V(out_weight.shape, BF16),
        V(expert_gate.shape[1:], BF16), V(expert_up.shape[1:], BF16), V(expert_down.shape[1:], BF16),
        V((1, width), F32), V((1, width), F32),
        V((n, g, depth), BF16), V((n, g, depth), BF16),
        V((nz, nx, nc, g, cw), BF16), V((nz, nx, nc, g, cw), BF16),
        V((nz, nc, g, cw), BF16), V((2, nz, nc, g, cw), BF16), V((nx - 1, nc - nc // 2, g, cw), BF16),
        V((g, chans), BF16), V((p, nh, g, sw), F32),
        V((ys, nh, g, sw), BF16), V((ys, nh, g, sw), F32), V((ys, nh, g, sw), BF16),
        V((ys, nh, g, sw), BF16), V((ys, nh, g, sw), BF16), V((nh, g, sw), F32),
        V((nh, g, sw), BF16), V((ys, nh, g, sw), BF16), V((ys - 1, nh, n, cap, sw), BF16),
        V((nh, n, cap, sw), BF16), V((nh, p, n, cap, sw), BF16), V((nh, slots, p * sw), BF16), V((slots, 1), F32),
        V((2, slots, hidden), F32), V((slots, hidden), BF16),
        V((nz, ys, nh, chunk, sw), BF16), V((nz, ys, nh, chunk, sw), F32), V((nz, ys, nh, chunk, sw), BF16),
        V((nz, ys, nh, chunk, sw), BF16), V((nz, ys, nh, chunk, sw), BF16),
        V((nh, n, cap, sw), BF16), V((nh, n, cap, sw), BF16),
        dma((8,)), dma((len(small),)), dma((3,)),
        dma, dma((nz,)), dma, dma((nz,)),
        dma, dma((nz, nx - 1, nc)), dma, dma((nz + 1, nc)), dma, dma((nx - 1, nc - nc // 2)),
        dma, dma((ys, nh)), dma, dma((ys - 1, nh)),
        dma, dma((ys - 1, nh)), dma,
        dma, dma((n, nh)), dma, dma((ys - 1, n, nh)), dma, dma((nh,)),
        dma, dma((nz, ys, nh)), dma, dma((nz, ys - 1, nh)), dma((ys - 1, nx, nh)), dma, dma((nh,)),
    ]
    outs = (
        jax.ShapeDtypeStruct((g, share), BF16),
        jax.ShapeDtypeStruct((g, chans), F32),
        jax.ShapeDtypeStruct((conv_in.shape[1], g, chans), BF16),
    )
    held = pl.pallas_call(
        functools.partial(kernel, n, p, nx, cap),
        out_shape=outs,
        in_specs=[hb] * 17,
        out_specs=(hb, hb, hb),
        scratch_shapes=scratch,
        compiler_params=pltpu.CompilerParams(
            collective_id=0, has_side_effects=True, vmem_limit_bytes=60 * 1024 * 1024
        ),
    )(
        *small,
        rnn_weight, gate_weight, rate_weight, input_weight, out_weight, expert_gate, expert_up, expert_down,
    )
    layer_out, state_out, conv_out = pl.pallas_call(
        finish,
        out_shape=outs,
        in_specs=[vm] * 3,
        out_specs=(vm, vm, vm),
    )(*held)
    return (layer_out, state_out, jnp.transpose(conv_out, (1, 0, 2)))


def solution(mesh):
    in_specs = (
        P("ep", None),
        P("ep", "tp"),
        P("ep", None, "tp"),
        P(),
        P("ep", "tp"),
        P("ep", "tp"),
        P(None, "tp"),
        P("tp", None, None),
        P("tp", None, None),
        P("tp"),
        P("tp", None),
        P(),
        P("ep", None, "tp"),
        P("ep", None, "tp"),
        P("ep", "tp", None),
        P("ep", None),
        P("ep", None),
    )
    out_specs = (P("ep", "tp"), P("ep", "tp"), P("ep", None, "tp"))
    body = functools.partial(shards, mesh.shape["ep"], mesh.shape["tp"])
    return jax.shard_map(body, mesh=mesh, in_specs=in_specs, out_specs=out_specs, check_vma=False)
```

```python
import functools

import jax
import jax.numpy as jnp
from jax import lax
from jax.experimental import pallas as pl
from jax.experimental.pallas import tpu as pltpu
from jax.sharding import PartitionSpec as P

MESH = pl.DeviceIdType.MESH
F32 = jnp.float32
BF16 = jnp.bfloat16
HALVES = 2


def dot(a, b):
    return jnp.dot(a, b, preferred_element_type=F32)


def remote(src, dst, send, recv, where):
    return pltpu.make_async_remote_copy(
        src_ref=src, dst_ref=dst, send_sem=send, recv_sem=recv, device_id=where, device_id_type=MESH
    )


def kernel(
    n, p, nx, cap,
    tokens_h, state_h, conv_h, mix_h, moe_h, taps_h, param_h, routes_h, prob_h,
    rnn_h, gate_h, rate_h, input_h, out_h, eg_h, eu_h, ed_h,
    layer_out, state_out, conv_out,
    tokens, state_in, conv_in, mix_gain_in, moe_gain_in, conv_w, rate_param, routes, prob,
    layer_v, state_v, conv_v,
    wr, wg, wrate, winput, wout, weg, weu, wed,
    mix_gain, moe_gain, normed, cols, part, bx, zsend, rz, zf, gated, oacc,
    op_p, op_o, op_r, hs, hr, mixed,
    mb, ag, sdo, sd, rows, xn, ssq, gacc, hid, e_p, e_o, e_r, es, er, outb, ret,
    wsem, lsem, osem, sa, ra, sa2, ra2, sb, rb, sz, rzs, szf, rzf, sd1, rd1, sd2, rd2,
    sag, rag, sco, sc1, rc1, sc2, rc2, sc3, rc3, se1, re1, se2, re2, ro2, se3, re3,
):
    e = lax.axis_index("ep")
    t = lax.axis_index("tp")
    core = lax.rem(t, 2)
    y = t // 2
    q = t + 1 - 2 * core
    ys = p // 2
    nz = n // nx
    z = e // nx
    x = lax.rem(e, nx)

    rows_g, width = tokens.shape
    depth = width // n
    share = width // p
    sw = share // HALVES
    slots = n * cap

    small = [
        pltpu.make_async_copy(a, b, lsem.at[i])
        for i, (a, b) in enumerate(
            [(tokens_h, tokens), (mix_h, mix_gain_in), (moe_h, moe_gain_in), (routes_h, routes), (prob_h, prob),
             (taps_h, conv_w), (param_h, rate_param), (conv_h, conv_in), (state_h, state_in)]
        )
    ]
    loads = [
        pltpu.make_async_copy(a, b, wsem.at[i])
        for i, (a, b) in enumerate(
            [(rnn_h, wr), (gate_h, wg), (rate_h, wrate), (input_h, winput), (out_h, wout),
             (eg_h.at[0], weg), (eu_h.at[0], weu), (ed_h.at[0], wed)]
        )
    ]
    small[0].start()
    small[1].start()

    barrier = pltpu.get_barrier_semaphore()

    @pl.loop(1, n)
    def _(d):
        pl.semaphore_signal(barrier, inc=1, device_id={"ep": lax.rem(e + d, n)}, device_id_type=MESH)

    @pl.loop(1, p)
    def _(d):
        pl.semaphore_signal(barrier, inc=1, device_id={"tp": lax.rem(t + d, p)}, device_id_type=MESH)

    for load in small[2:] + loads[:4]:
        load.start()

    @pl.when(z == 0)
    def _():
        rz[0] = jnp.zeros(rz.shape[1:], BF16)

    @pl.when(z == nz - 1)
    def _():
        rz[1] = jnp.zeros(rz.shape[1:], BF16)

    small[0].wait()
    small[1].wait()
    nc, bw = rate_h.shape[0], rate_h.shape[1]
    late = nc // 2
    paired = nz % 2 == 0 and nz > 2
    middle = (z == nz // 2) | (z == nz // 2 - 1)
    opposite = nz - 1 - z
    if paired:
        @pl.when(middle)
        def _():
            for dx in range(1, nx):
                bx[opposite, dx, late:] = jnp.zeros((nc - late,) + bx.shape[3:], BF16)

    for j in range(width // 128):
        cs = slice(j * 128, (j + 1) * 128)
        mix_gain[:, cs] = mix_gain_in[j:j + 1, :].astype(F32)

    total_sq = jnp.zeros((rows_g, 1), F32)
    for j in range(n):
        v = tokens[:, j * depth:(j + 1) * depth].astype(F32)
        total_sq = total_sq + jnp.sum(v * v, axis=1, keepdims=True)
    scale = lax.rsqrt(total_sq / width + 1e-06)
    for j in range(n):
        cs = slice(j * depth, (j + 1) * depth)
        normed[j] = (tokens[:, cs].astype(F32) * scale * mix_gain[:, cs]).astype(BF16)

    pl.semaphore_wait(barrier, n + p - 2)

    half = pl.ds(pl.multiple_of(core * (rows_g // 2), rows_g // 2), rows_g // 2)
    high = (2 * z) // nz
    folded = z + high * (nz - 1 - 2 * z)

    lead = nz - 1 - 2 * folded

    def across(j):
        plane = nz - 1 - j
        plane = plane - (folded >= plane).astype(jnp.int32)
        return plane + high * (nz - 1 - 2 * plane)

    def far(j):
        ahead = (j < lead).astype(jnp.int32)
        k = (1 - ahead) * (j - lead)
        turn = folded + (folded - k // 2) * (2 * lax.rem(k, 2) - 1)
        plane = ahead * (nz - 1 - j) + (1 - ahead) * turn
        return plane + high * (nz - 1 - 2 * plane)

    def beside(dx):
        return lax.rem(x + dx, nx)

    def peer_of(plane, dx):
        return plane * nx + beside(dx)

    def copy_a(peer):
        return remote(normed.at[peer, half], cols.at[e, half], sa, ra.at[z], {"ep": peer})

    def copy_a2(src, plane):
        return remote(cols.at[src, half], cols.at[src, half], sa2, ra2.at[plane], {"tp": q})

    def landed(plane, count, sem):
        block = cols.at[pl.ds(0, count), half]
        remote(block, block, sa, sem.at[plane], {"tp": q}).wait_recv()

    for dx in range(1, nx):
        copy_a(peer_of(z, dx)).start()

    @pl.loop(0, nz - 1)
    def _(j):
        for dx in range(nx):
            copy_a(peer_of(across(j), dx)).start()

    cols[e] = normed[e]

    for j in range(2, 5):
        small[j].wait()
    for j in range(width // 128):
        cs = slice(j * 128, (j + 1) * 128)
        moe_gain[:, cs] = moe_gain_in[j:j + 1, :].astype(F32)
    ids = routes[...]
    sub_e = lax.broadcasted_iota(jnp.int32, (n, rows_g), 0)
    named = [(ids[k:k + 1, :] == sub_e).astype(F32) for k in range(ids.shape[0])]
    member = functools.reduce(lambda a, b: a + b, named)
    earlier = (
        lax.broadcasted_iota(jnp.int32, (rows_g, rows_g), 0)
        < lax.broadcasted_iota(jnp.int32, (rows_g, rows_g), 1)
    ).astype(F32)
    before = dot(member.astype(BF16), earlier.astype(BF16))
    sub_s = lax.broadcasted_iota(jnp.int32, (slots, rows_g), 0).astype(F32)
    total_prob = jnp.sum(prob[...], axis=0, keepdims=True)
    dispatch = jnp.zeros((slots, rows_g), F32)
    comb = jnp.zeros((slots, rows_g), F32)
    for k in range(ids.shape[0]):
        slot = jnp.sum(before * named[k], axis=0, keepdims=True)
        target = ids[k:k + 1, :].astype(F32) * cap + slot
        hit = (sub_s == target).astype(F32)
        dispatch = dispatch + hit
        comb = comb + hit * (prob[k:k + 1, :] / total_prob)
    dispatch = dispatch.astype(BF16)
    comb_hi = comb.astype(BF16)
    comb_lo = (comb - comb_hi.astype(F32)).astype(BF16)

    loads[0].wait()
    loads[1].wait()
    for load in loads[4:]:
        load.start()

    def copy_x(plane, dx, c):
        return remote(
            part.at[plane, beside(dx), c], bx.at[plane, dx, c], sb, rb.at[plane, dx - 1, c],
            {"ep": peer_of(z, dx)},
        )

    def copy_f(dx, c):
        return remote(
            part.at[opposite, beside(dx), c], zf.at[dx - 1, c - late], szf, rzf.at[dx - 1, c - late],
            {"ep": opposite * nx + x},
        )

    def by_line(plane, c):
        return middle & (plane == opposite) if paired and c >= late else None

    def unless(flag, action):
        if flag is None:
            action()
        else:
            pl.when(jnp.logical_not(flag))(action)

    def project(plane, last, own):
        first = 1 if own else 0
        if nx > first:
            landed(plane, nx - first, ra)
            for dx in range(first, nx):
                copy_a2(peer_of(plane, dx), plane).start()
            landed(plane, nx - first, ra2)
        feats = cols[pl.ds(plane * nx, nx)].reshape(nx * rows_g, depth)
        for c in range(nc):
            cs = slice(c * bw, (c + 1) * bw)
            for lo, weight in ((0, wr), (bw, wg)):
                value = dot(feats, weight[:, cs]).astype(BF16)
                for i in range(nx):
                    part[plane, i, c, :, lo:lo + bw] = value[i * rows_g:(i + 1) * rows_g]
            if c < last:
                flag = None if own else by_line(plane, c)
                for dx in range(1, nx):
                    unless(flag, copy_x(plane, dx, c).start)
                    if flag is not None:
                        pl.when(flag)(copy_f(dx, c).start)

    project(z, late, True)

    @pl.loop(0, nz - 1)
    def _(j):
        project(far(j), nc, False)

    def rest_of_own():
        for c in range(late, nc):
            for dx in range(1, nx):
                if paired:
                    @pl.when(middle)
                    def _():
                        copy_f(dx, c).wait_recv()
                        mine = part[z, beside(dx), c].astype(F32)
                        part[z, beside(dx), c] = (mine + zf[dx - 1, c - late].astype(F32)).astype(BF16)

                copy_x(z, dx, c).start()

    def copy_z(side, plane, c, at=None):
        to = z + 1 - 2 * side
        slot = plane + side * ((to if at is None else at) == plane).astype(jnp.int32) * (nz - plane)
        return remote(
            zsend.at[plane, c], rz.at[side, plane, c], sz, rzs.at[slot, c],
            {"ep": to * nx + x},
        )

    def summed(sides, plane, c):
        for dx in range(1, nx):
            unless(by_line(plane, c) if len(sides) == 1 else None, copy_x(plane, dx, c).wait_recv)
        total = part[plane, x, c].astype(F32)
        for dx in range(1, nx):
            total = total + bx[plane, dx, c].astype(F32)
        for s in sides:
            origin = z - 1 + 2 * s

            @pl.when((origin >= 0) & (origin < nz))
            def _():
                copy_z(s, plane, c, z).wait_recv()

            total = total + rz[s, plane, c].astype(F32)
        return total

    def line_step(j):
        plane = far(j)
        side = (plane < z).astype(jnp.int32)
        for c in range(nc):
            zsend[plane, c] = summed([side], plane, c).astype(BF16)
            copy_z(side, plane, c).start()

    if nz > 1:
        line_step(jnp.int32(0))
    rest_of_own()
    if nz > 1:
        pl.loop(1, nz - 1)(line_step)

    def block(i, h):
        return pl.ds(pl.multiple_of(i * share + h * sw, sw), sw)

    for load in small[5:]:
        load.wait()
    loads[2].wait()
    loads[3].wait()
    loads[4].wait()
    for i in range(1, conv_in.shape[0]):
        conv_v[i - 1] = conv_in[i]
    for c in range(nc):
        cs = slice(c * bw, (c + 1) * bw)
        proj = summed([0, 1], z, c)
        moved = proj[:, :bw].astype(BF16)
        conv_v[conv_in.shape[0] - 1, :, cs] = moved
        taps = conv_w[:, cs].astype(F32)
        hist = conv_in[0, :, cs].astype(F32) * taps[0:1]
        for i in range(1, 3):
            hist = hist + conv_in[i, :, cs].astype(F32) * taps[i:i + 1]
        conv = (hist + moved.astype(F32) * taps[3:4]).astype(BF16)
        rate = jax.nn.sigmoid(dot(conv, wrate[c]))
        in_gate = jax.nn.sigmoid(dot(conv, winput[c]))
        log_decay = -8.0 * rate * jnp.log1p(jnp.exp(-rate_param[:, cs]))
        th = jnp.tanh(log_decay)
        rest = -2.0 * th / (1.0 - th)
        state = jnp.exp(log_decay) * state_in[:, cs] + jnp.sqrt(rest) * in_gate * conv.astype(F32)
        state_v[:, cs] = state
        gated[:, cs] = (state * jax.nn.gelu(proj[:, bw:], approximate=True)).astype(BF16)
        if c < nc - 1:
            for i in range(p):
                for h in range(HALVES):
                    lo = i * share + h * sw
                    piece = dot(gated[:, cs], wout[cs, lo:lo + sw])
                    oacc[i, h] = piece if c == 0 else oacc[i, h] + piece

    last = slice((nc - 1) * bw, nc * bw)

    def out_part(i, h):
        piece = dot(gated[:, last], wout[last, block(i, h)])
        return oacc[i, h] + piece if nc > 1 else piece

    def copy_d1(yy, h):
        return remote(op_p.at[yy, h], op_r.at[yy, h], sd1, rd1.at[yy, h], {"tp": q})

    def copy_d2(dy, h):
        ty = lax.rem(y + dy, ys)
        return remote(hs.at[ty, h], hr.at[y, h], sd2, rd2.at[dy - 1, h], {"tp": ty * 2 + core})

    def out_parts(dys):
        for yy in [lax.rem(y + dy, ys) for dy in dys]:
            for h in range(HALVES):
                op_p[yy, h] = out_part(yy * 2 + 1 - core, h).astype(BF16)
                copy_d1(yy, h).start()
        for yy in [lax.rem(y + dy, ys) for dy in dys]:
            for h in range(HALVES):
                op_o[yy, h] = out_part(yy * 2 + core, h)

    out_parts(range(1, ys))
    out_parts([0])
    for h in range(HALVES):
        for dy in range(1, ys):
            ty = lax.rem(y + dy, ys)
            copy_d1(ty, h).wait_recv()
            hs[ty, h] = (op_o[ty, h] + op_r[ty, h].astype(F32)).astype(BF16)
            copy_d2(dy, h).start()

    puts = [
        pltpu.make_async_copy(a, b, osem.at[i])
        for i, (a, b) in enumerate([(state_v, state_out), (conv_v, conv_out), (layer_v, layer_out)])
    ]
    puts[0].start()
    puts[1].start()

    def copy_c1(peer, h):
        return remote(sd.at[h, peer], rows.at[h, t, e], sc1, rc1.at[e, h], {"ep": peer})

    def landed_c1(src, h):
        return remote(sd.at[h, src], rows.at[h, t, src], sc1, rc1.at[src, h], {"ep": src})

    def copy_c2(dy, src, h):
        to = lax.rem(y + dy, ys) * 2 + core
        return remote(rows.at[h, t, src], rows.at[h, t, src], sc2, rc2.at[dy - 1, src, h], {"tp": to})

    def landed_c2(dy, src, h):
        held = lax.rem(y - dy + ys, ys) * 2 + core
        return remote(
            rows.at[h, held, src], rows.at[h, held, src], sc2, rc2.at[dy - 1, src, h], {"tp": held}
        )

    def copy_c3(dy, src, h, away=0):
        held = lax.rem(y - dy + ys, ys) * 2 + core
        return remote(
            rows.at[h, held, src], rows.at[h, held, src], sc3, rc3.at[h, away if h == HALVES - 1 and nz % 2 == 0 else 0], {"tp": q}
        )

    def copy_g(dy, h):
        ty = lax.rem(y + dy, ys)
        return remote(mb.at[h], ag.at[y, h], sag, rag.at[dy - 1, h], {"tp": ty * 2 + core})

    def copy_o(dy, peer, h):
        held = lax.rem(y - dy + ys, ys) * 2 + core
        return remote(sdo.at[dy - 1, h, peer], rows.at[h, held, e], sco, rc2.at[dy - 1, e, h], {"ep": peer})

    def landed_o(dy, src, h):
        held = lax.rem(y - dy + ys, ys) * 2 + core
        return remote(sdo.at[dy - 1, h, src], rows.at[h, held, src], sco, rc2.at[dy - 1, src, h], {"ep": src})

    ncross = nz // 2 if nz % 2 == 0 else nz - 1
    beyond = [[peer_of(across(j), dx) for dx in range(nx)] for j in reversed(range(ncross))]
    near = [peer_of(z, dx) for dx in range(1, nx)]
    near = near + [peer_of(across(j), dx) for j in range(ncross, nz - 1) for dx in range(nx)]

    def reduce_half(h):
        copy_d1(y, h).wait_recv()
        total = tokens[:, block(t, h)].astype(F32) + op_o[y, h] + op_r[y, h].astype(F32)
        for dy in range(1, ys):
            copy_d2(dy, h).wait_recv()
            total = total + hr[lax.rem(y - dy + ys, ys), h].astype(F32)
        mixed[h] = total
        mb[h] = total.astype(BF16)
        for dy in range(1, ys):
            copy_g(dy, h).start()
        sd[h] = dot(dispatch, mb[h]).reshape(n, cap, sw).astype(BF16)

    def send_half(h):
        @pl.loop(0, ncross)
        def _(j):
            for dx in range(nx):
                copy_c1(peer_of(across(j), dx), h).start()

        for peer in near:
            copy_c1(peer, h).start()
        rows[h, t, e] = sd[h, e]
        copy_c3(0, e, h).start()

    reduce_half(0)
    send_half(0)
    reduce_half(1)

    gs = min(n, max(1, 64 // cap))
    span = gs * cap
    hidden = hid.shape[1]
    fc = min(256, hidden)

    split = 2 if nz % 2 == 0 else 1
    count = n // split

    def scaled_rows(h, first, number, away):
        mate = rows.at[h, pl.ds(0, ys), pl.ds(0, number)]
        remote(mate, mate, sc3, rc3.at[h, away], {"tp": q}).wait_recv()

        @pl.loop(0, number // gs)
        def _(g):
            at = pl.ds(pl.multiple_of(first * cap + g * span, span), span)
            acc = jnp.zeros((span, 1), F32)
            for i in range(p):
                lo = i * share + h * sw
                v = rows[h, i, pl.ds(first + g * gs, gs)].astype(F32).reshape(span, sw)
                acc = acc + jnp.sum(v * v, axis=1, keepdims=True)
                xn[h, at, i * sw:(i + 1) * sw] = (v * moe_gain[:, lo:lo + sw]).astype(BF16)
            ssq[at, :] = acc if h == 0 else ssq[at, :] + acc

    def rows_at(first, number):
        return pl.ds(pl.multiple_of(first * cap, count * cap), number * cap)

    def partial_dot(weight, h, at, cs):
        acc = None
        for i in range(p):
            lo = i * share + h * sw
            piece = dot(xn[h, at, i * sw:(i + 1) * sw], weight[lo:lo + sw, cs])
            acc = piece if acc is None else acc + piece
        return acc

    def early(k, weight, f, h, first, number):
        cs = slice(f * fc, (f + 1) * fc)
        at = rows_at(first, number)
        value = partial_dot(weight, h, at, cs)
        gacc[k, at, cs] = value if h == 0 else gacc[k, at, cs] + value

    def dots(h, first, number):
        for f in range(hidden // fc):
            early(0, weg, f, h, first, number)
            early(1, weu, f, h, first, number)

    def activate(first, number):
        at = rows_at(first, number)
        row_scale = lax.rsqrt(ssq[at, :] / width + 1e-06)
        for f in range(hidden // fc):
            cs = slice(f * fc, (f + 1) * fc)
            gate_part = gacc[0, at, cs] * row_scale
            hid[at, cs] = (jax.nn.silu(gate_part) * (gacc[1, at, cs] * row_scale)).astype(BF16)

    here = high * count if split == 2 else 0
    there = (1 - high) * count if split == 2 else 0

    def gathered(h):
        for dy in range(1, ys):
            origin = lax.rem(y - dy + ys, ys)
            copy_g(dy, h).wait_recv()
            sdo[dy - 1, h] = dot(dispatch, ag[origin, h]).reshape(n, cap, sw).astype(BF16)
            for peer in near:
                copy_o(dy, peer, h).start()
            rows[h, origin * 2 + core, e] = sdo[dy - 1, h, e]
            copy_c3(dy, e, h).start()

    def near_own(src, h):
        landed_c1(src, h).wait_recv()
        copy_c3(0, src, h).start()

    def near_other(src, h):
        for dy in range(1, ys):
            landed_o(dy, src, h).wait_recv()
            copy_c3(dy, src, h).start()

    def pass_on(src, h):
        for dy in range(1, ys):
            landed_c2(dy, src, h).wait_recv()
            copy_c3(dy, src, h, 1).start()

    def cross(src, h):
        landed_c1(src, h).wait_recv()
        for dy in range(1, ys):
            copy_c2(dy, src, h).start()
        copy_c3(0, src, h, 1).start()

    def each(action, sources, h):
        for src in sources:
            action(src, h)

    nearest = beyond[0] if beyond else []
    farthest = [src for group in beyond[1:] for src in group]
    gathered(0)
    send_half(1)
    each(cross, farthest, 0)
    gathered(1)
    each(cross, nearest, 0)
    each(pass_on, farthest, 0)
    each(near_own, near, 0)
    each(near_other, near, 0)
    each(pass_on, nearest, 0)
    each(cross, farthest, 1)
    each(cross, nearest, 1)
    each(near_own, near, 1)
    each(near_other, near, 1)
    loads[5].wait()
    loads[6].wait()
    scaled_rows(0, 0, n, 0)
    dots(0, 0, n)
    each(pass_on, farthest, 1)
    each(pass_on, nearest, 1)
    if split == 2:
        scaled_rows(HALVES - 1, here, count, 0)
        dots(HALVES - 1, here, count)

    scaled_rows(HALVES - 1, there, count, split - 1)
    dots(HALVES - 1, there, count)
    activate(there, count)
    if split == 2:
        activate(here, count)

    loads[7].wait()
    chunk = nx * cap

    def copy_e1(plane, yy, h):
        return remote(e_p.at[plane, yy, h], e_r.at[plane, yy, h], se1, re1.at[plane, yy, h], {"tp": q})

    def copy_e2(plane, dy, h):
        ty = lax.rem(y + dy, ys)
        return remote(
            es.at[plane, ty, h], er.at[plane, y, h], se2, re2.at[plane, dy - 1, h],
            {"tp": ty * 2 + core},
        )

    def mine_of(dx):
        return pl.ds(pl.multiple_of(beside(dx) * cap, cap), cap)

    def copy_own(dy, dx, h):
        ty = lax.rem(y + dy, ys)
        return remote(
            es.at[z, ty, h, mine_of(dx)], er.at[z, y, h, mine_of(dx)], se2, ro2.at[dy - 1, dx, h],
            {"tp": ty * 2 + core},
        )

    own_order = [(dx, h) for dx in list(range(1, nx)) + [0] for h in range(HALVES)]

    def copy_e3(peer, h):
        return remote(outb.at[h, peer], ret.at[h, e], se3, re3.at[h], {"ep": peer})

    def issue(planes, dys):
        mine = jnp.concatenate([hid[pl.ds(pl.multiple_of(k * chunk, chunk), chunk), :] for k in planes], axis=0)
        for dy in dys:
            ty = lax.rem(y + dy, ys)
            for h in range(HALVES):
                value = dot(mine, wed[:, block(ty * 2 + 1 - core, h)]).astype(BF16)
                for i, k in enumerate(planes):
                    e_p[k, ty, h] = value[i * chunk:(i + 1) * chunk]
                    copy_e1(k, ty, h).start()
            for h in range(HALVES):
                value = dot(mine, wed[:, block(ty * 2 + core, h)])
                for i, k in enumerate(planes):
                    e_o[k, ty, h] = value[i * chunk:(i + 1) * chunk]

    def push(plane):
        for dy in range(1, ys):
            ty = lax.rem(y + dy, ys)
            for h in range(HALVES):
                copy_e1(plane, ty, h).wait_recv()
                es[plane, ty, h] = (e_o[plane, ty, h] + e_r[plane, ty, h].astype(F32)).astype(BF16)
                copy_e2(plane, dy, h).start()

    def push_own():
        for dy in range(1, ys):
            ty = lax.rem(y + dy, ys)
            for h in range(HALVES):
                copy_e1(z, ty, h).wait_recv()
            for dx, h in own_order:
                at = mine_of(dx)
                es[z, ty, h, at] = (e_o[z, ty, h, at] + e_r[z, ty, h, at].astype(F32)).astype(BF16)
                copy_own(dy, dx, h).start()

    def deliver_own():
        for h in range(HALVES):
            copy_e1(z, y, h).wait_recv()
        for dx, h in own_order:
            at = mine_of(dx)
            result = e_o[z, y, h, at] + e_r[z, y, h, at].astype(F32)
            for dy in range(1, ys):
                copy_own(dy, dx, h).wait_recv()
                result = result + er[z, lax.rem(y - dy + ys, ys), h, at].astype(F32)
            if dx:
                outb[h, peer_of(z, dx)] = result.astype(BF16)
                copy_e3(peer_of(z, dx), h).start()
            else:
                ret[h, e] = result.astype(BF16)

    def deliver(plane):
        for h in range(HALVES):
            copy_e1(plane, y, h).wait_recv()
            result = e_o[plane, y, h] + e_r[plane, y, h].astype(F32)
            for dy in range(1, ys):
                copy_e2(plane, dy, h).wait_recv()
                result = result + er[plane, lax.rem(y - dy + ys, ys), h].astype(F32)
            result = result.reshape(nx, cap, sw).astype(BF16)
            outb[h, pl.ds(plane * nx, nx)] = result
            for dx in range(nx):
                copy_e3(peer_of(plane, dx), h).start()

    order = [across(j) for j in range(nz - 1)] + [z]
    pairs = [order[i:i + 2] for i in range(0, nz, 2)]
    for planes in pairs:
        issue(planes, range(1, ys))
        issue(planes, [0])
        for plane in planes:
            push_own() if plane is z else push(plane)

    @pl.loop(0, nz - 1)
    def _(j):
        deliver(across(j))

    deliver_own()

    def combine(weights, back):
        return lax.dot_general(weights, back, (((0,), (0,)), ((), ())), preferred_element_type=F32)

    for h in range(HALVES):
        others = ret.at[h, pl.ds(0, n - 1)]
        remote(others, others, se3, re3.at[h], {"ep": peer_of(z, 1)}).wait_recv()
        back = ret[h].astype(F32).reshape(slots, sw).astype(BF16)
        layer_v[:, h * sw:(h + 1) * sw] = (
            mixed[h] + combine(comb_hi, back) + combine(comb_lo, back)
        ).astype(BF16)

    puts[2].start()

    def drain(ref, sem):
        remote(ref, ref, sem, ra.at[0], {"tp": q}).wait_send()

    drain(normed.at[pl.ds(0, n - 1), half], sa)
    drain(cols.at[pl.ds(0, n - 1), half], sa2)
    if paired:
        @pl.when(middle)
        def _():
            drain(part.at[pl.ds(0, nz - 1), pl.ds(0, nx - 1)], sb)
            drain(part.at[0, pl.ds(0, nx - 1), pl.ds(0, late)], sb)
            drain(zf, szf)

        @pl.when(jnp.logical_not(middle))
        def _():
            drain(part.at[:, pl.ds(0, nx - 1)], sb)
    else:
        drain(part.at[:, pl.ds(0, nx - 1)], sb)
    drain(zsend.at[pl.ds(0, nz - 1)], sz)
    drain(op_p, sd1)
    drain(hs.at[pl.ds(0, ys - 1)], sd2)
    drain(sd.at[:, pl.ds(0, n - 1)], sc1)
    drain(rows.at[:, pl.ds(0, ys - 1), pl.ds(0, n - 1 - len(near))], sc2)
    drain(ag.at[pl.ds(0, ys - 1)], sag)
    drain(sdo.at[:, :, pl.ds(0, len(near))], sco)
    drain(rows.at[:, pl.ds(0, ys)], sc3)
    drain(e_p, se1)
    drain(es.at[:, pl.ds(0, ys - 1)], se2)
    drain(outb.at[:, pl.ds(0, n - 1)], se3)

    for put in puts:
        put.wait()


def finish(layer_in, state_in, conv_in, layer_out, state_out, conv_out):
    layer_out[...] = layer_in[...]
    state_out[...] = state_in[...]
    conv_out[...] = conv_in[...]


def shards(
    n, p,
    tokens, state_in, conv_in, mix_gain, rnn_weight, gate_weight, conv_weight, rate_weight,
    input_weight, rate_param, out_weight, moe_gain, expert_gate, expert_up, expert_down, routes, route_prob,
):
    g, width = tokens.shape
    depth, chans = rnn_weight.shape
    share = width // p
    cap = max(2, 2 * g * routes.shape[1] // n)
    slots = n * cap
    hidden = expert_gate.shape[2]
    ys = p // 2
    nx = 1 << ((n.bit_length() - 1) // 2)
    nx = nx if n % nx == 0 else 1
    nz = n // nx
    nc, cw = rate_weight.shape[0], 2 * rate_weight.shape[1]
    nh, sw = HALVES, share // HALVES
    chunk = nx * cap
    vm = pl.BlockSpec(memory_space=pltpu.VMEM)
    hb = pl.BlockSpec(memory_space=pl.ANY)
    dma = pltpu.SemaphoreType.DMA
    V = pltpu.VMEM
    small = (
        tokens, state_in, jnp.transpose(conv_in, (1, 0, 2)), mix_gain.reshape(-1, 128), moe_gain.reshape(-1, 128),
        conv_weight, rate_param[None], routes.T, route_prob.T,
    )
    scratch = [V(a.shape, a.dtype) for a in small] + [
        V((g, share), BF16), V((g, chans), F32), V((conv_in.shape[1], g, chans), BF16),
        V((depth, chans), BF16), V((depth, chans), BF16),
        V(rate_weight.shape, BF16), V(input_weight.shape, BF16), V(out_weight.shape, BF16),
        V(expert_gate.shape[1:], BF16), V(expert_up.shape[1:], BF16), V(expert_down.shape[1:], BF16),
        V((1, width), F32), V((1, width), F32),
        V((n, g, depth), BF16), V((n, g, depth), BF16),
        V((nz, nx, nc, g, cw), BF16), V((nz, nx, nc, g, cw), BF16),
        V((nz, nc, g, cw), BF16), V((2, nz, nc, g, cw), BF16), V((nx - 1, nc - nc // 2, g, cw), BF16),
        V((g, chans), BF16), V((p, nh, g, sw), F32),
        V((ys, nh, g, sw), BF16), V((ys, nh, g, sw), F32), V((ys, nh, g, sw), BF16),
        V((ys, nh, g, sw), BF16), V((ys, nh, g, sw), BF16), V((nh, g, sw), F32),
        V((nh, g, sw), BF16), V((ys, nh, g, sw), BF16), V((ys - 1, nh, n, cap, sw), BF16),
        V((nh, n, cap, sw), BF16), V((nh, p, n, cap, sw), BF16), V((nh, slots, p * sw), BF16), V((slots, 1), F32),
        V((2, slots, hidden), F32), V((slots, hidden), BF16),
        V((nz, ys, nh, chunk, sw), BF16), V((nz, ys, nh, chunk, sw), F32), V((nz, ys, nh, chunk, sw), BF16),
        V((nz, ys, nh, chunk, sw), BF16), V((nz, ys, nh, chunk, sw), BF16),
        V((nh, n, cap, sw), BF16), V((nh, n, cap, sw), BF16),
        dma((8,)), dma((len(small),)), dma((3,)),
        dma, dma((nz,)), dma, dma((nz,)),
        dma, dma((nz, nx - 1, nc)), dma, dma((nz + 1, nc)), dma, dma((nx - 1, nc - nc // 2)),
        dma, dma((ys, nh)), dma, dma((ys - 1, nh)),
        dma, dma((ys - 1, nh)), dma,
        dma, dma((n, nh)), dma, dma((ys - 1, n, nh)), dma, dma((nh, 2)),
        dma, dma((nz, ys, nh)), dma, dma((nz, ys - 1, nh)), dma((ys - 1, nx, nh)), dma, dma((nh,)),
    ]
    outs = (
        jax.ShapeDtypeStruct((g, share), BF16),
        jax.ShapeDtypeStruct((g, chans), F32),
        jax.ShapeDtypeStruct((conv_in.shape[1], g, chans), BF16),
    )
    held = pl.pallas_call(
        functools.partial(kernel, n, p, nx, cap),
        out_shape=outs,
        in_specs=[hb] * 17,
        out_specs=(hb, hb, hb),
        scratch_shapes=scratch,
        compiler_params=pltpu.CompilerParams(
            collective_id=0, has_side_effects=True, vmem_limit_bytes=60 * 1024 * 1024
        ),
    )(
        *small,
        rnn_weight, gate_weight, rate_weight, input_weight, out_weight, expert_gate, expert_up, expert_down,
    )
    layer_out, state_out, conv_out = pl.pallas_call(
        finish,
        out_shape=outs,
        in_specs=[vm] * 3,
        out_specs=(vm, vm, vm),
    )(*held)
    return (layer_out, state_out, jnp.transpose(conv_out, (1, 0, 2)))


def solution(mesh):
    in_specs = (
        P("ep", None),
        P("ep", "tp"),
        P("ep", None, "tp"),
        P(),
        P("ep", "tp"),
        P("ep", "tp"),
        P(None, "tp"),
        P("tp", None, None),
        P("tp", None, None),
        P("tp"),
        P("tp", None),
        P(),
        P("ep", None, "tp"),
        P("ep", None, "tp"),
        P("ep", "tp", None),
        P("ep", None),
        P("ep", None),
    )
    out_specs = (P("ep", "tp"), P("ep", "tp"), P("ep", None, "tp"))
    body = functools.partial(shards, mesh.shape["ep"], mesh.shape["tp"])
    return jax.shard_map(body, mesh=mesh, in_specs=in_specs, out_specs=out_specs, check_vma=False)
```

```python
import functools

import jax
import jax.numpy as jnp
from jax import lax
from jax.experimental import pallas as pl
from jax.experimental.pallas import tpu as pltpu
from jax.sharding import PartitionSpec as P

MESH = pl.DeviceIdType.MESH
F32 = jnp.float32
BF16 = jnp.bfloat16
HALVES = 2


def dot(a, b):
    return jnp.dot(a, b, preferred_element_type=F32)


def remote(src, dst, send, recv, where):
    return pltpu.make_async_remote_copy(
        src_ref=src, dst_ref=dst, send_sem=send, recv_sem=recv, device_id=where, device_id_type=MESH
    )


def kernel(
    n, p, nx, cap,
    tokens_h, state_h, conv_h, mix_h, moe_h, taps_h, param_h, routes_h, prob_h,
    rnn_h, gate_h, rate_h, input_h, out_h, eg_h, eu_h, ed_h,
    layer_out, state_out, conv_out,
    tokens, state_in, conv_in, mix_gain_in, moe_gain_in, conv_w, rate_param, routes, prob,
    layer_v, state_v, conv_v,
    wr, wg, wrate, winput, wout, weg, weu, wed,
    mix_gain, moe_gain, normed, cols, part, bx, zsend, rz, zf, gated, oacc,
    op_p, op_o, op_r, hs, hr, mixed,
    mb, ag, sdo, sd, rows, xn, ssq, gacc, hid, e_p, e_o, e_r, es, er, outb, ret,
    wsem, lsem, osem, sa, ra, sa2, ra2, sb, rb, sz, rzs, szf, rzf, sd1, rd1, sd2, rd2,
    sag, rag, sco, sc1, rc1, sc2, rc2, sc3, rc3, se1, re1, se2, re2, ro2, se3, re3,
):
    e = lax.axis_index("ep")
    t = lax.axis_index("tp")
    core = lax.rem(t, 2)
    y = t // 2
    q = t + 1 - 2 * core
    ys = p // 2
    nz = n // nx
    z = e // nx
    x = lax.rem(e, nx)

    rows_g, width = tokens.shape
    depth = width // n
    share = width // p
    sw = share // HALVES
    slots = n * cap

    small = [
        pltpu.make_async_copy(a, b, lsem.at[i])
        for i, (a, b) in enumerate(
            [(tokens_h, tokens), (mix_h, mix_gain_in), (moe_h, moe_gain_in), (routes_h, routes), (prob_h, prob),
             (taps_h, conv_w), (param_h, rate_param), (conv_h, conv_in), (state_h, state_in)]
        )
    ]
    loads = [
        pltpu.make_async_copy(a, b, wsem.at[i])
        for i, (a, b) in enumerate(
            [(rnn_h, wr), (gate_h, wg), (rate_h, wrate), (input_h, winput), (out_h, wout),
             (eg_h.at[0], weg), (eu_h.at[0], weu), (ed_h.at[0], wed)]
        )
    ]
    small[0].start()
    small[1].start()

    barrier = pltpu.get_barrier_semaphore()

    @pl.loop(1, n)
    def _(d):
        pl.semaphore_signal(barrier, inc=1, device_id={"ep": lax.rem(e + d, n)}, device_id_type=MESH)

    @pl.loop(1, p)
    def _(d):
        pl.semaphore_signal(barrier, inc=1, device_id={"tp": lax.rem(t + d, p)}, device_id_type=MESH)

    @pl.when(z == 0)
    def _():
        rz[0] = jnp.zeros(rz.shape[1:], BF16)

    @pl.when(z == nz - 1)
    def _():
        rz[1] = jnp.zeros(rz.shape[1:], BF16)

    small[0].wait()
    small[1].wait()
    for load in loads[:2] + small[2:] + loads[2:4]:
        load.start()
    nc, bw = rate_h.shape[0], rate_h.shape[1]
    late = nc // 2
    paired = nz % 2 == 0 and nz > 2
    middle = (z == nz // 2) | (z == nz // 2 - 1)
    opposite = nz - 1 - z
    if paired:
        @pl.when(middle)
        def _():
            for dx in range(1, nx):
                bx[opposite, dx, late:] = jnp.zeros((nc - late,) + bx.shape[3:], BF16)

    for j in range(width // 128):
        cs = slice(j * 128, (j + 1) * 128)
        mix_gain[:, cs] = mix_gain_in[j:j + 1, :].astype(F32)

    total_sq = jnp.zeros((rows_g, 1), F32)
    for j in range(n):
        v = tokens[:, j * depth:(j + 1) * depth].astype(F32)
        total_sq = total_sq + jnp.sum(v * v, axis=1, keepdims=True)
    scale = lax.rsqrt(total_sq / width + 1e-06)
    for j in range(n):
        cs = slice(j * depth, (j + 1) * depth)
        normed[j] = (tokens[:, cs].astype(F32) * scale * mix_gain[:, cs]).astype(BF16)

    pl.semaphore_wait(barrier, n + p - 2)

    half = pl.ds(pl.multiple_of(core * (rows_g // 2), rows_g // 2), rows_g // 2)
    high = (2 * z) // nz
    folded = z + high * (nz - 1 - 2 * z)

    lead = nz - 1 - 2 * folded

    def across(j):
        plane = nz - 1 - j
        plane = plane - (folded >= plane).astype(jnp.int32)
        return plane + high * (nz - 1 - 2 * plane)

    def far(j):
        ahead = (j < lead).astype(jnp.int32)
        k = (1 - ahead) * (j - lead)
        turn = folded + (folded - k // 2) * (2 * lax.rem(k, 2) - 1)
        plane = ahead * (nz - 1 - j) + (1 - ahead) * turn
        return plane + high * (nz - 1 - 2 * plane)

    def beside(dx):
        return lax.rem(x + dx, nx)

    def peer_of(plane, dx):
        return plane * nx + beside(dx)

    def copy_a(peer):
        return remote(normed.at[peer, half], cols.at[e, half], sa, ra.at[z], {"ep": peer})

    def copy_a2(src, plane):
        return remote(cols.at[src, half], cols.at[src, half], sa2, ra2.at[plane], {"tp": q})

    def landed(plane, count, sem):
        block = cols.at[pl.ds(0, count), half]
        remote(block, block, sa, sem.at[plane], {"tp": q}).wait_recv()

    for dx in range(1, nx):
        copy_a(peer_of(z, dx)).start()

    @pl.loop(0, nz - 1)
    def _(j):
        for dx in range(nx):
            copy_a(peer_of(across(j), dx)).start()

    cols[e] = normed[e]

    for j in range(2, 5):
        small[j].wait()
    for j in range(width // 128):
        cs = slice(j * 128, (j + 1) * 128)
        moe_gain[:, cs] = moe_gain_in[j:j + 1, :].astype(F32)
    ids = routes[...]
    sub_e = lax.broadcasted_iota(jnp.int32, (n, rows_g), 0)
    named = [(ids[k:k + 1, :] == sub_e).astype(F32) for k in range(ids.shape[0])]
    member = functools.reduce(lambda a, b: a + b, named)
    earlier = (
        lax.broadcasted_iota(jnp.int32, (rows_g, rows_g), 0)
        < lax.broadcasted_iota(jnp.int32, (rows_g, rows_g), 1)
    ).astype(F32)
    before = dot(member.astype(BF16), earlier.astype(BF16))
    sub_s = lax.broadcasted_iota(jnp.int32, (slots, rows_g), 0).astype(F32)
    total_prob = jnp.sum(prob[...], axis=0, keepdims=True)
    dispatch = jnp.zeros((slots, rows_g), F32)
    comb = jnp.zeros((slots, rows_g), F32)
    for k in range(ids.shape[0]):
        slot = jnp.sum(before * named[k], axis=0, keepdims=True)
        target = ids[k:k + 1, :].astype(F32) * cap + slot
        hit = (sub_s == target).astype(F32)
        dispatch = dispatch + hit
        comb = comb + hit * (prob[k:k + 1, :] / total_prob)
    dispatch = dispatch.astype(BF16)
    comb_hi = comb.astype(BF16)
    comb_lo = (comb - comb_hi.astype(F32)).astype(BF16)

    loads[0].wait()
    loads[1].wait()
    for load in loads[4:]:
        load.start()

    def copy_x(plane, dx, c):
        return remote(
            part.at[plane, beside(dx), c], bx.at[plane, dx, c], sb, rb.at[plane, dx - 1, c],
            {"ep": peer_of(z, dx)},
        )

    def copy_f(dx, c):
        return remote(
            part.at[opposite, beside(dx), c], zf.at[dx - 1, c - late], szf, rzf.at[dx - 1, c - late],
            {"ep": opposite * nx + x},
        )

    def by_line(plane, c):
        return middle & (plane == opposite) if paired and c >= late else None

    def unless(flag, action):
        if flag is None:
            action()
        else:
            pl.when(jnp.logical_not(flag))(action)

    def project(plane, last, own):
        first = 1 if own else 0
        if nx > first:
            landed(plane, nx - first, ra)
            for dx in range(first, nx):
                copy_a2(peer_of(plane, dx), plane).start()
            landed(plane, nx - first, ra2)
        feats = cols[pl.ds(plane * nx, nx)].reshape(nx * rows_g, depth)
        for c in range(nc):
            cs = slice(c * bw, (c + 1) * bw)
            for lo, weight in ((0, wr), (bw, wg)):
                value = dot(feats, weight[:, cs]).astype(BF16)
                for i in range(nx):
                    part[plane, i, c, :, lo:lo + bw] = value[i * rows_g:(i + 1) * rows_g]
            if c < last:
                flag = None if own else by_line(plane, c)
                for dx in range(1, nx):
                    unless(flag, copy_x(plane, dx, c).start)
                    if flag is not None:
                        pl.when(flag)(copy_f(dx, c).start)

    project(z, late, True)

    @pl.loop(0, nz - 1)
    def _(j):
        project(far(j), nc, False)

    def rest_of_own():
        for c in range(late, nc):
            for dx in range(1, nx):
                if paired:
                    @pl.when(middle)
                    def _():
                        copy_f(dx, c).wait_recv()
                        mine = part[z, beside(dx), c].astype(F32)
                        part[z, beside(dx), c] = (mine + zf[dx - 1, c - late].astype(F32)).astype(BF16)

                copy_x(z, dx, c).start()

    def copy_z(side, plane, c, at=None):
        to = z + 1 - 2 * side
        slot = plane + side * ((to if at is None else at) == plane).astype(jnp.int32) * (nz - plane)
        return remote(
            zsend.at[plane, c], rz.at[side, plane, c], sz, rzs.at[slot, c],
            {"ep": to * nx + x},
        )

    def summed(sides, plane, c):
        for dx in range(1, nx):
            unless(by_line(plane, c) if len(sides) == 1 else None, copy_x(plane, dx, c).wait_recv)
        total = part[plane, x, c].astype(F32)
        for dx in range(1, nx):
            total = total + bx[plane, dx, c].astype(F32)
        for s in sides:
            origin = z - 1 + 2 * s

            @pl.when((origin >= 0) & (origin < nz))
            def _():
                copy_z(s, plane, c, z).wait_recv()

            total = total + rz[s, plane, c].astype(F32)
        return total

    def line_step(j):
        plane = far(j)
        side = (plane < z).astype(jnp.int32)
        for c in range(nc):
            zsend[plane, c] = summed([side], plane, c).astype(BF16)
            copy_z(side, plane, c).start()

    if nz > 1:
        line_step(jnp.int32(0))
    rest_of_own()
    if nz > 1:
        pl.loop(1, nz - 1)(line_step)

    def block(i, h):
        return pl.ds(pl.multiple_of(i * share + h * sw, sw), sw)

    for load in small[5:]:
        load.wait()
    loads[2].wait()
    loads[3].wait()
    loads[4].wait()
    for i in range(1, conv_in.shape[0]):
        conv_v[i - 1] = conv_in[i]
    for c in range(nc):
        cs = slice(c * bw, (c + 1) * bw)
        proj = summed([0, 1], z, c)
        moved = proj[:, :bw].astype(BF16)
        conv_v[conv_in.shape[0] - 1, :, cs] = moved
        taps = conv_w[:, cs].astype(F32)
        hist = conv_in[0, :, cs].astype(F32) * taps[0:1]
        for i in range(1, 3):
            hist = hist + conv_in[i, :, cs].astype(F32) * taps[i:i + 1]
        conv = (hist + moved.astype(F32) * taps[3:4]).astype(BF16)
        rate = jax.nn.sigmoid(dot(conv, wrate[c]))
        in_gate = jax.nn.sigmoid(dot(conv, winput[c]))
        log_decay = -8.0 * rate * jnp.log1p(jnp.exp(-rate_param[:, cs]))
        th = jnp.tanh(log_decay)
        rest = -2.0 * th / (1.0 - th)
        state = jnp.exp(log_decay) * state_in[:, cs] + jnp.sqrt(rest) * in_gate * conv.astype(F32)
        state_v[:, cs] = state
        gated[:, cs] = (state * jax.nn.gelu(proj[:, bw:], approximate=True)).astype(BF16)
        if c < nc - 1:
            for i in range(p):
                for h in range(HALVES):
                    lo = i * share + h * sw
                    piece = dot(gated[:, cs], wout[cs, lo:lo + sw])
                    oacc[i, h] = piece if c == 0 else oacc[i, h] + piece

    last = slice((nc - 1) * bw, nc * bw)

    def out_part(i, h):
        piece = dot(gated[:, last], wout[last, block(i, h)])
        return oacc[i, h] + piece if nc > 1 else piece

    def copy_d1(yy, h):
        return remote(op_p.at[yy, h], op_r.at[yy, h], sd1, rd1.at[yy, h], {"tp": q})

    def copy_d2(dy, h):
        ty = lax.rem(y + dy, ys)
        return remote(hs.at[ty, h], hr.at[y, h], sd2, rd2.at[dy - 1, h], {"tp": ty * 2 + core})

    def out_parts(dys):
        for yy in [lax.rem(y + dy, ys) for dy in dys]:
            for h in range(HALVES):
                op_p[yy, h] = out_part(yy * 2 + 1 - core, h).astype(BF16)
                copy_d1(yy, h).start()
        for yy in [lax.rem(y + dy, ys) for dy in dys]:
            for h in range(HALVES):
                op_o[yy, h] = out_part(yy * 2 + core, h)

    out_parts(range(1, ys))
    out_parts([0])
    for h in range(HALVES):
        for dy in range(1, ys):
            ty = lax.rem(y + dy, ys)
            copy_d1(ty, h).wait_recv()
            hs[ty, h] = (op_o[ty, h] + op_r[ty, h].astype(F32)).astype(BF16)
            copy_d2(dy, h).start()

    puts = [
        pltpu.make_async_copy(a, b, osem.at[i])
        for i, (a, b) in enumerate([(state_v, state_out), (conv_v, conv_out), (layer_v, layer_out)])
    ]
    puts[0].start()
    puts[1].start()

    def copy_c1(peer, h):
        return remote(sd.at[h, peer], rows.at[h, t, e], sc1, rc1.at[e, h], {"ep": peer})

    def landed_c1(src, h):
        return remote(sd.at[h, src], rows.at[h, t, src], sc1, rc1.at[src, h], {"ep": src})

    def copy_c2(dy, src, h):
        to = lax.rem(y + dy, ys) * 2 + core
        return remote(rows.at[h, t, src], rows.at[h, t, src], sc2, rc2.at[dy - 1, src, h], {"tp": to})

    def landed_c2(dy, src, h):
        held = lax.rem(y - dy + ys, ys) * 2 + core
        return remote(
            rows.at[h, held, src], rows.at[h, held, src], sc2, rc2.at[dy - 1, src, h], {"tp": held}
        )

    def copy_c3(dy, src, h, away=0):
        held = lax.rem(y - dy + ys, ys) * 2 + core
        return remote(
            rows.at[h, held, src], rows.at[h, held, src], sc3, rc3.at[h, away if h == HALVES - 1 and nz % 2 == 0 else 0], {"tp": q}
        )

    def copy_g(dy, h):
        ty = lax.rem(y + dy, ys)
        return remote(mb.at[h], ag.at[y, h], sag, rag.at[dy - 1, h], {"tp": ty * 2 + core})

    def copy_o(dy, peer, h):
        held = lax.rem(y - dy + ys, ys) * 2 + core
        return remote(sdo.at[dy - 1, h, peer], rows.at[h, held, e], sco, rc2.at[dy - 1, e, h], {"ep": peer})

    def landed_o(dy, src, h):
        held = lax.rem(y - dy + ys, ys) * 2 + core
        return remote(sdo.at[dy - 1, h, src], rows.at[h, held, src], sco, rc2.at[dy - 1, src, h], {"ep": src})

    ncross = nz // 2 if nz % 2 == 0 else nz - 1
    beyond = [[peer_of(across(j), dx) for dx in range(nx)] for j in reversed(range(ncross))]
    near = [peer_of(z, dx) for dx in range(1, nx)]
    near = near + [peer_of(across(j), dx) for j in range(ncross, nz - 1) for dx in range(nx)]

    def reduce_half(h):
        copy_d1(y, h).wait_recv()
        total = tokens[:, block(t, h)].astype(F32) + op_o[y, h] + op_r[y, h].astype(F32)
        for dy in range(1, ys):
            copy_d2(dy, h).wait_recv()
            total = total + hr[lax.rem(y - dy + ys, ys), h].astype(F32)
        mixed[h] = total
        mb[h] = total.astype(BF16)
        for dy in range(1, ys):
            copy_g(dy, h).start()
        sd[h] = dot(dispatch, mb[h]).reshape(n, cap, sw).astype(BF16)

    def send_half(h):
        @pl.loop(0, ncross)
        def _(j):
            for dx in range(nx):
                copy_c1(peer_of(across(j), dx), h).start()

        for peer in near:
            copy_c1(peer, h).start()
        rows[h, t, e] = sd[h, e]
        copy_c3(0, e, h).start()

    reduce_half(0)
    send_half(0)
    reduce_half(1)

    gs = min(n, max(1, 64 // cap))
    span = gs * cap
    hidden = hid.shape[1]
    fc = min(256, hidden)

    split = 2 if nz % 2 == 0 else 1
    count = n // split

    def scaled_rows(h, first, number, away):
        mate = rows.at[h, pl.ds(0, ys), pl.ds(0, number)]
        remote(mate, mate, sc3, rc3.at[h, away], {"tp": q}).wait_recv()

        @pl.loop(0, number // gs)
        def _(g):
            at = pl.ds(pl.multiple_of(first * cap + g * span, span), span)
            acc = jnp.zeros((span, 1), F32)
            for i in range(p):
                lo = i * share + h * sw
                v = rows[h, i, pl.ds(first + g * gs, gs)].astype(F32).reshape(span, sw)
                acc = acc + jnp.sum(v * v, axis=1, keepdims=True)
                xn[h, at, i * sw:(i + 1) * sw] = (v * moe_gain[:, lo:lo + sw]).astype(BF16)
            ssq[at, :] = acc if h == 0 else ssq[at, :] + acc

    def rows_at(first, number):
        return pl.ds(pl.multiple_of(first * cap, count * cap), number * cap)

    def partial_dot(weight, h, at, cs):
        acc = None
        for i in range(p):
            lo = i * share + h * sw
            piece = dot(xn[h, at, i * sw:(i + 1) * sw], weight[lo:lo + sw, cs])
            acc = piece if acc is None else acc + piece
        return acc

    def early(k, weight, f, h, first, number):
        cs = slice(f * fc, (f + 1) * fc)
        at = rows_at(first, number)
        value = partial_dot(weight, h, at, cs)
        gacc[k, at, cs] = value if h == 0 else gacc[k, at, cs] + value

    def dots(h, first, number):
        for f in range(hidden // fc):
            early(0, weg, f, h, first, number)
            early(1, weu, f, h, first, number)

    def activate(first, number):
        at = rows_at(first, number)
        row_scale = lax.rsqrt(ssq[at, :] / width + 1e-06)
        for f in range(hidden // fc):
            cs = slice(f * fc, (f + 1) * fc)
            gate_part = gacc[0, at, cs] * row_scale
            hid[at, cs] = (jax.nn.silu(gate_part) * (gacc[1, at, cs] * row_scale)).astype(BF16)

    here = high * count if split == 2 else 0
    there = (1 - high) * count if split == 2 else 0

    def gathered(h):
        for dy in range(1, ys):
            origin = lax.rem(y - dy + ys, ys)
            copy_g(dy, h).wait_recv()
            sdo[dy - 1, h] = dot(dispatch, ag[origin, h]).reshape(n, cap, sw).astype(BF16)
            for peer in near:
                copy_o(dy, peer, h).start()
            rows[h, origin * 2 + core, e] = sdo[dy - 1, h, e]
            copy_c3(dy, e, h).start()

    def near_own(src, h):
        landed_c1(src, h).wait_recv()
        copy_c3(0, src, h).start()

    def near_other(src, h):
        for dy in range(1, ys):
            landed_o(dy, src, h).wait_recv()
            copy_c3(dy, src, h).start()

    def pass_on(src, h):
        for dy in range(1, ys):
            landed_c2(dy, src, h).wait_recv()
            copy_c3(dy, src, h, 1).start()

    def cross(src, h):
        landed_c1(src, h).wait_recv()
        for dy in range(1, ys):
            copy_c2(dy, src, h).start()
        copy_c3(0, src, h, 1).start()

    def each(action, sources, h):
        for src in sources:
            action(src, h)

    nearest = beyond[0] if beyond else []
    farthest = [src for group in beyond[1:] for src in group]
    gathered(0)
    send_half(1)
    each(cross, farthest, 0)
    gathered(1)
    each(cross, nearest, 0)
    each(pass_on, farthest, 0)
    each(near_own, near, 0)
    each(near_other, near, 0)
    each(pass_on, nearest, 0)
    each(cross, farthest, 1)
    each(cross, nearest, 1)
    each(near_own, near, 1)
    each(near_other, near, 1)
    loads[5].wait()
    loads[6].wait()
    scaled_rows(0, 0, n, 0)
    dots(0, 0, n)
    each(pass_on, farthest, 1)
    each(pass_on, nearest, 1)
    if split == 2:
        scaled_rows(HALVES - 1, here, count, 0)
        dots(HALVES - 1, here, count)

    scaled_rows(HALVES - 1, there, count, split - 1)
    dots(HALVES - 1, there, count)
    activate(there, count)

    loads[7].wait()
    chunk = nx * cap

    def copy_e1(plane, yy, h):
        return remote(e_p.at[plane, yy, h], e_r.at[plane, yy, h], se1, re1.at[plane, yy, h], {"tp": q})

    def copy_e2(plane, dy, h):
        ty = lax.rem(y + dy, ys)
        return remote(
            es.at[plane, ty, h], er.at[plane, y, h], se2, re2.at[plane, dy - 1, h],
            {"tp": ty * 2 + core},
        )

    def mine_of(dx):
        return pl.ds(pl.multiple_of(beside(dx) * cap, cap), cap)

    def copy_own(dy, dx, h):
        ty = lax.rem(y + dy, ys)
        return remote(
            es.at[z, ty, h, mine_of(dx)], er.at[z, y, h, mine_of(dx)], se2, ro2.at[dy - 1, dx, h],
            {"tp": ty * 2 + core},
        )

    own_order = [(dx, h) for dx in list(range(1, nx)) + [0] for h in range(HALVES)]

    def copy_e3(peer, h):
        return remote(outb.at[h, peer], ret.at[h, e], se3, re3.at[h], {"ep": peer})

    def issue(planes, dys):
        mine = jnp.concatenate([hid[pl.ds(pl.multiple_of(k * chunk, chunk), chunk), :] for k in planes], axis=0)
        for dy in dys:
            ty = lax.rem(y + dy, ys)
            for h in range(HALVES):
                value = dot(mine, wed[:, block(ty * 2 + 1 - core, h)]).astype(BF16)
                for i, k in enumerate(planes):
                    e_p[k, ty, h] = value[i * chunk:(i + 1) * chunk]
                    copy_e1(k, ty, h).start()
            for h in range(HALVES):
                value = dot(mine, wed[:, block(ty * 2 + core, h)])
                for i, k in enumerate(planes):
                    e_o[k, ty, h] = value[i * chunk:(i + 1) * chunk]

    def push(plane):
        for dy in range(1, ys):
            ty = lax.rem(y + dy, ys)
            for h in range(HALVES):
                copy_e1(plane, ty, h).wait_recv()
                es[plane, ty, h] = (e_o[plane, ty, h] + e_r[plane, ty, h].astype(F32)).astype(BF16)
                copy_e2(plane, dy, h).start()

    def push_own():
        for dy in range(1, ys):
            ty = lax.rem(y + dy, ys)
            for h in range(HALVES):
                copy_e1(z, ty, h).wait_recv()
            for dx, h in own_order:
                at = mine_of(dx)
                es[z, ty, h, at] = (e_o[z, ty, h, at] + e_r[z, ty, h, at].astype(F32)).astype(BF16)
                copy_own(dy, dx, h).start()

    def deliver_own():
        for h in range(HALVES):
            copy_e1(z, y, h).wait_recv()
        for dx, h in own_order:
            at = mine_of(dx)
            result = e_o[z, y, h, at] + e_r[z, y, h, at].astype(F32)
            for dy in range(1, ys):
                copy_own(dy, dx, h).wait_recv()
                result = result + er[z, lax.rem(y - dy + ys, ys), h, at].astype(F32)
            if dx:
                outb[h, peer_of(z, dx)] = result.astype(BF16)
                copy_e3(peer_of(z, dx), h).start()
            else:
                ret[h, e] = result.astype(BF16)

    def deliver(plane):
        for h in range(HALVES):
            copy_e1(plane, y, h).wait_recv()
            result = e_o[plane, y, h] + e_r[plane, y, h].astype(F32)
            for dy in range(1, ys):
                copy_e2(plane, dy, h).wait_recv()
                result = result + er[plane, lax.rem(y - dy + ys, ys), h].astype(F32)
            result = result.reshape(nx, cap, sw).astype(BF16)
            outb[h, pl.ds(plane * nx, nx)] = result
            for dx in range(nx):
                copy_e3(peer_of(plane, dx), h).start()

    order = [across(j) for j in range(nz - 1)] + [z]
    pairs = [order[i:i + 2] for i in range(0, nz, 2)]
    waiting = split == 2
    for i, planes in enumerate(pairs):
        if waiting and 2 * i + len(planes) > ncross:
            waiting = False
            activate(here, count)
        issue(planes, range(1, ys))
        issue(planes, [0])
        for plane in planes:
            push_own() if plane is z else push(plane)

    @pl.loop(0, nz - 1)
    def _(j):
        deliver(across(j))

    deliver_own()

    def combine(weights, back):
        return lax.dot_general(weights, back, (((0,), (0,)), ((), ())), preferred_element_type=F32)

    for h in range(HALVES):
        others = ret.at[h, pl.ds(0, n - 1)]
        remote(others, others, se3, re3.at[h], {"ep": peer_of(z, 1)}).wait_recv()
        back = ret[h].astype(F32).reshape(slots, sw).astype(BF16)
        layer_v[:, h * sw:(h + 1) * sw] = (
            mixed[h] + combine(comb_hi, back) + combine(comb_lo, back)
        ).astype(BF16)

    puts[2].start()

    def drain(ref, sem):
        remote(ref, ref, sem, ra.at[0], {"tp": q}).wait_send()

    drain(normed.at[pl.ds(0, n - 1), half], sa)
    drain(cols.at[pl.ds(0, n - 1), half], sa2)
    if paired:
        @pl.when(middle)
        def _():
            drain(part.at[pl.ds(0, nz - 1), pl.ds(0, nx - 1)], sb)
            drain(part.at[0, pl.ds(0, nx - 1), pl.ds(0, late)], sb)
            drain(zf, szf)

        @pl.when(jnp.logical_not(middle))
        def _():
            drain(part.at[:, pl.ds(0, nx - 1)], sb)
    else:
        drain(part.at[:, pl.ds(0, nx - 1)], sb)
    drain(zsend.at[pl.ds(0, nz - 1)], sz)
    drain(op_p, sd1)
    drain(hs.at[pl.ds(0, ys - 1)], sd2)
    drain(sd.at[:, pl.ds(0, n - 1)], sc1)
    drain(rows.at[:, pl.ds(0, ys - 1), pl.ds(0, n - 1 - len(near))], sc2)
    drain(ag.at[pl.ds(0, ys - 1)], sag)
    drain(sdo.at[:, :, pl.ds(0, len(near))], sco)
    drain(rows.at[:, pl.ds(0, ys)], sc3)
    drain(e_p, se1)
    drain(es.at[:, pl.ds(0, ys - 1)], se2)
    drain(outb.at[:, pl.ds(0, n - 1)], se3)

    for put in puts:
        put.wait()


def finish(layer_in, state_in, conv_in, layer_out, state_out, conv_out):
    layer_out[...] = layer_in[...]
    state_out[...] = state_in[...]
    conv_out[...] = conv_in[...]


def shards(
    n, p,
    tokens, state_in, conv_in, mix_gain, rnn_weight, gate_weight, conv_weight, rate_weight,
    input_weight, rate_param, out_weight, moe_gain, expert_gate, expert_up, expert_down, routes, route_prob,
):
    g, width = tokens.shape
    depth, chans = rnn_weight.shape
    share = width // p
    cap = max(2, 2 * g * routes.shape[1] // n)
    slots = n * cap
    hidden = expert_gate.shape[2]
    ys = p // 2
    nx = 1 << ((n.bit_length() - 1) // 2)
    nx = nx if n % nx == 0 else 1
    nz = n // nx
    nc, cw = rate_weight.shape[0], 2 * rate_weight.shape[1]
    nh, sw = HALVES, share // HALVES
    chunk = nx * cap
    vm = pl.BlockSpec(memory_space=pltpu.VMEM)
    hb = pl.BlockSpec(memory_space=pl.ANY)
    dma = pltpu.SemaphoreType.DMA
    V = pltpu.VMEM
    small = (
        tokens, state_in, jnp.transpose(conv_in, (1, 0, 2)), mix_gain.reshape(-1, 128), moe_gain.reshape(-1, 128),
        conv_weight, rate_param[None], routes.T, route_prob.T,
    )
    scratch = [V(a.shape, a.dtype) for a in small] + [
        V((g, share), BF16), V((g, chans), F32), V((conv_in.shape[1], g, chans), BF16),
        V((depth, chans), BF16), V((depth, chans), BF16),
        V(rate_weight.shape, BF16), V(input_weight.shape, BF16), V(out_weight.shape, BF16),
        V(expert_gate.shape[1:], BF16), V(expert_up.shape[1:], BF16), V(expert_down.shape[1:], BF16),
        V((1, width), F32), V((1, width), F32),
        V((n, g, depth), BF16), V((n, g, depth), BF16),
        V((nz, nx, nc, g, cw), BF16), V((nz, nx, nc, g, cw), BF16),
        V((nz, nc, g, cw), BF16), V((2, nz, nc, g, cw), BF16), V((nx - 1, nc - nc // 2, g, cw), BF16),
        V((g, chans), BF16), V((p, nh, g, sw), F32),
        V((ys, nh, g, sw), BF16), V((ys, nh, g, sw), F32), V((ys, nh, g, sw), BF16),
        V((ys, nh, g, sw), BF16), V((ys, nh, g, sw), BF16), V((nh, g, sw), F32),
        V((nh, g, sw), BF16), V((ys, nh, g, sw), BF16), V((ys - 1, nh, n, cap, sw), BF16),
        V((nh, n, cap, sw), BF16), V((nh, p, n, cap, sw), BF16), V((nh, slots, p * sw), BF16), V((slots, 1), F32),
        V((2, slots, hidden), F32), V((slots, hidden), BF16),
        V((nz, ys, nh, chunk, sw), BF16), V((nz, ys, nh, chunk, sw), F32), V((nz, ys, nh, chunk, sw), BF16),
        V((nz, ys, nh, chunk, sw), BF16), V((nz, ys, nh, chunk, sw), BF16),
        V((nh, n, cap, sw), BF16), V((nh, n, cap, sw), BF16),
        dma((8,)), dma((len(small),)), dma((3,)),
        dma, dma((nz,)), dma, dma((nz,)),
        dma, dma((nz, nx - 1, nc)), dma, dma((nz + 1, nc)), dma, dma((nx - 1, nc - nc // 2)),
        dma, dma((ys, nh)), dma, dma((ys - 1, nh)),
        dma, dma((ys - 1, nh)), dma,
        dma, dma((n, nh)), dma, dma((ys - 1, n, nh)), dma, dma((nh, 2)),
        dma, dma((nz, ys, nh)), dma, dma((nz, ys - 1, nh)), dma((ys - 1, nx, nh)), dma, dma((nh,)),
    ]
    outs = (
        jax.ShapeDtypeStruct((g, share), BF16),
        jax.ShapeDtypeStruct((g, chans), F32),
        jax.ShapeDtypeStruct((conv_in.shape[1], g, chans), BF16),
    )
    held = pl.pallas_call(
        functools.partial(kernel, n, p, nx, cap),
        out_shape=outs,
        in_specs=[hb] * 17,
        out_specs=(hb, hb, hb),
        scratch_shapes=scratch,
        compiler_params=pltpu.CompilerParams(
            collective_id=0, has_side_effects=True, vmem_limit_bytes=60 * 1024 * 1024
        ),
    )(
        *small,
        rnn_weight, gate_weight, rate_weight, input_weight, out_weight, expert_gate, expert_up, expert_down,
    )
    layer_out, state_out, conv_out = pl.pallas_call(
        finish,
        out_shape=outs,
        in_specs=[vm] * 3,
        out_specs=(vm, vm, vm),
    )(*held)
    return (layer_out, state_out, jnp.transpose(conv_out, (1, 0, 2)))


def solution(mesh):
    in_specs = (
        P("ep", None),
        P("ep", "tp"),
        P("ep", None, "tp"),
        P(),
        P("ep", "tp"),
        P("ep", "tp"),
        P(None, "tp"),
        P("tp", None, None),
        P("tp", None, None),
        P("tp"),
        P("tp", None),
        P(),
        P("ep", None, "tp"),
        P("ep", None, "tp"),
        P("ep", "tp", None),
        P("ep", None),
        P("ep", None),
    )
    out_specs = (P("ep", "tp"), P("ep", "tp"), P("ep", None, "tp"))
    body = functools.partial(shards, mesh.shape["ep"], mesh.shape["tp"])
    return jax.shard_map(body, mesh=mesh, in_specs=in_specs, out_specs=out_specs, check_vma=False)
```
